128 devices in a mesh: sp: 32 (over z, y, core), tp: 4 (over x).
Axes of the slice: x: 4, y: 4, z: 4, core: 2. Of those that a mesh axis runs over, the one named last changes fastest.
Arguments:
- queries: bfloat16 [32768, 1024], P('sp', 'tp'), may hold values from -6 to 6
- keys: bfloat16 [32768, 1024], P('sp', 'tp'), may hold values from -6 to 6
- values: bfloat16 [32768, 1024], P('sp', 'tp'), may hold values from -6 to 6
- gates: bfloat16 [32768, 1024], P('sp', 'tp'), may hold values from -6 to 6
- log_decay: float32 [32768, 8], P('sp', 'tp'), may hold values from -1.6 to 0, as said below
- norm_gain: float32 [8, 128], P('tp'), may hold values from 0.1 to 1.9
- out_weight: bfloat16 [1024, 2048], P('tp'), may hold values from -0.1875 to 0.1875
- resid: bfloat16 [32768, 2048], P(('sp', 'tp')), may hold values from -6 to 6
- post_mix_gain: float32 [2048], replicated, may hold values from 0.1 to 1.9
- pre_ffn_gain: float32 [2048], replicated, may hold values from 0.1 to 1.9
- w_gate: bfloat16 [2048, 5632], P('sp', 'tp'), may hold values from -0.125 to 0.125
- w_up: bfloat16 [2048, 5632], P('sp', 'tp'), may hold values from -0.125 to 0.125
- w_down: bfloat16 [5632, 2048], P('tp', 'sp'), may hold values from -0.078125 to 0.078125
- post_ffn_gain: float32 [2048], replicated, may hold values from 0.1 to 1.9
Outputs:
- updated: bfloat16 [32768, 2048], P(('sp', 'tp'))
The draws below stay inside these ranges and needn't reach their ends.
Inputs may be any that keep to these rules, and one draw needn't show every extreme that they name: `log_decay`: every entry is negative.
All inputs are finite; a program needn't handle non-finite values.
Results may differ from the reference program's by a relative error of at most 0.02.
Values may be sent and summed in bfloat16 or wider, within the bound.
A program may use at most 128 MiB of HBM per device.

```python
import math
import jax
import jax.numpy as jnp
from jax import lax

D = 2048
RETENTION_HEADS = 8
HEAD_DIM = 128
FF = 5632
TOK_DEV = 1024
RET_W = 1024
BLOCK = 512
SEQUENCE_TOKENS = 32768
N_TP = 4


def draw_log_decay(key, part):
    random_child_keys = jax.random.split(jax.random.fold_in(key, 17), 6)
    fast_share = 0.5
    is_fast = jax.random.uniform(random_child_keys[0], (RETENTION_HEADS,), jnp.float32) < fast_share
    fast_rate = jax.random.uniform(random_child_keys[1], (RETENTION_HEADS,), jnp.float32, 0.08, 0.15)
    baseline_decay_rate = jnp.where(is_fast, fast_rate, 0.6 / SEQUENCE_TOKENS)
    span_count = SEQUENCE_TOKENS // TOK_DEV
    factor = jnp.exp(jax.random.uniform(random_child_keys[2], (span_count, RETENTION_HEADS), jnp.float32, math.log(0.4), math.log(1.6)))
    row_values = jnp.repeat(factor, TOK_DEV, axis=0)
    random_noise = jax.random.uniform(random_child_keys[3], (SEQUENCE_TOKENS, RETENTION_HEADS), jnp.float32, 0.5, 1.5)
    spike_position = jax.random.randint(random_child_keys[4], (2, RETENTION_HEADS), 0, SEQUENCE_TOKENS)
    spike_length = jnp.log(jax.random.uniform(random_child_keys[5], (2, RETENTION_HEADS), jnp.float32, 0.55, 0.8))
    token_positions = lax.broadcasted_iota(jnp.int32, (SEQUENCE_TOKENS, RETENTION_HEADS), 0)
    spike_events = jnp.where(token_positions == spike_position[0][None, :], spike_length[0][None, :], 0.0)
    spike_events = spike_events + jnp.where(token_positions == spike_position[1][None, :], spike_length[1][None, :], 0.0)
    return (-baseline_decay_rate[None, :] * row_values * random_noise + spike_events).astype(jnp.float32)


def steps_of(own_key, extent, shards, low, largest):
    loudness, own = 1.0, jax.random.fold_in(own_key, 6)
    for axis_at, blocks in shards:
        draws = jnp.exp(jax.random.uniform(jax.random.fold_in(own, axis_at), (blocks,), jnp.float32, low / len(shards), largest / len(shards)))
        loudness = loudness * jnp.repeat(draws, extent[axis_at] // blocks).reshape([-1 if axis == axis_at else 1 for axis in range(len(extent))])
    return loudness


def normal_values(own_key, shape, spread, reach, cuts=(), dtype=jnp.bfloat16):
    result = spread * jax.random.normal(own_key, shape, jnp.float32)
    if cuts:
        result = result * steps_of(own_key, shape, cuts, -0.22, 0.18)
    return jnp.clip(result, -reach, reach).astype(dtype)


def setup_inputs(seed: int = 0) -> dict:
    streams_of = jax.random.split(jax.random.key(seed), 15)
    return {
        "queries": normal_values(streams_of[0], (SEQUENCE_TOKENS, RET_W), 1.0, 6.0, ((0, 32), (1, 4))),
        "keys": normal_values(streams_of[1], (SEQUENCE_TOKENS, RET_W), 1.0, 6.0, ((0, 32), (1, 4))),
        "values": normal_values(streams_of[2], (SEQUENCE_TOKENS, RET_W), 1.0, 6.0, ((0, 32), (1, 4))),
        "gates": normal_values(streams_of[3], (SEQUENCE_TOKENS, RET_W), 1.0, 6.0, ((0, 32), (1, 4))),
        "log_decay": draw_log_decay(jax.random.fold_in(streams_of[14], 71), 0),
        "norm_gain": jnp.clip(1.0 + 0.18 * jax.random.normal(streams_of[5], (RETENTION_HEADS, HEAD_DIM), jnp.float32), 0.1, 1.9),
        "out_weight": normal_values(streams_of[6], (RET_W, D), RET_W ** -0.5, 0.1875, ((0, 4),)),
        "resid": normal_values(streams_of[7], (SEQUENCE_TOKENS, D), 1.0, 6.0, ((0, 128),)),
        "post_mix_gain": jnp.clip(1.0 + 0.18 * jax.random.normal(streams_of[8], (D,), jnp.float32), 0.1, 1.9),
        "pre_ffn_gain": jnp.clip(1.0 + 0.18 * jax.random.normal(streams_of[9], (D,), jnp.float32), 0.1, 1.9),
        "w_gate": normal_values(streams_of[10], (D, FF), D ** -0.5, 0.125, ((0, 32), (1, 4))),
        "w_up": normal_values(streams_of[11], (D, FF), D ** -0.5, 0.125, ((0, 32), (1, 4))),
        "w_down": normal_values(streams_of[12], (FF, D), FF ** -0.5, 0.078125, ((0, 4), (1, 32))),
        "post_ffn_gain": jnp.clip(1.0 + 0.18 * jax.random.normal(streams_of[13], (D,), jnp.float32), 0.1, 1.9),
    }


EPSILON = 1e-06

def rms_norm(values_in, gain_vec):
    widened = values_in.astype(jnp.float32)
    return widened * lax.rsqrt(lax.optimization_barrier(jnp.mean(widened * widened, axis=-1, keepdims=True)) + EPSILON) * gain_vec.astype(jnp.float32)

def block_step(carried, pieces):
    query_blk, key_blk, value_blk, decay_blk = pieces
    length = query_blk.shape[1]
    key_scale = query_blk.shape[2] ** (-0.5)
    query_wide = query_blk.astype(jnp.float32)
    key_wide = key_blk.astype(jnp.float32)
    value_wide = value_blk.astype(jnp.float32)
    cumulative = jnp.cumsum(decay_blk, axis=1)
    log_gap = cumulative[:, :, None] - cumulative[:, None, :]
    causal = lax.broadcasted_iota(jnp.int32, (length, length), 0) >= lax.broadcasted_iota(jnp.int32, (length, length), 1)
    weight = jnp.where(causal[None], jnp.exp(jnp.minimum(log_gap, 0.0)), 0.0)
    products = jnp.einsum('htd,hsd->hts', query_wide, key_wide)
    scores = lax.optimization_barrier((products * key_scale * weight).astype(jnp.bfloat16))
    within = jnp.einsum('hts,hsd->htd', scores.astype(jnp.float32), value_wide)
    carried_term = jnp.einsum('htd,hde->hte', query_wide, carried, precision=lax.Precision.HIGHEST) * jnp.exp(cumulative)[:, :, None]
    to_end = jnp.exp(cumulative[:, -1:] - cumulative) * key_scale
    scaled_keys = lax.optimization_barrier((key_wide * to_end[:, :, None]).astype(jnp.bfloat16))
    added = jnp.einsum('hsd,hse->hde', scaled_keys.astype(jnp.float32), value_wide)
    carried = jnp.exp(cumulative[:, -1])[:, None, None] * carried + added
    return (carried, within + carried_term)

def to_blocks(matrix, block_len, head_count):
    row_count = matrix.shape[0]
    return matrix.reshape(row_count // block_len, block_len, head_count, -1).transpose(0, 2, 1, 3)

def finish_heads(retention, gates, norm_gain):
    centered = retention - lax.optimization_barrier(jnp.mean(retention, axis=-1, keepdims=True))
    variance = lax.optimization_barrier(jnp.mean(centered * centered, axis=-1, keepdims=True))
    normed = centered * lax.rsqrt(variance + EPSILON) * norm_gain.astype(jnp.float32)[None]
    gate_vals = gates.astype(jnp.float32).reshape(normed.shape)
    return (jax.nn.silu(gate_vals) * normed).reshape(normed.shape[0], -1).astype(jnp.bfloat16)

def grouped_product(left, right, group_count):
    inner = left.shape[1] // group_count
    total = jnp.zeros((left.shape[0], right.shape[1]), jnp.float32)
    for group in range(group_count):
        part = jnp.dot(left[:, group * inner:(group + 1) * inner], right[group * inner:(group + 1) * inner], preferred_element_type=jnp.float32)
        total = total + part.astype(jnp.bfloat16).astype(jnp.float32)
    return total.astype(jnp.bfloat16)

def reference(queries, keys, values, gates, log_decay, norm_gain, out_weight, resid, post_mix_gain, pre_ffn_gain, w_gate, w_up, w_down, post_ffn_gain):
    block_count = SEQUENCE_TOKENS // BLOCK
    query_blocks = to_blocks(queries, BLOCK, RETENTION_HEADS)
    key_blocks = to_blocks(keys, BLOCK, RETENTION_HEADS)
    value_blocks = to_blocks(values, BLOCK, RETENTION_HEADS)
    decay_blocks = log_decay.reshape(block_count, BLOCK, RETENTION_HEADS).transpose(0, 2, 1)
    start_state = jnp.zeros((RETENTION_HEADS, HEAD_DIM, HEAD_DIM), jnp.float32)
    _, outputs = lax.scan(block_step, start_state, (query_blocks, key_blocks, value_blocks, decay_blocks))
    retention = outputs.transpose(0, 2, 1, 3).reshape(SEQUENCE_TOKENS, RETENTION_HEADS, HEAD_DIM)
    retained = finish_heads(retention, gates, norm_gain)
    mixed = grouped_product(retained, out_weight, N_TP)
    middle = (resid.astype(jnp.float32) + rms_norm(mixed, post_mix_gain)).astype(jnp.bfloat16)
    ffn_input = rms_norm(middle, pre_ffn_gain).astype(jnp.bfloat16)

    def ffn_rows(row_block):
        gate_act = jnp.dot(row_block, w_gate, preferred_element_type=jnp.float32)
        up_act = jnp.dot(row_block, w_up, preferred_element_type=jnp.float32)
        hidden = (jax.nn.silu(gate_act) * up_act).astype(jnp.bfloat16)
        return grouped_product(hidden, w_down, N_TP)
    branch = lax.map(ffn_rows, ffn_input.reshape(SEQUENCE_TOKENS // TOK_DEV, TOK_DEV, D)).reshape(SEQUENCE_TOKENS, D)
    return (middle.astype(jnp.float32) + rms_norm(branch, post_ffn_gain)).astype(jnp.bfloat16)
```

```python
import jax
import jax.numpy as jnp
from jax import lax
from jax.experimental import pallas as pl
from jax.experimental.pallas import tpu as pltpu
from jax.sharding import Mesh
from jax.sharding import PartitionSpec as P

BLOCK = 512
SP = ("sp_0", "sp_1", "sp_2")
SP_TP = ("sp_0", "sp_1", "sp_2", "tp")


EPSILON = 1e-06
MESH_ID = pl.DeviceIdType.MESH
Z, Y, C, X = SP_TP


class Links:
    def __init__(self, send_sem, recv_sem):
        self.send_sem, self.recv_sem, self.copies = send_sem, recv_sem, []

    def send(self, src, dst, **where):
        at = len(self.copies)
        copy = pltpu.make_async_remote_copy(
            src_ref=src,
            dst_ref=dst,
            send_sem=self.send_sem.at[at],
            recv_sem=self.recv_sem.at[at],
            device_id={axis: index for axis, index in where.items()},
            device_id_type=MESH_ID,
        )
        copy.start()
        self.copies.append(copy)
        return copy

    def finish(self):
        for copy in self.copies:
            copy.wait_send()


class PlaneGather:
    def __init__(self, links, at, first, second, here, core):
        self.links, self.at, self.first, self.second, self.core = links, at, first, second, core
        self.i, self.j = here
        self.i_up, self.i_down = lax.rem(self.i + 1, 4), lax.rem(self.i + 3, 4)
        self.j_up, self.j_down = lax.rem(self.j + 1, 4), lax.rem(self.j + 3, 4)
        self.across = []

    def both_ways(self, axis, up, down, block):
        return (
            self.links.send(block, block, **{axis: up}),
            self.links.send(block, block, **{axis: down}),
        )

    def own(self):
        self.up, self.down = self.both_ways(
            self.first, self.i_up, self.i_down, self.at(self.i, self.j)
        )

    def pass_on(self):
        self.up.wait_recv()
        block = self.at(self.i_down, self.j, part=0)
        up = self.links.send(block, block, **{self.first: self.i_up})
        self.down.wait_recv()
        block = self.at(self.i_up, self.j, part=1)
        self.up, self.down = up, self.links.send(block, block, **{self.first: self.i_down})

    def give(self, j):
        block = self.at(pl.ds(0, 4), j)
        self.across.append(self.links.send(block, block, **{C: 1 - self.core}))

    def line(self):
        self.up.wait_recv()
        self.down.wait_recv()
        self.up, self.down = self.both_ways(
            self.second, self.j_up, self.j_down, self.at(pl.ds(0, 4), self.j)
        )
        self.give(self.j)

    def pass_line(self):
        self.up.wait_recv()
        block = self.at(pl.ds(0, 2), self.j_down)
        up = self.links.send(block, block, **{self.second: self.j_up})
        self.down.wait_recv()
        block = self.at(pl.ds(2, 2), self.j_up)
        down = self.links.send(block, block, **{self.second: self.j_down})
        self.up, self.down = up, down
        self.give(self.j_down)
        self.give(self.j_up)

    def end_line(self):
        self.up.wait_recv()
        self.down.wait_recv()
        self.give(lax.rem(self.j + 2, 4))

    def arrive(self):
        for copy in self.across:
            copy.wait_recv()


def ffn_kernel(
    ffn_in, middle, w_gate, w_up, w_down, gain, out,
    gate_all, up_all, down_all, rows, hidden, partial, relay, final, half_down, local_sem, send_sem, recv_sem,
):
    z, y, c, x = (lax.axis_index(axis) for axis in SP_TP)
    other, x_up, x_down, x_far = 1 - c, lax.rem(x + 1, 4), lax.rem(x + 3, 4), lax.rem(x + 2, 4)
    copies = [
        pltpu.make_async_copy(w_gate, gate_all.at[z, y, c], local_sem.at[0]),
        pltpu.make_async_copy(w_up, up_all.at[z, y, c], local_sem.at[1]),
        pltpu.make_async_copy(
            w_down.at[pl.ds(pl.multiple_of(704 * c, 64), 704)], half_down.at[c], local_sem.at[2]
        ),
        pltpu.make_async_copy(ffn_in, rows.at[x], local_sem.at[3]),
    ]
    for copy in copies:
        copy.start()

    barrier = pltpu.get_barrier_semaphore()
    near = [{C: other}]
    for axis, index in ((X, x), (Y, y), (Z, z)):
        near += [{axis: lax.rem(index + 1, 4)}, {axis: lax.rem(index + 3, 4)}]
    for where in near:
        pl.semaphore_signal(barrier, inc=1, device_id=where, device_id_type=MESH_ID)
    pl.semaphore_wait(barrier, len(near))

    links = Links(send_sem, recv_sem)
    swap = links.send(
        w_down.at[pl.ds(pl.multiple_of(704 * other, 64), 704)], half_down.at[c], **{C: other}
    )

    def gate_at(i, j, part=None):
        lines = pl.ds(0, 64) if part is None else pl.ds(32 * part, 32)
        return gate_all.at[j, i, c, lines]

    def up_at(i, j, part=None):
        lines = pl.ds(0, 64) if part is None else pl.ds(32 * part, 32)
        return up_all.at[i, j, c, lines]

    def down_lines(start, part):
        first, length = (start, 352) if part is None else (start + 176 * part, 176)
        return pl.ds(pl.multiple_of(704 * c + first, 16), length)

    gathers = (
        PlaneGather(links, gate_at, Y, Z, (y, z), c),
        PlaneGather(links, up_at, Z, Y, (z, y), c),
        PlaneGather(
            links, lambda i, j, part=None: down_all.at[j, i, down_lines(0, part)], Y, Z, (y, z), c
        ),
        PlaneGather(
            links, lambda i, j, part=None: down_all.at[i, j, down_lines(352, part)], Z, Y, (z, y), c
        ),
    )
    wide, narrow = gathers[:2], gathers[2:]
    copies[0].wait()
    copies[1].wait()
    for g in wide:
        g.own()
    copies[3].wait()
    top, bottom = pl.ds(0, 128), pl.ds(128, 128)
    up_top = links.send(rows.at[x, top], rows.at[x, top], **{X: x_up})
    down_bottom = links.send(rows.at[x, bottom], rows.at[x, bottom], **{X: x_down})
    copies[2].wait()
    swap.wait_recv()
    down_all[z, y, pl.ds(pl.multiple_of(704 * c, 64), 704), :] = jnp.concatenate(
        [half_down[0], half_down[1]], axis=1
    )
    for g in wide:
        g.pass_on()
    for g in narrow:
        g.own()
    for g in wide:
        g.line()
    for g in narrow:
        g.pass_on()
    up_top.wait_recv()
    far_top = links.send(rows.at[x_down, top], rows.at[x_down, top], **{X: x_up})
    down_bottom.wait_recv()
    far_bottom = links.send(rows.at[x_up, bottom], rows.at[x_up, bottom], **{X: x_down})
    up_bottom = links.send(rows.at[x, bottom], rows.at[x, bottom], **{X: x_up})
    down_top = links.send(rows.at[x, top], rows.at[x, top], **{X: x_down})
    for g in narrow:
        g.line()
    for g in wide:
        g.pass_line()
    for g in wide:
        g.end_line()
    for g in narrow:
        g.pass_line()
    for g in wide:
        g.arrive()

    def gate_up(owner, slot):
        block = rows[owner]
        for j in range(11):
            lanes = slice(128 * j, 128 * (j + 1))
            weights = jnp.concatenate(
                [
                    gate_all[:, :, :, :, lanes].reshape(2048, 128),
                    up_all[:, :, :, :, lanes].reshape(2048, 128),
                ],
                axis=1,
            )
            both = jnp.dot(block, weights, preferred_element_type=jnp.float32)
            hidden[slot, :, lanes] = (jax.nn.silu(both[:, :128]) * both[:, 128:]).astype(jnp.bfloat16)

    def down(slot, to, lines=pl.ds(0, 256), extra=None):
        block = hidden[slot, lines, :]
        for j in range(8):
            weights = jnp.concatenate(
                [down_all[j // 2, 2 * j % 4], down_all[j // 2, 2 * j % 4 + 1]], axis=1
            )
            part = jnp.dot(block, weights, preferred_element_type=jnp.float32)
            lanes = slice(256 * j, 256 * (j + 1))
            if extra is not None:
                part = part + relay[extra, :, lanes].astype(jnp.float32)
            partial[to, lines, lanes] = part.astype(jnp.bfloat16)

    gate_up(x, 0)
    far_top.wait_recv()
    far_bottom.wait_recv()
    gate_up(x_far, 1)
    for g in narrow:
        g.end_line()
    for g in narrow:
        g.arrive()
    down(1, 1)
    relay_up = links.send(partial.at[1, top], relay.at[0], **{X: x_up})
    relay_down = links.send(partial.at[1, bottom], relay.at[1], **{X: x_down})
    down(0, 0)
    up_bottom.wait_recv()
    down_top.wait_recv()
    gate_up(x_up, 0)
    down(0, 2, bottom)
    last = [links.send(partial.at[2, bottom], final.at[0, bottom], **{X: x_up})]
    gate_up(x_down, 1)
    down(1, 3, top)
    last.append(links.send(partial.at[3, top], final.at[1, top], **{X: x_down}))
    relay_up.wait_recv()
    down(0, 2, top, 0)
    last.append(links.send(partial.at[2, top], final.at[0, top], **{X: x_up}))
    relay_down.wait_recv()
    down(1, 3, bottom, 1)
    last.append(links.send(partial.at[3, bottom], final.at[1, bottom], **{X: x_down}))
    for copy in last:
        copy.wait_recv()

    @pl.loop(0, 16)
    def _(step):
        lines = pl.ds(pl.multiple_of(16 * step, 16), 16)
        branch = (
            partial[0, lines, :].astype(jnp.float32)
            + final[0, lines, :].astype(jnp.float32)
            + final[1, lines, :].astype(jnp.float32)
        ).astype(jnp.bfloat16)
        out[lines, :] = (
            middle[lines, :].astype(jnp.float32) + rms_norm(branch, gain[...])
        ).astype(jnp.bfloat16)

    links.finish()


def feed_forward(ffn_in, middle, w_gate, w_up, w_down, gain):
    in_hbm, in_vmem = pl.BlockSpec(memory_space=pl.ANY), pl.BlockSpec(memory_space=pltpu.VMEM)
    bf16 = jnp.bfloat16
    return pl.pallas_call(
        ffn_kernel,
        out_shape=jax.ShapeDtypeStruct((256, 2048), bf16),
        in_specs=[in_hbm, in_vmem, in_hbm, in_hbm, in_hbm, in_vmem],
        out_specs=in_vmem,
        scratch_shapes=[
            pltpu.VMEM((4, 4, 2, 64, 1408), bf16),
            pltpu.VMEM((4, 4, 2, 64, 1408), bf16),
            pltpu.VMEM((4, 4, 1408, 128), bf16),
            pltpu.VMEM((4, 256, 2048), bf16),
            pltpu.VMEM((2, 256, 1408), bf16),
            pltpu.VMEM((4, 256, 2048), bf16),
            pltpu.VMEM((2, 128, 2048), bf16),
            pltpu.VMEM((2, 256, 2048), bf16),
            pltpu.VMEM((2, 704, 64), bf16),
            pltpu.SemaphoreType.DMA((4,)),
            pltpu.SemaphoreType.DMA((72,)),
            pltpu.SemaphoreType.DMA((72,)),
        ],
        compiler_params=pltpu.CompilerParams(
            collective_id=0, has_side_effects=True, vmem_limit_bytes=60 * 2**20
        ),
        name="feed_forward",
    )(ffn_in, middle, w_gate, w_up, w_down, gain)


def filled_with(x, identity):
    return jax.tree.map(
        lambda part, zero: jnp.zeros_like(part) + jnp.asarray(zero, part.dtype), x, identity
    )


def entering(x, axes, combine, identity):
    before = start = filled_with(x, identity)
    subtotal = x
    for axis in reversed(axes):
        devices, index = (lax.axis_size(axis), lax.axis_index(axis))
        pieces = jax.tree.map(
            lambda part, kind: lax.all_gather(part.astype(kind), axis),
            subtotal,
            (jnp.bfloat16, jnp.bfloat16),
        )
        inside, subtotal = (start, start)
        for k in range(devices):
            passed = k < index
            subtotal = combine(
                subtotal, jax.tree.map(lambda part, own: part[k].astype(own.dtype), pieces, x)
            )
            inside = jax.tree.map(lambda new, old: jnp.where(passed, new, old), subtotal, inside)
        before = combine(inside, before)
    return before


def rms_norm(values_in, gain_vec):
    widened = values_in.astype(jnp.float32)
    return (
        widened
        * lax.rsqrt(jnp.mean(widened * widened, axis=-1, keepdims=True) + EPSILON)
        * gain_vec
    )


def block_step(carried, pieces):
    query_blk, key_blk, value_blk, decay_blk = pieces
    length = query_blk.shape[1]
    key_scale = query_blk.shape[2] ** (-0.5)
    cumulative = jnp.cumsum(decay_blk, axis=1)
    log_gap = cumulative[:, :, None] - cumulative[:, None, :]
    causal = lax.broadcasted_iota(jnp.int32, (length, length), 0) >= lax.broadcasted_iota(
        jnp.int32, (length, length), 1
    )
    weight = jnp.where(causal[None], jnp.exp(jnp.minimum(log_gap, 0.0)), 0.0)
    products = jnp.einsum("htd,hsd->hts", query_blk, key_blk, preferred_element_type=jnp.float32)
    scores = (products * key_scale * weight).astype(jnp.bfloat16)
    within = jnp.einsum("hts,hsd->htd", scores, value_blk, preferred_element_type=jnp.float32)
    carried_term = (
        jnp.einsum(
            "htd,hde->hte", query_blk.astype(jnp.float32), carried, precision=lax.Precision.HIGHEST
        )
        * jnp.exp(cumulative)[:, :, None]
    )
    to_end = jnp.exp(cumulative[:, -1:] - cumulative) * key_scale
    scaled_keys = (key_blk.astype(jnp.float32) * to_end[:, :, None]).astype(jnp.bfloat16)
    added = jnp.einsum("hsd,hse->hde", scaled_keys, value_blk, preferred_element_type=jnp.float32)
    carried = jnp.exp(cumulative[:, -1])[:, None, None] * carried + added
    return (carried, within + carried_term)


def to_blocks(matrix, block_len, head_count):
    row_count = matrix.shape[0]
    return matrix.reshape(row_count // block_len, block_len, head_count, -1).transpose(0, 2, 1, 3)


def finish_heads(retention, gates, norm_gain):
    centered = retention - jnp.mean(retention, axis=-1, keepdims=True)
    variance = jnp.mean(centered * centered, axis=-1, keepdims=True)
    normed = centered * lax.rsqrt(variance + EPSILON) * norm_gain[None]
    gate_vals = gates.astype(jnp.float32).reshape(normed.shape)
    return (jax.nn.silu(gate_vals) * normed).reshape(normed.shape[0], -1).astype(jnp.bfloat16)


def combine_states(earlier, later):
    return (earlier[0] * later[0], later[0][:, None, None] * earlier[1] + later[1])


def per_device(
    queries,
    keys,
    values,
    gates,
    log_decay,
    norm_gain,
    out_weight,
    resid,
    post_mix_gain,
    pre_ffn_gain,
    w_gate,
    w_up,
    w_down,
    post_ffn_gain,
):
    row_count = queries.shape[0]
    head_count = log_decay.shape[1]
    head_dim = queries.shape[1] // head_count
    block_count = row_count // BLOCK
    query_blocks = to_blocks(queries, BLOCK, head_count)
    key_blocks = to_blocks(keys, BLOCK, head_count)
    value_blocks = to_blocks(values, BLOCK, head_count)
    decay_blocks = log_decay.reshape(block_count, BLOCK, head_count).transpose(0, 2, 1)
    start_state = jnp.zeros((head_count, head_dim, head_dim), jnp.float32)
    local_state, outputs = lax.scan(
        block_step, start_state, (query_blocks, key_blocks, value_blocks, decay_blocks)
    )
    retention = outputs.transpose(0, 2, 1, 3).reshape(row_count, head_count, head_dim)
    cumulative = jnp.cumsum(log_decay, axis=0)
    local_decay = jnp.exp(cumulative[-1])
    identity = (jnp.ones_like(local_decay), jnp.zeros_like(local_state))
    incoming = entering((local_decay, local_state), SP, combine_states, identity)
    query_rows = queries.reshape(row_count, head_count, head_dim).astype(jnp.float32)
    retention = (
        retention
        + jnp.einsum("thd,hde->the", query_rows, incoming[1], precision=lax.Precision.HIGHEST)
        * jnp.exp(cumulative)[:, :, None]
    )
    retained = finish_heads(retention, gates, norm_gain)
    quarter = resid.shape[0]
    regrouped = lax.all_to_all(retained, "tp", split_axis=0, concat_axis=1, tiled=True)
    group_rows = out_weight.shape[0]
    empty_mix = jnp.zeros((quarter, out_weight.shape[1]), jnp.float32)
    running = empty_mix
    shard_piece = lax.all_gather(out_weight, "tp", axis=0, tiled=True)
    for offset in range(shard_piece.shape[0] // group_rows):
        columns = lax.dynamic_slice_in_dim(regrouped, offset * group_rows, group_rows, 1)
        part = jnp.dot(
            columns,
            shard_piece[offset * group_rows : (offset + 1) * group_rows],
            preferred_element_type=jnp.float32,
        )
        running = running + part.astype(jnp.bfloat16).astype(jnp.float32)
    mixed = running
    mixed = mixed.astype(jnp.bfloat16)
    middle = (resid.astype(jnp.float32) + rms_norm(mixed, post_mix_gain)).astype(jnp.bfloat16)
    ffn_input = rms_norm(middle, pre_ffn_gain).astype(jnp.bfloat16)
    return feed_forward(ffn_input, middle, w_gate, w_up, w_down, post_ffn_gain[None])


def solution(mesh):
    split = Mesh(mesh.devices.reshape(4, 4, 2, mesh.shape["tp"]), ("sp_0", "sp_1", "sp_2", "tp"))
    placed = (
        P(SP, "tp"),
        P(SP, "tp"),
        P(SP, "tp"),
        P(SP, "tp"),
        P(SP, "tp"),
        P("tp", None),
        P("tp", None),
        P(SP_TP, None),
        P(),
        P(),
        P(SP, "tp"),
        P(SP, "tp"),
        P("tp", SP),
        P(),
    )
    return jax.shard_map(
        per_device, mesh=split, in_specs=placed, out_specs=P(SP_TP, None), check_vma=False
    )
```

```python
import jax
import jax.numpy as jnp
from jax import lax
from jax.experimental import pallas as pl
from jax.experimental.pallas import tpu as pltpu
from jax.sharding import Mesh
from jax.sharding import PartitionSpec as P

BLOCK = 512
SP = ("sp_0", "sp_1", "sp_2")
SP_TP = ("sp_0", "sp_1", "sp_2", "tp")


EPSILON = 1e-06
MESH_ID = pl.DeviceIdType.MESH
Z, Y, C, X = SP_TP


class Links:
    def __init__(self, send_sem, recv_sem):
        self.send_sem, self.recv_sem, self.copies = send_sem, recv_sem, []

    def send(self, src, dst, **where):
        at = len(self.copies)
        copy = pltpu.make_async_remote_copy(
            src_ref=src,
            dst_ref=dst,
            send_sem=self.send_sem.at[at],
            recv_sem=self.recv_sem.at[at],
            device_id={axis: index for axis, index in where.items()},
            device_id_type=MESH_ID,
        )
        copy.start()
        self.copies.append(copy)
        return copy

    def finish(self):
        for copy in self.copies:
            copy.wait_send()


class PlaneGather:
    def __init__(self, links, at, first, second, here, core):
        self.links, self.at, self.first, self.second, self.core = links, at, first, second, core
        self.i, self.j = here
        self.i_up, self.i_down = lax.rem(self.i + 1, 4), lax.rem(self.i + 3, 4)
        self.j_up, self.j_down = lax.rem(self.j + 1, 4), lax.rem(self.j + 3, 4)
        self.across = []

    def both_ways(self, axis, up, down, block):
        return (
            self.links.send(block, block, **{axis: up}),
            self.links.send(block, block, **{axis: down}),
        )

    def own(self):
        self.up, self.down = self.both_ways(
            self.first, self.i_up, self.i_down, self.at(self.i, self.j)
        )

    def pass_on(self):
        self.up.wait_recv()
        block = self.at(self.i_down, self.j, part=0)
        up = self.links.send(block, block, **{self.first: self.i_up})
        self.down.wait_recv()
        block = self.at(self.i_up, self.j, part=1)
        self.up, self.down = up, self.links.send(block, block, **{self.first: self.i_down})

    def give(self, j):
        block = self.at(pl.ds(0, 4), j)
        self.across.append(self.links.send(block, block, **{C: 1 - self.core}))

    def line(self):
        self.up.wait_recv()
        self.down.wait_recv()
        self.up, self.down = self.both_ways(
            self.second, self.j_up, self.j_down, self.at(pl.ds(0, 4), self.j)
        )
        self.give(self.j)

    def pass_line(self):
        self.up.wait_recv()
        block = self.at(pl.ds(0, 2), self.j_down)
        up = self.links.send(block, block, **{self.second: self.j_up})
        self.down.wait_recv()
        block = self.at(pl.ds(2, 2), self.j_up)
        down = self.links.send(block, block, **{self.second: self.j_down})
        self.up, self.down = up, down
        self.give(self.j_down)
        self.give(self.j_up)

    def end_line(self):
        self.up.wait_recv()
        self.down.wait_recv()
        self.give(lax.rem(self.j + 2, 4))

    def arrive(self):
        for copy in self.across:
            copy.wait_recv()


class LineGather(PlaneGather):
    def __init__(self, links, at, axis, index, core):
        super().__init__(links, lambda i, j, part=None: at(i, part), axis, axis, (index, index), core)

    def share(self, i):
        block = self.at(i, 0)
        self.across.append(self.links.send(block, block, **{C: 1 - self.core}))

    def pass_on(self):
        super().pass_on()
        for i in (self.i, self.i_down, self.i_up):
            self.share(i)

    def end(self):
        self.up.wait_recv()
        self.down.wait_recv()
        self.share(lax.rem(self.i + 2, 4))


def rms_norm(values_in, gain_vec):
    widened = values_in.astype(jnp.float32)
    return (
        widened
        * lax.rsqrt(jnp.mean(widened * widened, axis=-1, keepdims=True) + EPSILON)
        * gain_vec
    )


def over_lanes(scalar):
    return jnp.broadcast_to(scalar, (1, 128))


def write_state(ref, state, decay):
    ref[pl.ds(0, 128), :] = state[0].astype(jnp.bfloat16)
    ref[pl.ds(128, 128), :] = state[1].astype(jnp.bfloat16)
    row = lax.broadcasted_iota(jnp.int32, (16, 128), 0)
    large = [d.astype(jnp.bfloat16).astype(jnp.float32) for d in decay]
    both = jnp.where(
        row == 0,
        large[0],
        jnp.where(row == 1, decay[0] - large[0], jnp.where(row == 2, large[1], decay[1] - large[1])),
    )
    ref[pl.ds(256, 16), :] = both.astype(jnp.bfloat16)


def read_state(ref):
    both = ref[pl.ds(256, 16), :].astype(jnp.float32)
    return (
        [ref[pl.ds(128 * h, 128), :].astype(jnp.float32) for h in range(2)],
        [both[2 * h : 2 * h + 1] + both[2 * h + 1 : 2 * h + 2] for h in range(2)],
    )


def followed_by(earlier, later):
    return (
        [later[1][h] * earlier[0][h] + later[0][h] for h in range(2)],
        [later[1][h] * earlier[1][h] for h in range(2)],
    )


def chosen(which, a, b):
    return jax.tree.map(lambda p, q: jnp.where(which, p, q), a, b)


def layer_kernel(
    queries, keys, values, gates, log_decay, norm_gain, out_weight, resid, mix_gain, in_gain,
    w_gate, w_up, w_down, out_gain, out,
    gate_all, up_all, down_all, rows, hidden, partial, relay, final, half_down, turned,
    q, k, v, g, retention, decayed, state_c, state_y, state_z, retained, regrouped, out_all, middle,
    local_sem, send_sem, recv_sem,
):
    f32, bf16 = jnp.float32, jnp.bfloat16
    z, y, c, x = (lax.axis_index(axis) for axis in SP_TP)
    other, x_up, x_down, x_far = 1 - c, lax.rem(x + 1, 4), lax.rem(x + 3, 4), lax.rem(x + 2, 4)
    own_half = pl.ds(pl.multiple_of(704 * c, 64), 704)
    names = ("k", "v", "gate", "up", "q", "down", "weight", "g", "resid")
    moves = (
        (keys, k), (values, v), (w_gate, gate_all.at[z, y, c]), (w_up, up_all.at[z, y, c]), (queries, q),
        (w_down, half_down.at[c]), (out_weight, out_all.at[x]), (gates, g), (resid, middle),
    )
    local = {
        name: pltpu.make_async_copy(src, dst, local_sem.at[at])
        for at, (name, (src, dst)) in enumerate(zip(names, moves))
    }
    for copy in local.values():
        copy.start()

    barrier = pltpu.get_barrier_semaphore()
    near = [{C: other}]
    for axis, index in ((X, x), (Y, y), (Z, z)):
        near += [{axis: lax.rem(index + step, 4)} for step in (1, 2, 3)]
    for where in near:
        pl.semaphore_signal(barrier, inc=1, device_id=where, device_id_type=MESH_ID)
    pl.semaphore_wait(barrier, len(near))

    links = Links(send_sem, recv_sem)

    def gate_at(i, j, part=None):
        lines = pl.ds(0, 64) if part is None else pl.ds(32 * part, 32)
        return gate_all.at[j, i, c, lines]

    def up_at(i, j, part=None):
        lines = pl.ds(0, 64) if part is None else pl.ds(32 * part, 32)
        return up_all.at[i, j, c, lines]

    def down_lines(start, part):
        first, length = (start, 352) if part is None else (start + 176 * part, 176)
        return pl.ds(pl.multiple_of(704 * c + first, 16), length)

    def weight_at(i, part=None):
        first, length = (0, 128) if part is None else (64 * part, 64)
        return out_all.at[i, pl.ds(pl.multiple_of(128 * c + first, 64), length)]

    wide = (
        PlaneGather(links, gate_at, Y, Z, (y, z), c),
        PlaneGather(links, up_at, Z, Y, (z, y), c),
    )
    narrow = (
        PlaneGather(
            links, lambda i, j, part=None: down_all.at[j, i, down_lines(0, part)], Y, Z, (y, z), c
        ),
        PlaneGather(
            links, lambda i, j, part=None: down_all.at[i, j, down_lines(352, part)], Z, Y, (z, y), c
        ),
    )
    weight = LineGather(links, weight_at, X, x, c)

    scale = 128 ** (-0.5)
    at_row = lax.broadcasted_iota(jnp.int32, (BLOCK, BLOCK), 0)
    at_col = lax.broadcasted_iota(jnp.int32, (BLOCK, BLOCK), 1)
    upto = jnp.where(at_row <= at_col, 1.0, 0.0).astype(f32)
    cum_rows, cum_cols = [], []
    for b in range(2):
        logs = jnp.concatenate(
            [log_decay[:, BLOCK * b : BLOCK * (b + 1)], jnp.zeros((6, BLOCK), f32)], axis=0
        )
        cum = jnp.dot(logs, upto, precision=lax.Precision.HIGHEST, preferred_element_type=f32)
        cum_rows.append(cum)
        cum_cols.append(cum.T)
    ends = [[cum_rows[b][h : h + 1, BLOCK - 1 : BLOCK] for b in range(2)] for h in range(2)]
    local["k"].wait()
    local["v"].wait()
    first_state, span_state, span_decay = [], [], []
    for h in range(2):
        heads = slice(128 * h, 128 * (h + 1))
        added = []
        for b in range(2):
            lines = slice(BLOCK * b, BLOCK * (b + 1))
            to_end = jnp.exp(ends[h][b] - cum_cols[b][:, h : h + 1]) * scale
            scaled = (k[lines, heads].astype(f32) * to_end).astype(bf16)
            added.append(
                lax.dot_general(
                    scaled, v[lines, heads], (((0,), (0,)), ((), ())), preferred_element_type=f32
                )
            )
        first_state.append(added[0])
        span_state.append(jnp.exp(over_lanes(ends[h][1])) * added[0] + added[1])
        span_decay.append(jnp.exp(over_lanes(ends[h][0] + ends[h][1])))
    span = (span_state, span_decay)
    write_state(state_c.at[0], *span)
    pair = links.send(state_c.at[0], state_c.at[1], **{C: other})
    local["gate"].wait()
    local["up"].wait()
    for gather in wide:
        gather.own()
    local["weight"].wait()
    weight.own()
    local["down"].wait()
    swap = links.send(half_down.at[c], half_down.at[c], **{C: other})

    def within(h, b):
        heads, lines = slice(128 * h, 128 * (h + 1)), slice(BLOCK * b, BLOCK * (b + 1))
        col, row = cum_cols[b][:, h : h + 1], cum_rows[b][h : h + 1]
        products = lax.dot_general(
            q[lines, heads], k[lines, heads], (((1,), (1,)), ((), ())), preferred_element_type=f32
        )
        factor = jnp.where(at_row >= at_col, jnp.exp(jnp.minimum(col - row, 0.0)), 0.0)
        scores = (products * scale * factor).astype(bf16)
        result = jnp.dot(scores, v[lines, heads], preferred_element_type=f32)
        if b == 1:
            result = result + jnp.exp(col) * jnp.dot(
                q[lines, heads], first_state[h].astype(bf16), preferred_element_type=f32
            )
            col = col + ends[h][0]
        retention[h, lines, :] = result
        decayed[h, lines, :] = jnp.broadcast_to(jnp.exp(col), (BLOCK, 128))

    nothing = ([jnp.zeros((128, 128), f32)] * 2, [jnp.ones((1, 128), f32)] * 2)

    def among(slots, axis, index):
        sent = [
            links.send(slots.at[index], slots.at[index], **{axis: lax.rem(index + step, 4)})
            for step in (1, 2, 3)
        ]

        def fold():
            for copy in sent:
                copy.wait_recv()
            total, before = nothing, nothing
            for at in range(4):
                total = followed_by(total, read_state(slots.at[at]))
                before = chosen(at < index, total, before)
            return total, before

        return fold

    local["q"].wait()
    within(0, 0)
    pair.wait_recv()
    partner = read_state(state_c.at[1])
    first = c == 0
    chip = followed_by(chosen(first, span, partner), chosen(first, partner, span))
    before_core = chosen(first, nothing, partner)
    write_state(state_y.at[y], *chip)
    fold_y = among(state_y, Y, y)
    within(0, 1)
    for gather in wide:
        gather.pass_on()
    within(1, 0)
    line, before_y = fold_y()
    write_state(state_z.at[z], *line)
    fold_z = among(state_z, Z, z)
    swap.wait_recv()
    turned[...] = jnp.concatenate([half_down[0], half_down[1]], axis=0).T
    down_all[z, y, own_half, :] = turned[own_half, :]
    within(1, 1)
    for gather in narrow:
        gather.own()
    for gather in wide:
        gather.line()
    weight.pass_on()
    _, before_z = fold_z()
    entering = followed_by(followed_by(before_z, before_y), before_core)[0]
    entering = [state.astype(bf16) for state in entering]
    local["g"].wait()

    sent = []
    for step in (2, 1, 3, 0):
        quarter = lax.rem(x + step, 4)
        lines = pl.ds(pl.multiple_of(256 * quarter, 256), 256)
        for h in range(2):
            heads = slice(128 * h, 128 * (h + 1))
            carried = jnp.dot(q[lines, heads], entering[h], preferred_element_type=f32)
            value = retention[h, lines, :] + carried * decayed[h, lines, :]
            centered = value - jnp.mean(value, axis=-1, keepdims=True)
            variance = jnp.mean(centered * centered, axis=-1, keepdims=True)
            normed = centered * lax.rsqrt(variance + EPSILON) * norm_gain[h : h + 1, :]
            retained[quarter, :, heads] = (
                jax.nn.silu(g[lines, heads].astype(f32)) * normed
            ).astype(bf16)
        if step:
            sent.append(links.send(retained.at[quarter], regrouped.at[x], **{X: quarter}))
    for gather in narrow:
        gather.pass_on()
    weight.end()
    local["resid"].wait()
    for copy in weight.across:
        copy.wait_recv()
    for copy in sent:
        copy.wait_recv()

    for j in range(8):
        lanes = slice(256 * j, 256 * (j + 1))
        total = jnp.zeros((256, 256), f32)
        for step in range(4):
            owner = lax.rem(x + step, 4)
            block = regrouped[owner] if step else retained[x]
            part = jnp.dot(block, out_all[owner, :, lanes], preferred_element_type=f32)
            total = total + part.astype(bf16).astype(f32)
        partial[0, :, lanes] = total.astype(bf16)

    @pl.loop(0, 16)
    def _(step):
        lines = pl.ds(pl.multiple_of(16 * step, 16), 16)
        mid = (
            middle[lines, :].astype(f32) + rms_norm(partial[0, lines, :], mix_gain[...])
        ).astype(bf16)
        middle[lines, :] = mid
        rows[x, lines, :] = rms_norm(mid, in_gain[...]).astype(bf16)

    top, bottom = pl.ds(0, 128), pl.ds(128, 128)
    up_top = links.send(rows.at[x, top], rows.at[x, top], **{X: x_up})
    down_bottom = links.send(rows.at[x, bottom], rows.at[x, bottom], **{X: x_down})
    for gather in wide:
        gather.pass_line()
    for gather in narrow:
        gather.line()
    for gather in wide:
        gather.end_line()
    up_top.wait_recv()
    far_top = links.send(rows.at[x_down, top], rows.at[x_down, top], **{X: x_up})
    down_bottom.wait_recv()
    far_bottom = links.send(rows.at[x_up, bottom], rows.at[x_up, bottom], **{X: x_down})
    up_bottom = links.send(rows.at[x, bottom], rows.at[x, bottom], **{X: x_up})
    down_top = links.send(rows.at[x, top], rows.at[x, top], **{X: x_down})
    for gather in wide:
        gather.arrive()

    def gate_up(owner, slot):
        block = rows[owner]
        for j in range(11):
            lanes = slice(128 * j, 128 * (j + 1))
            weights = jnp.concatenate(
                [
                    gate_all[:, :, :, :, lanes].reshape(2048, 128),
                    up_all[:, :, :, :, lanes].reshape(2048, 128),
                ],
                axis=1,
            )
            both = jnp.dot(block, weights, preferred_element_type=f32)
            hidden[slot, :, lanes] = (jax.nn.silu(both[:, :128]) * both[:, 128:]).astype(bf16)

    def down(slot, to, lines=pl.ds(0, 256), extra=None):
        block = hidden[slot, lines, :]
        for j in range(8):
            weights = jnp.concatenate(
                [down_all[j // 2, 2 * j % 4], down_all[j // 2, 2 * j % 4 + 1]], axis=1
            )
            part = jnp.dot(block, weights, preferred_element_type=f32)
            lanes = slice(256 * j, 256 * (j + 1))
            if extra is not None:
                part = part + relay[extra, :, lanes].astype(f32)
            partial[to, lines, lanes] = part.astype(bf16)

    gate_up(x, 0)
    for gather in narrow:
        gather.pass_line()
    far_top.wait_recv()
    far_bottom.wait_recv()
    gate_up(x_far, 1)
    for gather in narrow:
        gather.end_line()
    for gather in narrow:
        gather.arrive()
    down(1, 1)
    relay_up = links.send(partial.at[1, top], relay.at[0], **{X: x_up})
    relay_down = links.send(partial.at[1, bottom], relay.at[1], **{X: x_down})
    down(0, 0)
    up_bottom.wait_recv()
    down_top.wait_recv()
    gate_up(x_up, 0)
    down(0, 2, bottom)
    last = [links.send(partial.at[2, bottom], final.at[0, bottom], **{X: x_up})]
    gate_up(x_down, 1)
    down(1, 3, top)
    last.append(links.send(partial.at[3, top], final.at[1, top], **{X: x_down}))
    relay_up.wait_recv()
    down(0, 2, top, 0)
    last.append(links.send(partial.at[2, top], final.at[0, top], **{X: x_up}))
    relay_down.wait_recv()
    down(1, 3, bottom, 1)
    last.append(links.send(partial.at[3, bottom], final.at[1, bottom], **{X: x_down}))
    for copy in last:
        copy.wait_recv()

    @pl.loop(0, 16)
    def _(step):
        lines = pl.ds(pl.multiple_of(16 * step, 16), 16)
        branch = (
            partial[0, lines, :].astype(f32)
            + final[0, lines, :].astype(f32)
            + final[1, lines, :].astype(f32)
        ).astype(bf16)
        out[lines, :] = (middle[lines, :].astype(f32) + rms_norm(branch, out_gain[...])).astype(bf16)

    links.finish()


def per_device(
    queries, keys, values, gates, log_decay, norm_gain, out_weight, resid, post_mix_gain, pre_ffn_gain,
    w_gate, w_up, w_down, post_ffn_gain,
):
    hbm, vmem = pl.BlockSpec(memory_space=pl.ANY), pl.BlockSpec(memory_space=pltpu.VMEM)
    f32, bf16 = jnp.float32, jnp.bfloat16
    return pl.pallas_call(
        layer_kernel,
        out_shape=jax.ShapeDtypeStruct((256, 2048), bf16),
        in_specs=[hbm, hbm, hbm, hbm, vmem, vmem, hbm, hbm, vmem, vmem, hbm, hbm, hbm, vmem],
        out_specs=vmem,
        scratch_shapes=[
            pltpu.VMEM((4, 4, 2, 64, 1408), bf16),
            pltpu.VMEM((4, 4, 2, 64, 1408), bf16),
            pltpu.VMEM((4, 4, 1408, 128), bf16),
            pltpu.VMEM((4, 256, 2048), bf16),
            pltpu.VMEM((2, 256, 1408), bf16),
            pltpu.VMEM((4, 256, 2048), bf16),
            pltpu.VMEM((2, 128, 2048), bf16),
            pltpu.VMEM((2, 256, 2048), bf16),
            pltpu.VMEM((2, 64, 1408), bf16),
            pltpu.VMEM((1408, 128), bf16),
            pltpu.VMEM((1024, 256), bf16),
            pltpu.VMEM((1024, 256), bf16),
            pltpu.VMEM((1024, 256), bf16),
            pltpu.VMEM((1024, 256), bf16),
            pltpu.VMEM((2, 1024, 128), f32),
            pltpu.VMEM((2, 1024, 128), f32),
            pltpu.VMEM((2, 272, 128), bf16),
            pltpu.VMEM((4, 272, 128), bf16),
            pltpu.VMEM((4, 272, 128), bf16),
            pltpu.VMEM((4, 256, 256), bf16),
            pltpu.VMEM((4, 256, 256), bf16),
            pltpu.VMEM((4, 256, 2048), bf16),
            pltpu.VMEM((256, 2048), bf16),
            pltpu.SemaphoreType.DMA((9,)),
            pltpu.SemaphoreType.DMA((96,)),
            pltpu.SemaphoreType.DMA((96,)),
        ],
        compiler_params=pltpu.CompilerParams(
            collective_id=0, has_side_effects=True, vmem_limit_bytes=60 * 2**20
        ),
        name="layer",
    )(
        queries, keys, values, gates, log_decay.T, norm_gain, out_weight, resid, post_mix_gain[None],
        pre_ffn_gain[None], w_gate, w_up, w_down.T, post_ffn_gain[None],
    )


def solution(mesh):
    split = Mesh(mesh.devices.reshape(4, 4, 2, mesh.shape["tp"]), ("sp_0", "sp_1", "sp_2", "tp"))
    placed = (
        P(SP, "tp"),
        P(SP, "tp"),
        P(SP, "tp"),
        P(SP, "tp"),
        P(SP, "tp"),
        P("tp", None),
        P("tp", None),
        P(SP_TP, None),
        P(),
        P(),
        P(SP, "tp"),
        P(SP, "tp"),
        P("tp", SP),
        P(),
    )
    return jax.shard_map(
        per_device, mesh=split, in_specs=placed, out_specs=P(SP_TP, None), check_vma=False
    )
```

```python
import jax
import jax.numpy as jnp
from jax import lax
from jax.experimental import pallas as pl
from jax.experimental.pallas import tpu as pltpu
from jax.sharding import Mesh
from jax.sharding import PartitionSpec as P

BLOCK = 512
SP = ("sp_0", "sp_1", "sp_2")
SP_TP = ("sp_0", "sp_1", "sp_2", "tp")


EPSILON = 1e-06
MESH_ID = pl.DeviceIdType.MESH
Z, Y, C, X = SP_TP


class Links:
    def __init__(self, send_sem, recv_sem):
        self.send_sem, self.recv_sem, self.copies = send_sem, recv_sem, []

    def send(self, src, dst, **where):
        at = len(self.copies)
        copy = pltpu.make_async_remote_copy(
            src_ref=src,
            dst_ref=dst,
            send_sem=self.send_sem.at[at],
            recv_sem=self.recv_sem.at[at],
            device_id={axis: index for axis, index in where.items()},
            device_id_type=MESH_ID,
        )
        copy.start()
        self.copies.append(copy)
        return copy

    def finish(self):
        for copy in self.copies:
            copy.wait_send()


class PlaneGather:
    def __init__(self, links, at, first, second, here, core):
        self.links, self.at, self.first, self.second, self.core = links, at, first, second, core
        self.i, self.j = here
        self.i_up, self.i_down = lax.rem(self.i + 1, 4), lax.rem(self.i + 3, 4)
        self.j_up, self.j_down = lax.rem(self.j + 1, 4), lax.rem(self.j + 3, 4)
        self.across = []

    def both_ways(self, axis, up, down, block):
        return (
            self.links.send(block, block, **{axis: up}),
            self.links.send(block, block, **{axis: down}),
        )

    def own(self):
        self.up, self.down = self.both_ways(
            self.first, self.i_up, self.i_down, self.at(self.i, self.j)
        )

    def pass_on(self):
        self.up.wait_recv()
        block = self.at(self.i_down, self.j, part=0)
        up = self.links.send(block, block, **{self.first: self.i_up})
        self.down.wait_recv()
        block = self.at(self.i_up, self.j, part=1)
        self.up, self.down = up, self.links.send(block, block, **{self.first: self.i_down})

    def give(self, j):
        block = self.at(pl.ds(0, 4), j)
        self.across.append(self.links.send(block, block, **{C: 1 - self.core}))

    def line(self):
        self.up.wait_recv()
        self.down.wait_recv()
        self.up, self.down = self.both_ways(
            self.second, self.j_up, self.j_down, self.at(pl.ds(0, 4), self.j)
        )

    def pass_line(self):
        self.up.wait_recv()
        up = self.one_way(self.j_up, (0, 1), self.j_down)
        self.down.wait_recv()
        self.passed = (up, self.one_way(self.j_down, (2, 3), self.j_up))
        self.give(self.j_down)
        self.give(self.j_up)

    def one_way(self, target, items, j):
        blocks = [self.at(pl.ds(i, 1), j) for i in items]
        return [self.links.send(block, block, **{self.second: target}) for block in blocks]

    def end_line(self):
        far = lax.rem(self.j + 2, 4)
        for at in range(2):
            for copies, start in zip(self.passed, (0, 2)):
                copies[at].wait_recv()
                block = self.at(pl.ds(start + at, 1), far)
                self.across.append(self.links.send(block, block, **{C: 1 - self.core}))

    def arrive(self):
        for copy in self.across:
            copy.wait_recv()


class Ring:
    def __init__(self, links, where, own, passed):
        self.links, self.where, self.own, self.passed = links, where, own, passed

    def both_ways(self, pairs, after=None):
        copies = []
        for at, (step, (src, dst)) in enumerate(zip((1, 3), pairs)):
            if after:
                after[at].wait_recv()
            copies.append(self.links.send(src, dst, **self.where(step)))
        return copies

    def start(self):
        self.copies = self.both_ways(self.own)

    def pass_on(self):
        self.copies = self.both_ways(self.passed, self.copies)

    def finish(self):
        for copy in self.copies:
            copy.wait_recv()


def rms_norm(values_in, gain_vec):
    widened = values_in.astype(jnp.float32)
    return (
        widened
        * lax.rsqrt(jnp.mean(widened * widened, axis=-1, keepdims=True) + EPSILON)
        * gain_vec
    )


def over_lanes(scalar):
    return jnp.broadcast_to(scalar, (1, 128))


def write_state(ref, state, decay):
    ref[pl.ds(0, 128), :] = state.astype(jnp.bfloat16)
    row = lax.broadcasted_iota(jnp.int32, (16, 128), 0)
    large = decay.astype(jnp.bfloat16).astype(jnp.float32)
    ref[pl.ds(128, 16), :] = jnp.where(row == 0, large, decay - large).astype(jnp.bfloat16)


def read_state(ref):
    both = ref[pl.ds(128, 16), :].astype(jnp.float32)
    return ref[pl.ds(0, 128), :].astype(jnp.float32), both[0:1] + both[1:2]


def followed_by(earlier, later):
    return later[1] * earlier[0] + later[0], later[1] * earlier[1]


def chosen(which, a, b):
    return jax.tree.map(lambda p, q: jnp.where(which, p, q), a, b)


def layer_kernel(
    queries, keys, values, gates, log_decay, norm_gain, out_weight, resid, mix_gain, in_gain,
    w_gate, w_up, w_down, out_gain, out,
    gate_all, up_all, down_all, rows, hidden, partial, relay, final, half_down, turned,
    q, k, v, g, retention, decayed, state_c, state_y, state_z, state_in, retained, regrouped, passing, out_all, middle, result,
    local_sem, out_sem, send_sem, recv_sem,
):
    f32, bf16 = jnp.float32, jnp.bfloat16
    z, y, c, x = (lax.axis_index(axis) for axis in SP_TP)
    other, x_up, x_down, x_far = 1 - c, lax.rem(x + 1, 4), lax.rem(x + 3, 4), lax.rem(x + 2, 4)
    own_half = pl.ds(pl.multiple_of(704 * c, 64), 704)
    names = ("k", "v", "gate", "up", "q", "down", "weight", "g", "resid")
    moves = (
        (keys, k), (values, v), (w_gate, gate_all.at[z, y, c]), (w_up, up_all.at[z, y, c]), (queries, q),
        (w_down, half_down.at[c]), (out_weight, out_all.at[0]), (gates, g), (resid, middle),
    )
    local = {
        name: pltpu.make_async_copy(src, dst, local_sem.at[at])
        for at, (name, (src, dst)) in enumerate(zip(names, moves))
    }
    for copy in local.values():
        copy.start()

    barrier = pltpu.get_barrier_semaphore()
    near = [{C: other}]
    for axis, index in ((X, x), (Y, y), (Z, z)):
        near += [{axis: lax.rem(index + step, 4)} for step in (1, 2, 3)]
    for where in near:
        pl.semaphore_signal(barrier, inc=1, device_id=where, device_id_type=MESH_ID)

    links = Links(send_sem, recv_sem)

    def gate_at(i, j, part=None):
        lines = pl.ds(0, 64) if part is None else pl.ds(32 * part, 32)
        return gate_all.at[j, i, c, lines]

    def up_at(i, j, part=None):
        lines = pl.ds(0, 64) if part is None else pl.ds(32 * part, 32)
        return up_all.at[i, j, c, lines]

    def down_lines(start, part):
        first, length = (start, 352) if part is None else (start + 176 * part, 176)
        return pl.ds(pl.multiple_of(704 * c + first, 16), length)

    wide = (
        PlaneGather(links, gate_at, Y, Z, (y, z), c),
        PlaneGather(links, up_at, Z, Y, (z, y), c),
    )
    narrow = (
        PlaneGather(
            links, lambda i, j, part=None: down_all.at[j, i, down_lines(0, part)], Y, Z, (y, z), c
        ),
        PlaneGather(
            links, lambda i, j, part=None: down_all.at[i, j, down_lines(352, part)], Z, Y, (z, y), c
        ),
    )

    along = (1 - c) * y + c * z

    def part_rows(i, part=None):
        first, length = (0, 32) if part is None else (16 * part, 16)
        return pl.ds(pl.multiple_of(128 * c + 32 * i + first, 16), length)

    def on_line(step):
        return {Y: lax.rem(y + (1 - c) * step, 4), Z: lax.rem(z + c * step, 4)}

    weight_x = Ring(
        links,
        lambda step: {X: lax.rem(x + step, 4)},
        (
            (out_all.at[0, part_rows(along)], out_all.at[2, part_rows(along)]),
            (out_all.at[0, part_rows(along)], out_all.at[1, part_rows(along)]),
        ),
        (
            (out_all.at[2, part_rows(along, 0)], out_all.at[3, part_rows(along, 0)]),
            (out_all.at[1, part_rows(along, 1)], out_all.at[3, part_rows(along, 1)]),
        ),
    )

    def weight_ring(slots):
        own, low, high = (
            out_all.at[slots, part_rows(along)],
            out_all.at[slots, part_rows(lax.rem(along + 3, 4), 0)],
            out_all.at[slots, part_rows(lax.rem(along + 1, 4), 1)],
        )
        return Ring(links, on_line, ((own, own), (own, own)), ((low, low), (high, high)))

    weight_near, weight_far = weight_ring(pl.ds(1, 2)), weight_ring(pl.ds(3, 1))
    half_rows = pl.ds(pl.multiple_of(128 * c, 128), 128)

    scale = 128 ** (-0.5)
    at_row = lax.broadcasted_iota(jnp.int32, (BLOCK, BLOCK), 0)
    at_col = lax.broadcasted_iota(jnp.int32, (BLOCK, BLOCK), 1)
    upto = jnp.where(at_row <= at_col, 1.0, 0.0).astype(f32)
    cum_rows, cum_cols = [], []
    for b in range(2):
        logs = jnp.concatenate(
            [log_decay[:, BLOCK * b : BLOCK * (b + 1)], jnp.zeros((6, BLOCK), f32)], axis=0
        )
        cum = jnp.dot(logs, upto, precision=lax.Precision.HIGHEST, preferred_element_type=f32)
        cum_rows.append(cum)
        cum_cols.append(cum.T)
    ends = [[cum_rows[b][h : h + 1, BLOCK - 1 : BLOCK] for b in range(2)] for h in range(2)]
    local["k"].wait()
    local["v"].wait()
    first_state, span = [], []
    for h in range(2):
        heads = slice(128 * h, 128 * (h + 1))
        added = []
        for b in range(2):
            lines = slice(BLOCK * b, BLOCK * (b + 1))
            to_end = jnp.exp(ends[h][b] - cum_cols[b][:, h : h + 1]) * scale
            scaled = (k[lines, heads].astype(f32) * to_end).astype(bf16)
            added.append(
                lax.dot_general(
                    scaled, v[lines, heads], (((0,), (0,)), ((), ())), preferred_element_type=f32
                )
            )
        first_state.append(added[0])
        span.append(
            (
                jnp.exp(over_lanes(ends[h][1])) * added[0] + added[1],
                jnp.exp(over_lanes(ends[h][0] + ends[h][1])),
            )
        )
        write_state(state_c.at[0, h], *span[h])
    pl.semaphore_wait(barrier, len(near))
    pair = links.send(state_c.at[0], state_c.at[1], **{C: other})
    local["up"].wait()
    wide[1].own()
    local["weight"].wait()
    weight_x.start()
    local["down"].wait()
    swap = links.send(half_down.at[c], half_down.at[c], **{C: other})
    local["gate"].wait()

    def within(h, b):
        heads, lines = slice(128 * h, 128 * (h + 1)), slice(BLOCK * b, BLOCK * (b + 1))
        col, row = cum_cols[b][:, h : h + 1], cum_rows[b][h : h + 1]
        products = lax.dot_general(
            q[lines, heads], k[lines, heads], (((1,), (1,)), ((), ())), preferred_element_type=f32
        )
        factor = jnp.where(at_row >= at_col, jnp.exp(jnp.minimum(col - row, 0.0)), 0.0)
        scores = (products * scale * factor).astype(bf16)
        result = jnp.dot(scores, v[lines, heads], preferred_element_type=f32)
        if b == 1:
            result = result + jnp.exp(col) * jnp.dot(
                q[lines, heads], first_state[h].astype(bf16), preferred_element_type=f32
            )
            col = col + ends[h][0]
        retention[h, lines, :] = result
        decayed[h, lines, :] = jnp.broadcast_to(jnp.exp(col), (BLOCK, 128))

    nothing = (jnp.zeros((128, 128), f32), jnp.ones((1, 128), f32))

    def among(slots, axis, index):
        sent = [
            links.send(slots.at[index], slots.at[index], **{axis: lax.rem(index + step, 4)})
            for step in (2, 1, 3)
        ]

        def fold():
            for copy in sent:
                copy.wait_recv()
            total, before = nothing, nothing
            for at in range(4):
                total = followed_by(total, read_state(slots.at[at]))
                before = chosen(at < index, total, before)
            return total, before

        return fold

    local["q"].wait()
    within(0, 0)
    pair.wait_recv()
    partner = [read_state(state_c.at[1, h]) for h in range(2)]
    first = c == 0
    chip = [
        followed_by(chosen(first, span[h], partner[h]), chosen(first, partner[h], span[h]))
        for h in range(2)
    ]
    write_state(state_y.at[y], *chosen(first, chip[0], chip[1]))
    fold_y = among(state_y, Y, y)
    wide[0].own()
    within(0, 1)
    within(1, 0)
    line, before_y = fold_y()
    write_state(state_z.at[z], *line)
    fold_z = among(state_z, Z, z)
    swap.wait_recv()
    turned[...] = jnp.concatenate([half_down[0], half_down[1]], axis=0).T
    down_all[z, y, own_half, :] = turned[own_half, :]
    within(1, 1)
    weight_x.pass_on()
    weight_near.start()
    _, before_z = fold_z()
    state_in[c] = followed_by(before_z, before_y)[0]
    both_heads = links.send(state_in.at[c], state_in.at[c], **{C: other})
    weight_x.finish()
    weight_far.start()
    for gather in (wide[1], wide[0]):
        gather.pass_on()
    for gather in narrow:
        gather.own()
    local["g"].wait()
    both_heads.wait_recv()
    entering = [
        jnp.where(first, state_in[h], partner[h][1] * state_in[h] + partner[h][0]).astype(bf16)
        for h in range(2)
    ]

    top, bottom = pl.ds(0, 128), pl.ds(128, 128)
    sent = []
    for step in (2, 1, 3, 0):
        quarter = lax.rem(x + step, 4)
        lines = pl.ds(pl.multiple_of(256 * quarter, 256), 256)
        for h in range(2):
            heads = slice(128 * h, 128 * (h + 1))
            carried = jnp.dot(q[lines, heads], entering[h], preferred_element_type=f32)
            value = retention[h, lines, :] + carried * decayed[h, lines, :]
            centered = value - jnp.mean(value, axis=-1, keepdims=True)
            variance = jnp.mean(centered * centered, axis=-1, keepdims=True)
            normed = centered * lax.rsqrt(variance + EPSILON) * norm_gain[h : h + 1, :]
            retained[step, :, heads] = (jax.nn.silu(g[lines, heads].astype(f32)) * normed).astype(
                bf16
            )
        if step == 2:
            sent.append(links.send(retained.at[2, top], regrouped.at[3, top], **{X: x_far}))
            to_pass = links.send(retained.at[2, bottom], passing, **{X: x_down})
        elif step:
            slot = 2 if step == 1 else 1
            sent.append(links.send(retained.at[step], regrouped.at[slot], **{X: quarter}))
    weight_near.pass_on()
    weight_far.pass_on()
    for gather in narrow:
        gather.pass_on()
    for gather in (wide[1], wide[0]):
        gather.line()
    to_pass.wait_recv()
    sent.append(links.send(passing, regrouped.at[3, bottom], **{X: x_down}))
    weight_near.finish()
    near_half = out_all.at[pl.ds(1, 2), half_rows]
    shared = [links.send(near_half, near_half, **{C: other})]
    weight_far.finish()
    far_half = out_all.at[3, half_rows]
    shared.append(links.send(far_half, far_half, **{C: other}))
    local["resid"].wait()
    for copy in sent:
        copy.wait_recv()
    for copy in shared:
        copy.wait_recv()

    for j in range(8):
        lanes = slice(256 * j, 256 * (j + 1))
        total = jnp.zeros((256, 256), f32)
        for slot in range(4):
            block = regrouped[slot] if slot else retained[0]
            part = jnp.dot(block, out_all[slot, :, lanes], preferred_element_type=f32)
            total = total + part.astype(bf16).astype(f32)
        partial[0, :, lanes] = total.astype(bf16)

    piece = [pl.ds(64 * at, 64) for at in range(4)]
    to_up, to_down = [], []
    for at in range(2):

        @pl.loop(0, 4)
        def _(step):
            for start in (64 * at, 64 * at + 128):
                lines = pl.ds(pl.multiple_of(start + 16 * step, 16), 16)
                mid = (
                    middle[lines, :].astype(f32) + rms_norm(partial[0, lines, :], mix_gain[...])
                ).astype(bf16)
                middle[lines, :] = mid
                rows[x, lines, :] = rms_norm(mid, in_gain[...]).astype(bf16)

        for to, target, lines in ((to_up, x_up, piece[at]), (to_down, x_down, piece[2 + at])):
            to.append(links.send(rows.at[x, lines], rows.at[x, lines], **{X: target}))
    far, nearby = [], []
    for gather in narrow:
        gather.line()
    for gather in (*wide, *narrow):
        gather.give(gather.j)
    forward = ((to_up, x_up, x_down, 0), (to_down, x_down, x_up, 2))
    for at in range(2):
        for to, target, source, start in forward:
            to[at].wait_recv()
            lines = piece[start + at]
            far.append(links.send(rows.at[source, lines], rows.at[source, lines], **{X: target}))
        if at == 0:
            for gather in wide:
                gather.pass_line()
    for lines, target in ((bottom, x_up), (top, x_down)):
        nearby.append(links.send(rows.at[x, lines], rows.at[x, lines], **{X: target}))
    for gather in narrow:
        gather.pass_line()
    for gather in wide:
        gather.end_line()
    for gather in wide:
        gather.arrive()

    def gate_up(owner, slot):
        block = rows[owner]
        for j in range(11):
            lanes = slice(128 * j, 128 * (j + 1))
            weights = jnp.concatenate(
                [
                    gate_all[:, :, :, :, lanes].reshape(2048, 128),
                    up_all[:, :, :, :, lanes].reshape(2048, 128),
                ],
                axis=1,
            )
            both = jnp.dot(block, weights, preferred_element_type=f32)
            hidden[slot, :, lanes] = (jax.nn.silu(both[:, :128]) * both[:, 128:]).astype(bf16)

    def down(slot, to, lines=pl.ds(0, 256), extra=None):
        block = hidden[slot, lines, :]
        for j in range(8):
            weights = jnp.concatenate(
                [down_all[j // 2, 2 * j % 4], down_all[j // 2, 2 * j % 4 + 1]], axis=1
            )
            part = jnp.dot(block, weights, preferred_element_type=f32)
            lanes = slice(256 * j, 256 * (j + 1))
            if extra is not None:
                part = part + relay[extra, :, lanes].astype(f32)
            partial[to, lines, lanes] = part.astype(bf16)

    for copy in far:
        copy.wait_recv()
    gate_up(x_far, 2)
    for gather in narrow:
        gather.end_line()
    for gather in narrow:
        gather.arrive()
    down(2, 1)
    relay_up = links.send(partial.at[1, top], relay.at[0], **{X: x_up})
    relay_down = links.send(partial.at[1, bottom], relay.at[1], **{X: x_down})
    for copy in nearby:
        copy.wait_recv()
    gate_up(x_up, 0)
    down(0, 2, bottom)
    last = [links.send(partial.at[2, bottom], final.at[0, bottom], **{X: x_up})]
    gate_up(x_down, 1)
    down(1, 3, top)
    last.append(links.send(partial.at[3, top], final.at[1, top], **{X: x_down}))
    gate_up(x, 2)
    relay_up.wait_recv()
    down(0, 2, top, 0)
    for at in range(2):
        last.append(links.send(partial.at[2, piece[at]], final.at[0, piece[at]], **{X: x_up}))
    relay_down.wait_recv()
    down(1, 3, bottom, 1)
    for at in range(2):
        last.append(links.send(partial.at[3, piece[2 + at]], final.at[1, piece[2 + at]], **{X: x_down}))
    down(2, 0)
    written = []
    last[0].wait_recv()
    last[1].wait_recv()
    for at in range(2):
        last[2 + at].wait_recv()
        last[4 + at].wait_recv()

        @pl.loop(0, 4)
        def _(step):
            for start in (64 * at, 64 * at + 128):
                lines = pl.ds(pl.multiple_of(start + 16 * step, 16), 16)
                branch = (
                    partial[0, lines, :].astype(f32)
                    + final[0, lines, :].astype(f32)
                    + final[1, lines, :].astype(f32)
                ).astype(bf16)
                result[lines, :] = (
                    middle[lines, :].astype(f32) + rms_norm(branch, out_gain[...])
                ).astype(bf16)

        for lines in (piece[at], piece[2 + at]):
            written.append(pltpu.make_async_copy(result.at[lines], out.at[lines], out_sem.at[len(written)]))
            written[-1].start()
    for copy in written:
        copy.wait()
    links.finish()


def per_device(
    queries, keys, values, gates, log_decay, norm_gain, out_weight, resid, post_mix_gain, pre_ffn_gain,
    w_gate, w_up, w_down, post_ffn_gain,
):
    hbm, vmem = pl.BlockSpec(memory_space=pl.ANY), pl.BlockSpec(memory_space=pltpu.VMEM)
    f32, bf16 = jnp.float32, jnp.bfloat16
    return pl.pallas_call(
        layer_kernel,
        out_shape=jax.ShapeDtypeStruct((256, 2048), bf16),
        in_specs=[hbm, hbm, hbm, hbm, vmem, vmem, hbm, hbm, vmem, vmem, hbm, hbm, hbm, vmem],
        out_specs=hbm,
        scratch_shapes=[
            pltpu.VMEM((4, 4, 2, 64, 1408), bf16),
            pltpu.VMEM((4, 4, 2, 64, 1408), bf16),
            pltpu.VMEM((4, 4, 1408, 128), bf16),
            pltpu.VMEM((4, 256, 2048), bf16),
            pltpu.VMEM((3, 256, 1408), bf16),
            pltpu.VMEM((4, 256, 2048), bf16),
            pltpu.VMEM((2, 128, 2048), bf16),
            pltpu.VMEM((2, 256, 2048), bf16),
            pltpu.VMEM((2, 64, 1408), bf16),
            pltpu.VMEM((1408, 128), bf16),
            pltpu.VMEM((1024, 256), bf16),
            pltpu.VMEM((1024, 256), bf16),
            pltpu.VMEM((1024, 256), bf16),
            pltpu.VMEM((1024, 256), bf16),
            pltpu.VMEM((2, 1024, 128), f32),
            pltpu.VMEM((2, 1024, 128), f32),
            pltpu.VMEM((2, 2, 144, 128), bf16),
            pltpu.VMEM((4, 144, 128), bf16),
            pltpu.VMEM((4, 144, 128), bf16),
            pltpu.VMEM((2, 128, 128), f32),
            pltpu.VMEM((4, 256, 256), bf16),
            pltpu.VMEM((4, 256, 256), bf16),
            pltpu.VMEM((128, 256), bf16),
            pltpu.VMEM((4, 256, 2048), bf16),
            pltpu.VMEM((256, 2048), bf16),
            pltpu.VMEM((256, 2048), bf16),
            pltpu.SemaphoreType.DMA((9,)),
            pltpu.SemaphoreType.DMA((4,)),
            pltpu.SemaphoreType.DMA((136,)),
            pltpu.SemaphoreType.DMA((136,)),
        ],
        compiler_params=pltpu.CompilerParams(
            collective_id=0, has_side_effects=True, vmem_limit_bytes=60 * 2**20
        ),
        name="layer",
    )(
        queries, keys, values, gates, log_decay.T, norm_gain, out_weight, resid, post_mix_gain[None],
        pre_ffn_gain[None], w_gate, w_up, w_down.T, post_ffn_gain[None],
    )


def solution(mesh):
    split = Mesh(mesh.devices.reshape(4, 4, 2, mesh.shape["tp"]), ("sp_0", "sp_1", "sp_2", "tp"))
    placed = (
        P(SP, "tp"),
        P(SP, "tp"),
        P(SP, "tp"),
        P(SP, "tp"),
        P(SP, "tp"),
        P("tp", None),
        P("tp", None),
        P(SP_TP, None),
        P(),
        P(),
        P(SP, "tp"),
        P(SP, "tp"),
        P("tp", SP),
        P(),
    )
    return jax.shard_map(
        per_device, mesh=split, in_specs=placed, out_specs=P(SP_TP, None), check_vma=False
    )
```

```python
import jax
import jax.numpy as jnp
from jax import lax
from jax.experimental import pallas as pl
from jax.experimental.pallas import tpu as pltpu
from jax.sharding import Mesh
from jax.sharding import PartitionSpec as P

BLOCK = 512
SP = ("sp_0", "sp_1", "sp_2")
SP_TP = ("sp_0", "sp_1", "sp_2", "tp")


EPSILON = 1e-06
MESH_ID = pl.DeviceIdType.MESH
SENDS, ARRIVALS = 40, 48
Z, Y, C, X = SP_TP


class Arrival:
    def __init__(self, links, at):
        self.links, self.at = links, at

    def wait(self, as_large):
        pltpu.make_async_remote_copy(
            src_ref=as_large,
            dst_ref=as_large,
            send_sem=self.links.send_sem.at[0],
            recv_sem=self.links.recv_sem.at[self.at],
            device_id={X: lax.rem(lax.axis_index(X) + 1, 4)},
            device_id_type=MESH_ID,
        ).wait_recv()


class Links:
    def __init__(self, send_sem, recv_sem):
        self.send_sem, self.recv_sem, self.copies, self.arrivals = send_sem, recv_sem, [], 0

    def arrival(self):
        self.arrivals += 1
        return Arrival(self, self.arrivals - 1)

    def send(self, arrival, src, dst, **where):
        at = len(self.copies)
        if at >= SENDS:
            self.copies[at - SENDS].wait_send()
        copy = pltpu.make_async_remote_copy(
            src_ref=src,
            dst_ref=dst,
            send_sem=self.send_sem.at[at % SENDS],
            recv_sem=self.recv_sem.at[arrival.at],
            device_id={axis: index for axis, index in where.items()},
            device_id_type=MESH_ID,
        )
        copy.start()
        self.copies.append(copy)

    def finish(self):
        for copy in self.copies[-SENDS:]:
            copy.wait_send()
        assert self.arrivals <= ARRIVALS


class PlaneGather:
    def __init__(self, links, at, first, second, here, core):
        self.links, self.at, self.first, self.second, self.core = links, at, first, second, core
        self.i, self.j = here
        self.i_up, self.i_down = lax.rem(self.i + 1, 4), lax.rem(self.i + 3, 4)
        self.j_up, self.j_down = lax.rem(self.j + 1, 4), lax.rem(self.j + 3, 4)
        self.across = links.arrival()

    def both_ways(self, axis, up, down, block_up, block_down):
        arrival = self.links.arrival()
        self.links.send(arrival, block_up, block_up, **{axis: up})
        self.links.send(arrival, block_down, block_down, **{axis: down})
        return arrival

    def own(self):
        block = self.at(self.i, self.j)
        self.came = self.both_ways(self.first, self.i_up, self.i_down, block, block)

    def pass_on(self):
        self.came.wait(self.at(pl.ds(0, 2), self.j))
        self.came = self.both_ways(
            self.first,
            self.i_up,
            self.i_down,
            self.at(self.i_down, self.j, part=0),
            self.at(self.i_up, self.j, part=1),
        )

    def give(self, j, items=pl.ds(0, 4)):
        block = self.at(items, j)
        self.links.send(self.across, block, block, **{C: 1 - self.core})

    def line(self):
        self.came.wait(self.at(self.i, self.j))
        block = self.at(pl.ds(0, 4), self.j)
        self.came = self.both_ways(self.second, self.j_up, self.j_down, block, block)

    def pass_line(self):
        self.came.wait(self.at(pl.ds(0, 4), pl.ds(0, 2)))
        self.passed = [
            self.both_ways(
                self.second,
                self.j_up,
                self.j_down,
                self.at(pl.ds(at, 1), self.j_down),
                self.at(pl.ds(2 + at, 1), self.j_up),
            )
            for at in range(2)
        ]
        self.give(self.j_down)
        self.give(self.j_up)

    def end_line(self):
        far = lax.rem(self.j + 2, 4)
        for at, arrival in enumerate(self.passed):
            arrival.wait(self.at(pl.ds(0, 2), far))
            for start in (0, 2):
                self.give(far, pl.ds(start + at, 1))

    def arrive(self):
        self.across.wait(self.at(pl.ds(0, 4), pl.ds(0, 4)))


class Ring:
    def __init__(self, links, where, own, passed, as_large):
        self.links, self.where, self.own, self.passed, self.as_large = links, where, own, passed, as_large

    def both_ways(self, pairs):
        self.came = self.links.arrival()
        for step, (src, dst) in zip((1, 3), pairs):
            self.links.send(self.came, src, dst, **self.where(step))

    def start(self):
        self.both_ways(self.own)

    def pass_on(self):
        self.came.wait(self.as_large[0])
        self.both_ways(self.passed)

    def finish(self):
        self.came.wait(self.as_large[1])


def rms_norm(values_in, gain_vec):
    widened = values_in.astype(jnp.float32)
    return (
        widened
        * lax.rsqrt(jnp.mean(widened * widened, axis=-1, keepdims=True) + EPSILON)
        * gain_vec
    )


def over_lanes(scalar):
    return jnp.broadcast_to(scalar, (1, 128))


def write_state(ref, state, decay):
    ref[pl.ds(0, 128), :] = state.astype(jnp.bfloat16)
    row = lax.broadcasted_iota(jnp.int32, (16, 128), 0)
    large = decay.astype(jnp.bfloat16).astype(jnp.float32)
    ref[pl.ds(128, 16), :] = jnp.where(row == 0, large, decay - large).astype(jnp.bfloat16)


def read_state(ref):
    both = ref[pl.ds(128, 16), :].astype(jnp.float32)
    return ref[pl.ds(0, 128), :].astype(jnp.float32), both[0:1] + both[1:2]


def followed_by(earlier, later):
    return later[1] * earlier[0] + later[0], later[1] * earlier[1]


def chosen(which, a, b):
    return jax.tree.map(lambda p, q: jnp.where(which, p, q), a, b)


def layer_kernel(
    queries, keys, values, gates, log_decay, norm_gain, out_weight, resid, mix_gain, in_gain,
    w_gate, w_up, w_down, out_gain, out,
    gate_all, up_all, down_all, rows, hidden, partial, relay, final, half_down, turned,
    q, k, v, g, retention, decayed, state_c, state_y, state_z, state_in, retained, regrouped, passing, out_all, middle, logs_in, gains, norm_in,
    local_sem, send_sem, recv_sem,
):
    f32, bf16 = jnp.float32, jnp.bfloat16
    z, y, c, x = (lax.axis_index(axis) for axis in SP_TP)
    other, x_up, x_down, x_far = 1 - c, lax.rem(x + 1, 4), lax.rem(x + 3, 4), lax.rem(x + 2, 4)
    own_half = pl.ds(pl.multiple_of(704 * c, 64), 704)
    names = ("logs", "k", "v", "gate", "up", "q", "down", "weight", "g", "resid", "mix", "in", "out", "norm")
    moves = (
        (log_decay, logs_in), (keys, k), (values, v), (w_gate, gate_all.at[z, y, c]), (w_up, up_all.at[z, y, c]), (queries, q),
        (w_down, half_down.at[c]), (out_weight, out_all.at[0]), (gates, g), (resid, middle),
        (mix_gain, gains.at[0]), (in_gain, gains.at[1]), (out_gain, gains.at[2]), (norm_gain, norm_in),
    )
    local = {
        name: pltpu.make_async_copy(src, dst, local_sem.at[at])
        for at, (name, (src, dst)) in enumerate(zip(names, moves))
    }
    for copy in local.values():
        copy.start()

    barrier = pltpu.get_barrier_semaphore()
    near = [{C: other}]
    for axis, index in ((X, x), (Y, y), (Z, z)):
        near += [{axis: lax.rem(index + step, 4)} for step in (1, 2, 3)]
    for where in near:
        pl.semaphore_signal(barrier, inc=1, device_id=where, device_id_type=MESH_ID)

    links = Links(send_sem, recv_sem)

    def gate_at(i, j, part=None):
        lines = pl.ds(0, 64) if part is None else pl.ds(32 * part, 32)
        return gate_all.at[j, i, c, lines]

    def up_at(i, j, part=None):
        lines = pl.ds(0, 64) if part is None else pl.ds(32 * part, 32)
        return up_all.at[i, j, c, lines]

    def down_lines(start, part):
        first, length = (start, 352) if part is None else (start + 176 * part, 176)
        return pl.ds(pl.multiple_of(704 * c + first, 16), length)

    wide = (
        PlaneGather(links, gate_at, Y, Z, (y, z), c),
        PlaneGather(links, up_at, Z, Y, (z, y), c),
    )
    narrow = (
        PlaneGather(
            links, lambda i, j, part=None: down_all.at[j, i, down_lines(0, part)], Y, Z, (y, z), c
        ),
        PlaneGather(
            links, lambda i, j, part=None: down_all.at[i, j, down_lines(352, part)], Z, Y, (z, y), c
        ),
    )

    along = (1 - c) * y + c * z

    def part_rows(i, part=None):
        first, length = (0, 32) if part is None else (16 * part, 16)
        return pl.ds(pl.multiple_of(128 * c + 32 * i + first, 16), length)

    def on_line(step):
        return {Y: lax.rem(y + (1 - c) * step, 4), Z: lax.rem(z + c * step, 4)}

    weight_x = Ring(
        links,
        lambda step: {X: lax.rem(x + step, 4)},
        (
            (out_all.at[0, part_rows(along)], out_all.at[2, part_rows(along)]),
            (out_all.at[0, part_rows(along)], out_all.at[1, part_rows(along)]),
        ),
        (
            (out_all.at[2, part_rows(along, 0)], out_all.at[3, part_rows(along, 0)]),
            (out_all.at[1, part_rows(along, 1)], out_all.at[3, part_rows(along, 1)]),
        ),
        (out_all.at[pl.ds(1, 2), part_rows(along)], out_all.at[3, part_rows(along)]),
    )

    def weight_ring(slots):
        own, low, high = (
            out_all.at[slots, part_rows(along)],
            out_all.at[slots, part_rows(lax.rem(along + 3, 4), 0)],
            out_all.at[slots, part_rows(lax.rem(along + 1, 4), 1)],
        )
        return Ring(
            links,
            on_line,
            ((own, own), (own, own)),
            ((low, low), (high, high)),
            (out_all.at[slots, pl.ds(0, 64)], own),
        )

    weight_near, weight_far = weight_ring(pl.ds(1, 2)), weight_ring(pl.ds(3, 1))
    half_rows = pl.ds(pl.multiple_of(128 * c, 128), 128)

    scale = 128 ** (-0.5)
    at_row = lax.broadcasted_iota(jnp.int32, (BLOCK, BLOCK), 0)
    at_col = lax.broadcasted_iota(jnp.int32, (BLOCK, BLOCK), 1)
    upto = jnp.where(at_row <= at_col, 1.0, 0.0).astype(f32)
    cum_rows, cum_cols = [], []
    local["logs"].wait()
    for b in range(2):
        logs = jnp.concatenate(
            [logs_in[:, BLOCK * b : BLOCK * (b + 1)], jnp.zeros((6, BLOCK), f32)], axis=0
        )
        cum = jnp.dot(logs, upto, precision=lax.Precision.HIGHEST, preferred_element_type=f32)
        cum_rows.append(cum)
        cum_cols.append(cum.T)
    ends = [[cum_rows[b][h : h + 1, BLOCK - 1 : BLOCK] for b in range(2)] for h in range(2)]
    local["k"].wait()
    local["v"].wait()
    first_state, span = [], []
    for h in range(2):
        heads = slice(128 * h, 128 * (h + 1))
        added = []
        for b in range(2):
            lines = slice(BLOCK * b, BLOCK * (b + 1))
            to_end = jnp.exp(ends[h][b] - cum_cols[b][:, h : h + 1]) * scale
            scaled = (k[lines, heads].astype(f32) * to_end).astype(bf16)
            added.append(
                lax.dot_general(
                    scaled, v[lines, heads], (((0,), (0,)), ((), ())), preferred_element_type=f32
                )
            )
        first_state.append(added[0])
        span.append(
            (
                jnp.exp(over_lanes(ends[h][1])) * added[0] + added[1],
                jnp.exp(over_lanes(ends[h][0] + ends[h][1])),
            )
        )
        write_state(state_c.at[0, h], *span[h])
    pl.semaphore_wait(barrier, len(near))
    pair = links.arrival()
    links.send(pair, state_c.at[0], state_c.at[1], **{C: other})
    local["up"].wait()
    wide[1].own()
    local["weight"].wait()
    weight_x.start()
    local["down"].wait()
    swap = links.arrival()
    links.send(swap, half_down.at[c], half_down.at[c], **{C: other})
    local["gate"].wait()

    def within(h, b):
        heads, lines = slice(128 * h, 128 * (h + 1)), slice(BLOCK * b, BLOCK * (b + 1))
        col, row = cum_cols[b][:, h : h + 1], cum_rows[b][h : h + 1]
        products = lax.dot_general(
            q[lines, heads], k[lines, heads], (((1,), (1,)), ((), ())), preferred_element_type=f32
        )
        factor = jnp.where(at_row >= at_col, jnp.exp(jnp.minimum(col - row, 0.0)), 0.0)
        scores = (products * scale * factor).astype(bf16)
        result = jnp.dot(scores, v[lines, heads], preferred_element_type=f32)
        if b == 1:
            result = result + jnp.exp(col) * jnp.dot(
                q[lines, heads], first_state[h].astype(bf16), preferred_element_type=f32
            )
            col = col + ends[h][0]
        retention[h, lines, :] = result
        decayed[h, lines, :] = jnp.broadcast_to(jnp.exp(col), (BLOCK, 128))

    nothing = (jnp.zeros((128, 128), f32), jnp.ones((1, 128), f32))

    def among(slots, axis, index):
        came = links.arrival()
        for step in (2, 1, 3):
            links.send(came, slots.at[index], slots.at[index], **{axis: lax.rem(index + step, 4)})

        def fold():
            came.wait(slots.at[pl.ds(0, 3)])
            total, before = nothing, nothing
            for at in range(4):
                total = followed_by(total, read_state(slots.at[at]))
                before = chosen(at < index, total, before)
            return total, before

        return fold

    local["q"].wait()
    within(0, 0)
    pair.wait(state_c.at[1])
    partner = [read_state(state_c.at[1, h]) for h in range(2)]
    first = c == 0
    chip = [
        followed_by(chosen(first, span[h], partner[h]), chosen(first, partner[h], span[h]))
        for h in range(2)
    ]
    write_state(state_y.at[y], *chosen(first, chip[0], chip[1]))
    fold_y = among(state_y, Y, y)
    wide[0].own()
    within(0, 1)
    within(1, 0)
    line, before_y = fold_y()
    write_state(state_z.at[z], *line)
    fold_z = among(state_z, Z, z)
    swap.wait(half_down.at[other])
    turned[...] = jnp.concatenate([half_down[0], half_down[1]], axis=0).T
    down_all[z, y, own_half, :] = turned[own_half, :]
    within(1, 1)
    weight_x.pass_on()
    weight_near.start()
    _, before_z = fold_z()
    state_in[c] = followed_by(before_z, before_y)[0]
    both_heads = links.arrival()
    links.send(both_heads, state_in.at[c], state_in.at[c], **{C: other})
    weight_x.finish()
    weight_far.start()
    for gather in (wide[1], wide[0]):
        gather.pass_on()
    for gather in narrow:
        gather.own()
    for name in ("g", "norm"):
        local[name].wait()
    both_heads.wait(state_in.at[other])
    entering = [
        jnp.where(first, state_in[h], partner[h][1] * state_in[h] + partner[h][0]).astype(bf16)
        for h in range(2)
    ]

    top, bottom = pl.ds(0, 128), pl.ds(128, 128)
    came, to_pass = links.arrival(), links.arrival()
    for step in (2, 1, 3, 0):
        quarter = lax.rem(x + step, 4)
        lines = pl.ds(pl.multiple_of(256 * quarter, 256), 256)
        for h in range(2):
            heads = slice(128 * h, 128 * (h + 1))
            carried = jnp.dot(q[lines, heads], entering[h], preferred_element_type=f32)
            value = retention[h, lines, :] + carried * decayed[h, lines, :]
            centered = value - jnp.mean(value, axis=-1, keepdims=True)
            variance = jnp.mean(centered * centered, axis=-1, keepdims=True)
            normed = centered * lax.rsqrt(variance + EPSILON) * norm_in[h : h + 1, :]
            retained[step, :, heads] = (jax.nn.silu(g[lines, heads].astype(f32)) * normed).astype(
                bf16
            )
        if step == 2:
            links.send(came, retained.at[2, top], regrouped.at[3, top], **{X: x_far})
            links.send(to_pass, retained.at[2, bottom], passing, **{X: x_down})
        elif step:
            slot = 2 if step == 1 else 1
            links.send(came, retained.at[step], regrouped.at[slot], **{X: quarter})
    weight_near.pass_on()
    weight_far.pass_on()
    for gather in narrow:
        gather.pass_on()
    for gather in (wide[1], wide[0]):
        gather.line()
    to_pass.wait(passing)
    links.send(came, passing, regrouped.at[3, bottom], **{X: x_down})
    weight_near.finish()
    near_half = out_all.at[pl.ds(1, 2), half_rows]
    shared = links.arrival()
    links.send(shared, near_half, near_half, **{C: other})
    weight_far.finish()
    far_half = out_all.at[3, half_rows]
    links.send(shared, far_half, far_half, **{C: other})
    for name in ("resid", "mix", "in", "out"):
        local[name].wait()
    came.wait(regrouped.at[pl.ds(1, 3)])
    shared.wait(out_all.at[pl.ds(1, 3), half_rows])

    for j in range(8):
        lanes = slice(256 * j, 256 * (j + 1))
        total = jnp.zeros((256, 256), f32)
        for slot in range(4):
            block = regrouped[slot] if slot else retained[0]
            part = jnp.dot(block, out_all[slot, :, lanes], preferred_element_type=f32)
            total = total + part.astype(bf16).astype(f32)
        partial[0, :, lanes] = total.astype(bf16)

    piece = [pl.ds(64 * at, 64) for at in range(4)]
    first_rows = [links.arrival(), links.arrival()]
    for at in range(2):

        @pl.loop(0, 4)
        def _(step):
            for start in (64 * at, 64 * at + 128):
                lines = pl.ds(pl.multiple_of(start + 16 * step, 16), 16)
                mid = (
                    middle[lines, :].astype(f32) + rms_norm(partial[0, lines, :], gains[0])
                ).astype(bf16)
                middle[lines, :] = mid
                rows[x, lines, :] = rms_norm(mid, gains[1]).astype(bf16)

        for target, lines in ((x_up, piece[at]), (x_down, piece[2 + at])):
            links.send(first_rows[at], rows.at[x, lines], rows.at[x, lines], **{X: target})
    for gather in narrow:
        gather.line()
    for gather in (*wide, *narrow):
        gather.give(gather.j)
    far, nearby = links.arrival(), links.arrival()
    for at in range(2):
        first_rows[at].wait(rows.at[x, top])
        for target, source, lines in ((x_up, x_down, piece[at]), (x_down, x_up, piece[2 + at])):
            links.send(far, rows.at[source, lines], rows.at[source, lines], **{X: target})
        if at == 0:
            for gather in wide:
                gather.pass_line()
    for lines, target in ((bottom, x_up), (top, x_down)):
        links.send(nearby, rows.at[x, lines], rows.at[x, lines], **{X: target})
    for gather in narrow:
        gather.pass_line()
    for gather in wide:
        gather.end_line()
    for gather in wide:
        gather.arrive()

    def gate_up(owner, slot):
        block = rows[owner]
        for j in range(11):
            lanes = slice(128 * j, 128 * (j + 1))
            weights = jnp.concatenate(
                [
                    gate_all[:, :, :, :, lanes].reshape(2048, 128),
                    up_all[:, :, :, :, lanes].reshape(2048, 128),
                ],
                axis=1,
            )
            both = jnp.dot(block, weights, preferred_element_type=f32)
            hidden[slot, :, lanes] = (jax.nn.silu(both[:, :128]) * both[:, 128:]).astype(bf16)

    def down(slot, to, lines=pl.ds(0, 256), extra=None):
        block = hidden[slot, lines, :]
        for j in range(8):
            weights = jnp.concatenate(
                [down_all[j // 2, 2 * j % 4], down_all[j // 2, 2 * j % 4 + 1]], axis=1
            )
            part = jnp.dot(block, weights, preferred_element_type=f32)
            lanes = slice(256 * j, 256 * (j + 1))
            if extra is not None:
                part = part + relay[extra, :, lanes].astype(f32)
            partial[to, lines, lanes] = part.astype(bf16)

    far.wait(rows.at[x_far])
    gate_up(x_far, 2)
    for gather in narrow:
        gather.end_line()
    for gather in narrow:
        gather.arrive()
    down(2, 1)
    relay_up, relay_down = links.arrival(), links.arrival()
    links.send(relay_up, partial.at[1, top], relay.at[0], **{X: x_up})
    links.send(relay_down, partial.at[1, bottom], relay.at[1], **{X: x_down})
    nearby.wait(rows.at[x_up])
    gate_up(x_up, 0)
    down(0, 2, bottom)
    last = [links.arrival() for _ in range(3)]
    links.send(last[2], partial.at[2, bottom], final.at[0, bottom], **{X: x_up})
    gate_up(x_down, 1)
    down(1, 3, top)
    links.send(last[2], partial.at[3, top], final.at[1, top], **{X: x_down})
    gate_up(x, 2)
    relay_up.wait(relay.at[0])
    down(0, 2, top, 0)
    for at in range(2):
        links.send(last[at], partial.at[2, piece[at]], final.at[0, piece[at]], **{X: x_up})
    relay_down.wait(relay.at[1])
    down(1, 3, bottom, 1)
    for at in range(2):
        links.send(last[at], partial.at[3, piece[2 + at]], final.at[1, piece[2 + at]], **{X: x_down})
    down(2, 0)
    last[2].wait(final.at[0])
    for at in range(2):
        last[at].wait(final.at[0, top])

        @pl.loop(0, 4)
        def _(step):
            for start in (64 * at, 64 * at + 128):
                lines = pl.ds(pl.multiple_of(start + 16 * step, 16), 16)
                branch = (
                    partial[0, lines, :].astype(f32)
                    + final[0, lines, :].astype(f32)
                    + final[1, lines, :].astype(f32)
                ).astype(bf16)
                out[lines, :] = (
                    middle[lines, :].astype(f32) + rms_norm(branch, gains[2])
                ).astype(bf16)

    links.finish()


def per_device(
    queries, keys, values, gates, log_decay, norm_gain, out_weight, resid, post_mix_gain, pre_ffn_gain,
    w_gate, w_up, w_down, post_ffn_gain,
):
    f32, bf16 = jnp.float32, jnp.bfloat16
    operands = (
        queries, keys, values, gates, log_decay.T, norm_gain, out_weight, resid, post_mix_gain[None],
        pre_ffn_gain[None], w_gate, w_up, w_down.T, post_ffn_gain[None],
    )
    return pl.pallas_call(
        layer_kernel,
        out_shape=jax.ShapeDtypeStruct((256, 2048), bf16),
        in_specs=[pl.BlockSpec(memory_space=pl.ANY)] * 14,
        out_specs=pl.BlockSpec(memory_space=pltpu.VMEM),
        scratch_shapes=[
            pltpu.VMEM((4, 4, 2, 64, 1408), bf16),
            pltpu.VMEM((4, 4, 2, 64, 1408), bf16),
            pltpu.VMEM((4, 4, 1408, 128), bf16),
            pltpu.VMEM((4, 256, 2048), bf16),
            pltpu.VMEM((3, 256, 1408), bf16),
            pltpu.VMEM((4, 256, 2048), bf16),
            pltpu.VMEM((2, 128, 2048), bf16),
            pltpu.VMEM((2, 256, 2048), bf16),
            pltpu.VMEM((2, 64, 1408), bf16),
            pltpu.VMEM((1408, 128), bf16),
            pltpu.VMEM((1024, 256), bf16),
            pltpu.VMEM((1024, 256), bf16),
            pltpu.VMEM((1024, 256), bf16),
            pltpu.VMEM((1024, 256), bf16),
            pltpu.VMEM((2, 1024, 128), f32),
            pltpu.VMEM((2, 1024, 128), f32),
            pltpu.VMEM((2, 2, 144, 128), bf16),
            pltpu.VMEM((4, 144, 128), bf16),
            pltpu.VMEM((4, 144, 128), bf16),
            pltpu.VMEM((2, 128, 128), f32),
            pltpu.VMEM((4, 256, 256), bf16),
            pltpu.VMEM((4, 256, 256), bf16),
            pltpu.VMEM((128, 256), bf16),
            pltpu.VMEM((4, 256, 2048), bf16),
            pltpu.VMEM((256, 2048), bf16),
            pltpu.VMEM((2, 1024), f32),
            pltpu.VMEM((3, 1, 2048), f32),
            pltpu.VMEM((2, 128), f32),
            pltpu.SemaphoreType.DMA((14,)),
            pltpu.SemaphoreType.DMA((SENDS,)),
            pltpu.SemaphoreType.DMA((ARRIVALS,)),
        ],
        compiler_params=pltpu.CompilerParams(
            collective_id=0, has_side_effects=True, vmem_limit_bytes=48 * 2**20
        ),
        name="layer",
    )(*(pltpu.with_memory_space_constraint(a, pltpu.HBM) for a in operands))


def solution(mesh):
    split = Mesh(mesh.devices.reshape(4, 4, 2, mesh.shape["tp"]), ("sp_0", "sp_1", "sp_2", "tp"))
    placed = (
        P(SP, "tp"),
        P(SP, "tp"),
        P(SP, "tp"),
        P(SP, "tp"),
        P(SP, "tp"),
        P("tp", None),
        P("tp", None),
        P(SP_TP, None),
        P(),
        P(),
        P(SP, "tp"),
        P(SP, "tp"),
        P("tp", SP),
        P(),
    )
    return jax.shard_map(
        per_device, mesh=split, in_specs=placed, out_specs=P(SP_TP, None), check_vma=False
    )
```

```python
import jax
import jax.numpy as jnp
from jax import lax
from jax.experimental import pallas as pl
from jax.experimental.pallas import tpu as pltpu
from jax.sharding import Mesh
from jax.sharding import PartitionSpec as P

BLOCK = 512
SP = ("sp_0", "sp_1", "sp_2")
SP_TP = ("sp_0", "sp_1", "sp_2", "tp")


EPSILON = 1e-06
MESH_ID = pl.DeviceIdType.MESH
SENDS, ARRIVALS = 40, 48
Z, Y, C, X = SP_TP


class Arrival:
    def __init__(self, links, at):
        self.links, self.at = links, at

    def wait(self, as_large):
        pltpu.make_async_remote_copy(
            src_ref=as_large,
            dst_ref=as_large,
            send_sem=self.links.send_sem.at[0],
            recv_sem=self.links.recv_sem.at[self.at],
            device_id={X: lax.rem(lax.axis_index(X) + 1, 4)},
            device_id_type=MESH_ID,
        ).wait_recv()


class Links:
    def __init__(self, send_sem, recv_sem):
        self.send_sem, self.recv_sem, self.copies, self.arrivals = send_sem, recv_sem, [], 0

    def arrival(self):
        self.arrivals += 1
        return Arrival(self, self.arrivals - 1)

    def send(self, arrival, src, dst, **where):
        at = len(self.copies)
        if at >= SENDS:
            self.copies[at - SENDS].wait_send()
        copy = pltpu.make_async_remote_copy(
            src_ref=src,
            dst_ref=dst,
            send_sem=self.send_sem.at[at % SENDS],
            recv_sem=self.recv_sem.at[arrival.at],
            device_id={axis: index for axis, index in where.items()},
            device_id_type=MESH_ID,
        )
        copy.start()
        self.copies.append(copy)

    def finish(self):
        for copy in self.copies[-SENDS:]:
            copy.wait_send()
        assert self.arrivals <= ARRIVALS


class PlaneGather:
    def __init__(self, links, at, first, second, here, core):
        self.links, self.at, self.first, self.second, self.core = links, at, first, second, core
        self.i, self.j = here
        self.i_up, self.i_down = lax.rem(self.i + 1, 4), lax.rem(self.i + 3, 4)
        self.j_up, self.j_down = lax.rem(self.j + 1, 4), lax.rem(self.j + 3, 4)
        self.across = links.arrival()

    def both_ways(self, axis, up, down, block_up, block_down):
        arrival = self.links.arrival()
        self.links.send(arrival, block_up, block_up, **{axis: up})
        self.links.send(arrival, block_down, block_down, **{axis: down})
        return arrival

    def own(self):
        block = self.at(self.i, self.j)
        self.came = self.both_ways(self.first, self.i_up, self.i_down, block, block)

    def pass_on(self):
        self.came.wait(self.at(pl.ds(0, 2), self.j))
        self.came = self.both_ways(
            self.first,
            self.i_up,
            self.i_down,
            self.at(self.i_down, self.j, part=0),
            self.at(self.i_up, self.j, part=1),
        )

    def give(self, j, items=pl.ds(0, 4)):
        block = self.at(items, j)
        self.links.send(self.across, block, block, **{C: 1 - self.core})

    def line(self):
        self.came.wait(self.at(self.i, self.j))
        block = self.at(pl.ds(0, 4), self.j)
        self.came = self.both_ways(self.second, self.j_up, self.j_down, block, block)

    def pass_line(self):
        self.came.wait(self.at(pl.ds(0, 4), pl.ds(0, 2)))
        self.passed = [
            self.both_ways(
                self.second,
                self.j_up,
                self.j_down,
                self.at(pl.ds(at, 1), self.j_down),
                self.at(pl.ds(2 + at, 1), self.j_up),
            )
            for at in range(2)
        ]
        self.give(self.j_down)
        self.give(self.j_up)

    def end_line(self):
        far = lax.rem(self.j + 2, 4)
        for at, arrival in enumerate(self.passed):
            arrival.wait(self.at(pl.ds(0, 2), far))
            for start in (0, 2):
                self.give(far, pl.ds(start + at, 1))

    def arrive(self):
        self.across.wait(self.at(pl.ds(0, 4), pl.ds(0, 4)))


class Ring:
    def __init__(self, links, where, own, passed, as_large):
        self.links, self.where, self.own, self.passed, self.as_large = links, where, own, passed, as_large

    def both_ways(self, pairs):
        self.came = self.links.arrival()
        for step, (src, dst) in zip((1, 3), pairs):
            self.links.send(self.came, src, dst, **self.where(step))

    def start(self):
        self.both_ways(self.own)

    def pass_on(self):
        self.came.wait(self.as_large[0])
        self.both_ways(self.passed)

    def finish(self):
        self.came.wait(self.as_large[1])


def rms_norm(values_in, gain_vec):
    widened = values_in.astype(jnp.float32)
    return (
        widened
        * lax.rsqrt(jnp.mean(widened * widened, axis=-1, keepdims=True) + EPSILON)
        * gain_vec
    )


def over_lanes(scalar):
    return jnp.broadcast_to(scalar, (1, 128))


def write_state(ref, state, decay):
    ref[pl.ds(0, 128), :] = state.astype(jnp.bfloat16)
    row = lax.broadcasted_iota(jnp.int32, (16, 128), 0)
    large = decay.astype(jnp.bfloat16).astype(jnp.float32)
    ref[pl.ds(128, 16), :] = jnp.where(row == 0, large, decay - large).astype(jnp.bfloat16)


def read_state(ref):
    both = ref[pl.ds(128, 16), :].astype(jnp.float32)
    return ref[pl.ds(0, 128), :].astype(jnp.float32), both[0:1] + both[1:2]


def followed_by(earlier, later):
    return later[1] * earlier[0] + later[0], later[1] * earlier[1]


def chosen(which, a, b):
    return jax.tree.map(lambda p, q: jnp.where(which, p, q), a, b)


def layer_kernel(
    queries, keys, values, gates, log_decay, norm_gain, out_weight, resid, mix_gain, in_gain,
    w_gate, w_up, w_down, out_gain, out,
    gate_all, up_all, down_all, rows, hidden, partial, relay, final, half_down, turned,
    q, k, v, g, retention, decayed, state_c, state_y, state_z, state_in, retained, regrouped, passing, out_all, mixed, middle, logs_in, gains, norm_in,
    local_sem, send_sem, recv_sem,
):
    f32, bf16 = jnp.float32, jnp.bfloat16
    z, y, c, x = (lax.axis_index(axis) for axis in SP_TP)
    other, x_up, x_down, x_far = 1 - c, lax.rem(x + 1, 4), lax.rem(x + 3, 4), lax.rem(x + 2, 4)
    own_half = pl.ds(pl.multiple_of(704 * c, 64), 704)
    names = ("logs", "k", "v", "gate", "up", "q", "down", "weight", "g", "resid", "mix", "in", "out", "norm")
    moves = (
        (log_decay, logs_in), (keys, k), (values, v), (w_gate, gate_all.at[z, y, c]), (w_up, up_all.at[z, y, c]), (queries, q),
        (w_down, half_down.at[c]), (out_weight, out_all.at[0]), (gates, g), (resid, middle),
        (mix_gain, gains.at[0]), (in_gain, gains.at[1]), (out_gain, gains.at[2]), (norm_gain, norm_in),
    )
    local = {
        name: pltpu.make_async_copy(src, dst, local_sem.at[at])
        for at, (name, (src, dst)) in enumerate(zip(names, moves))
    }
    for copy in local.values():
        copy.start()

    barrier = pltpu.get_barrier_semaphore()
    near = [{C: other}]
    for axis, index in ((X, x), (Y, y), (Z, z)):
        near += [{axis: lax.rem(index + step, 4)} for step in (1, 2, 3)]
    for where in near:
        pl.semaphore_signal(barrier, inc=1, device_id=where, device_id_type=MESH_ID)

    links = Links(send_sem, recv_sem)

    def gate_at(i, j, part=None):
        lines = pl.ds(0, 64) if part is None else pl.ds(32 * part, 32)
        return gate_all.at[j, i, c, lines]

    def up_at(i, j, part=None):
        lines = pl.ds(0, 64) if part is None else pl.ds(32 * part, 32)
        return up_all.at[i, j, c, lines]

    def down_lines(start, part):
        first, length = (start, 352) if part is None else (start + 176 * part, 176)
        return pl.ds(pl.multiple_of(704 * c + first, 16), length)

    wide = (
        PlaneGather(links, gate_at, Y, Z, (y, z), c),
        PlaneGather(links, up_at, Z, Y, (z, y), c),
    )
    narrow = (
        PlaneGather(
            links, lambda i, j, part=None: down_all.at[j, i, down_lines(0, part)], Y, Z, (y, z), c
        ),
        PlaneGather(
            links, lambda i, j, part=None: down_all.at[i, j, down_lines(352, part)], Z, Y, (z, y), c
        ),
    )

    along = (1 - c) * y + c * z

    def part_rows(i, part=None):
        first, length = (0, 32) if part is None else (16 * part, 16)
        return pl.ds(pl.multiple_of(128 * c + 32 * i + first, 16), length)

    def on_line(step):
        return {Y: lax.rem(y + (1 - c) * step, 4), Z: lax.rem(z + c * step, 4)}

    weight_x = Ring(
        links,
        lambda step: {X: lax.rem(x + step, 4)},
        (
            (out_all.at[0, part_rows(along)], out_all.at[2, part_rows(along)]),
            (out_all.at[0, part_rows(along)], out_all.at[1, part_rows(along)]),
        ),
        (
            (out_all.at[2, part_rows(along, 0)], out_all.at[3, part_rows(along, 0)]),
            (out_all.at[1, part_rows(along, 1)], out_all.at[3, part_rows(along, 1)]),
        ),
        (out_all.at[pl.ds(1, 2), part_rows(along)], out_all.at[3, part_rows(along)]),
    )

    def weight_ring(slots):
        own, low, high = (
            out_all.at[slots, part_rows(along)],
            out_all.at[slots, part_rows(lax.rem(along + 3, 4), 0)],
            out_all.at[slots, part_rows(lax.rem(along + 1, 4), 1)],
        )
        return Ring(
            links,
            on_line,
            ((own, own), (own, own)),
            ((low, low), (high, high)),
            (out_all.at[slots, pl.ds(0, 64)], own),
        )

    weight_far = weight_ring(pl.ds(3, 1))
    weight_rest = links.arrival()

    def send_rest(steps):
        for step in steps:
            part = part_rows(lax.rem(along + step, 4))
            for slot, target in ((2, x_up), (1, x_down)):
                links.send(weight_rest, out_all.at[0, part], out_all.at[slot, part], **{X: target})

    half_rows = pl.ds(pl.multiple_of(128 * c, 128), 128)

    scale = 128 ** (-0.5)
    at_row = lax.broadcasted_iota(jnp.int32, (BLOCK, BLOCK), 0)
    at_col = lax.broadcasted_iota(jnp.int32, (BLOCK, BLOCK), 1)
    upto = jnp.where(at_row <= at_col, 1.0, 0.0).astype(f32)
    cum_rows, cum_cols = [], []
    local["logs"].wait()
    for b in range(2):
        logs = jnp.concatenate(
            [logs_in[:, BLOCK * b : BLOCK * (b + 1)], jnp.zeros((6, BLOCK), f32)], axis=0
        )
        cum = jnp.dot(logs, upto, precision=lax.Precision.HIGHEST, preferred_element_type=f32)
        cum_rows.append(cum)
        cum_cols.append(cum.T)
    ends = [[cum_rows[b][h : h + 1, BLOCK - 1 : BLOCK] for b in range(2)] for h in range(2)]
    local["k"].wait()
    local["v"].wait()
    first_state, span = [], []
    for h in range(2):
        heads = slice(128 * h, 128 * (h + 1))
        added = []
        for b in range(2):
            lines = slice(BLOCK * b, BLOCK * (b + 1))
            to_end = jnp.exp(ends[h][b] - cum_cols[b][:, h : h + 1]) * scale
            scaled = (k[lines, heads].astype(f32) * to_end).astype(bf16)
            added.append(
                lax.dot_general(
                    scaled, v[lines, heads], (((0,), (0,)), ((), ())), preferred_element_type=f32
                )
            )
        first_state.append(added[0])
        span.append(
            (
                jnp.exp(over_lanes(ends[h][1])) * added[0] + added[1],
                jnp.exp(over_lanes(ends[h][0] + ends[h][1])),
            )
        )
        write_state(state_c.at[0, h], *span[h])
    pl.semaphore_wait(barrier, len(near))
    pair = links.arrival()
    links.send(pair, state_c.at[0], state_c.at[1], **{C: other})
    local["up"].wait()
    wide[1].own()
    local["weight"].wait()
    weight_x.start()
    send_rest((1,))
    local["down"].wait()
    swap = links.arrival()
    links.send(swap, half_down.at[c], half_down.at[c], **{C: other})
    local["gate"].wait()

    def within(h, b):
        heads, lines = slice(128 * h, 128 * (h + 1)), slice(BLOCK * b, BLOCK * (b + 1))
        col, row = cum_cols[b][:, h : h + 1], cum_rows[b][h : h + 1]
        products = lax.dot_general(
            q[lines, heads], k[lines, heads], (((1,), (1,)), ((), ())), preferred_element_type=f32
        )
        factor = jnp.where(at_row >= at_col, jnp.exp(jnp.minimum(col - row, 0.0)), 0.0)
        scores = (products * scale * factor).astype(bf16)
        result = jnp.dot(scores, v[lines, heads], preferred_element_type=f32)
        if b == 1:
            result = result + jnp.exp(col) * jnp.dot(
                q[lines, heads], first_state[h].astype(bf16), preferred_element_type=f32
            )
            col = col + ends[h][0]
        retention[h, lines, :] = result
        decayed[h, lines, :] = jnp.broadcast_to(jnp.exp(col), (BLOCK, 128))

    nothing = (jnp.zeros((128, 128), f32), jnp.ones((1, 128), f32))

    def among(slots, axis, index):
        came = links.arrival()
        for step in (2, 1, 3):
            links.send(came, slots.at[index], slots.at[index], **{axis: lax.rem(index + step, 4)})

        def fold():
            came.wait(slots.at[pl.ds(0, 3)])
            total, before = nothing, nothing
            for at in range(4):
                total = followed_by(total, read_state(slots.at[at]))
                before = chosen(at < index, total, before)
            return total, before

        return fold

    local["q"].wait()
    within(0, 0)
    pair.wait(state_c.at[1])
    partner = [read_state(state_c.at[1, h]) for h in range(2)]
    first = c == 0
    chip = [
        followed_by(chosen(first, span[h], partner[h]), chosen(first, partner[h], span[h]))
        for h in range(2)
    ]
    write_state(state_y.at[y], *chosen(first, chip[0], chip[1]))
    fold_y = among(state_y, Y, y)
    wide[0].own()
    within(0, 1)
    within(1, 0)
    line, before_y = fold_y()
    write_state(state_z.at[z], *line)
    fold_z = among(state_z, Z, z)
    swap.wait(half_down.at[other])
    turned[...] = jnp.concatenate([half_down[0], half_down[1]], axis=0).T
    down_all[z, y, own_half, :] = turned[own_half, :]
    within(1, 1)
    weight_x.pass_on()
    send_rest((2, 3))
    wide[1].pass_on()
    _, before_z = fold_z()
    state_in[c] = followed_by(before_z, before_y)[0]
    both_heads = links.arrival()
    links.send(both_heads, state_in.at[c], state_in.at[c], **{C: other})
    wide[0].pass_on()
    weight_x.finish()
    weight_far.start()
    for gather in narrow:
        gather.own()
    for name in ("g", "norm"):
        local[name].wait()
    both_heads.wait(state_in.at[other])
    entering = [
        jnp.where(first, state_in[h], partner[h][1] * state_in[h] + partner[h][0]).astype(bf16)
        for h in range(2)
    ]

    top, bottom = pl.ds(0, 128), pl.ds(128, 128)
    near_came, far_came, to_pass = (links.arrival() for _ in range(3))
    for step in (2, 1, 3, 0):
        quarter = lax.rem(x + step, 4)
        lines = pl.ds(pl.multiple_of(256 * quarter, 256), 256)
        for h in range(2):
            heads = slice(128 * h, 128 * (h + 1))
            carried = jnp.dot(q[lines, heads], entering[h], preferred_element_type=f32)
            value = retention[h, lines, :] + carried * decayed[h, lines, :]
            centered = value - jnp.mean(value, axis=-1, keepdims=True)
            variance = jnp.mean(centered * centered, axis=-1, keepdims=True)
            normed = centered * lax.rsqrt(variance + EPSILON) * norm_in[h : h + 1, :]
            retained[step, :, heads] = (jax.nn.silu(g[lines, heads].astype(f32)) * normed).astype(
                bf16
            )
        if step == 2:
            links.send(far_came, retained.at[2, top], regrouped.at[3, top], **{X: x_far})
            links.send(to_pass, retained.at[2, bottom], passing, **{X: x_down})
        elif step:
            slot = 2 if step == 1 else 1
            links.send(near_came, retained.at[step], regrouped.at[slot], **{X: quarter})
    weight_far.pass_on()
    for gather in narrow:
        gather.pass_on()
    for gather in (wide[1], wide[0]):
        gather.line()
    to_pass.wait(passing)
    links.send(far_came, passing, regrouped.at[3, bottom], **{X: x_down})
    shared, shared_far = links.arrival(), links.arrival()
    weight_rest.wait(out_all.at[pl.ds(1, 2), pl.ds(0, 96)])
    near_half, far_half = out_all.at[pl.ds(1, 2), half_rows], out_all.at[3, half_rows]
    links.send(shared, near_half, near_half, **{C: other})
    weight_far.finish()
    links.send(shared_far, far_half, far_half, **{C: other})
    for name in ("resid", "mix", "in", "out"):
        local[name].wait()
    near_came.wait(regrouped.at[pl.ds(1, 2)])
    shared.wait(out_all.at[pl.ds(1, 2), half_rows])

    def mix_part(slot, lanes):
        block = regrouped[slot] if slot else retained[0]
        part = jnp.dot(block, out_all[slot, :, lanes], preferred_element_type=f32)
        return part.astype(bf16).astype(f32)

    for j in range(8):
        lanes = slice(256 * j, 256 * (j + 1))
        mixed[:, lanes] = mix_part(0, lanes) + mix_part(1, lanes) + mix_part(2, lanes)
    far_came.wait(regrouped.at[3])
    shared_far.wait(out_all.at[3, half_rows])
    for j in range(8):
        lanes = slice(256 * j, 256 * (j + 1))
        partial[0, :, lanes] = (mixed[:, lanes] + mix_part(3, lanes)).astype(bf16)

    piece = [pl.ds(64 * at, 64) for at in range(4)]
    first_rows = [links.arrival(), links.arrival()]
    for at in range(4):

        @pl.loop(0, 2)
        def _(step):
            for start in (32 * at, 32 * at + 128):
                lines = pl.ds(pl.multiple_of(start + 16 * step, 16), 16)
                mid = (
                    middle[lines, :].astype(f32) + rms_norm(partial[0, lines, :], gains[0])
                ).astype(bf16)
                middle[lines, :] = mid
                rows[x, lines, :] = rms_norm(mid, gains[1]).astype(bf16)

        for target, start in ((x_up, 32 * at), (x_down, 32 * at + 128)):
            lines = pl.ds(start, 32)
            links.send(first_rows[at // 2], rows.at[x, lines], rows.at[x, lines], **{X: target})
    for gather in narrow:
        gather.line()
    for gather in (*wide, *narrow):
        gather.give(gather.j)
    far, nearby = links.arrival(), links.arrival()
    for at in range(2):
        first_rows[at].wait(rows.at[x, top])
        for target, source, lines in ((x_up, x_down, piece[at]), (x_down, x_up, piece[2 + at])):
            links.send(far, rows.at[source, lines], rows.at[source, lines], **{X: target})
        if at == 0:
            for gather in wide:
                gather.pass_line()
    for lines, target in ((bottom, x_up), (top, x_down)):
        links.send(nearby, rows.at[x, lines], rows.at[x, lines], **{X: target})
    for gather in narrow:
        gather.pass_line()
    for gather in wide:
        gather.end_line()
    for gather in wide:
        gather.arrive()

    def gate_up(owner, slot, tiles=range(11)):
        block = rows[owner]
        for j in tiles:
            lanes = slice(128 * j, 128 * (j + 1))
            weights = jnp.concatenate(
                [
                    gate_all[:, :, :, :, lanes].reshape(2048, 128),
                    up_all[:, :, :, :, lanes].reshape(2048, 128),
                ],
                axis=1,
            )
            both = jnp.dot(block, weights, preferred_element_type=f32)
            hidden[slot, :, lanes] = (jax.nn.silu(both[:, :128]) * both[:, 128:]).astype(bf16)

    def down(slot, to, lines=pl.ds(0, 256), extra=None):
        block = hidden[slot, lines, :]
        for j in range(8):
            weights = jnp.concatenate(
                [down_all[j // 2, 2 * j % 4], down_all[j // 2, 2 * j % 4 + 1]], axis=1
            )
            part = jnp.dot(block, weights, preferred_element_type=f32)
            lanes = slice(256 * j, 256 * (j + 1))
            if extra is not None:
                part = part + relay[extra, :, lanes].astype(f32)
            partial[to, lines, lanes] = part.astype(bf16)

    far.wait(rows.at[x_far])
    gate_up(x_far, 2, range(6))
    for gather in narrow:
        gather.end_line()
    gate_up(x_far, 2, range(6, 11))
    for gather in narrow:
        gather.arrive()
    down(2, 1)
    relay_up, relay_down = links.arrival(), links.arrival()
    links.send(relay_up, partial.at[1, top], relay.at[0], **{X: x_up})
    links.send(relay_down, partial.at[1, bottom], relay.at[1], **{X: x_down})
    nearby.wait(rows.at[x_up])
    gate_up(x_up, 0)
    down(0, 2, bottom)
    last = [links.arrival() for _ in range(3)]
    links.send(last[2], partial.at[2, bottom], final.at[0, bottom], **{X: x_up})
    gate_up(x_down, 1)
    down(1, 3, top)
    links.send(last[2], partial.at[3, top], final.at[1, top], **{X: x_down})
    gate_up(x, 2)
    relay_up.wait(relay.at[0])
    down(0, 2, top, 0)
    for at in range(2):
        links.send(last[at], partial.at[2, piece[at]], final.at[0, piece[at]], **{X: x_up})
    relay_down.wait(relay.at[1])
    down(1, 3, bottom, 1)
    for at in range(2):
        links.send(last[at], partial.at[3, piece[2 + at]], final.at[1, piece[2 + at]], **{X: x_down})
    down(2, 0)
    last[2].wait(final.at[0])

    @pl.loop(0, 2)
    def _(at):
        Arrival(links, last[0].at + at).wait(final.at[0, top])

        @pl.loop(0, 4)
        def _(step):
            for start in (0, 128):
                lines = pl.ds(pl.multiple_of(start + 64 * at + 16 * step, 16), 16)
                branch = (
                    partial[0, lines, :].astype(f32)
                    + final[0, lines, :].astype(f32)
                    + final[1, lines, :].astype(f32)
                ).astype(bf16)
                out[lines, :] = (
                    middle[lines, :].astype(f32) + rms_norm(branch, gains[2])
                ).astype(bf16)

    links.finish()


def per_device(
    queries, keys, values, gates, log_decay, norm_gain, out_weight, resid, post_mix_gain, pre_ffn_gain,
    w_gate, w_up, w_down, post_ffn_gain,
):
    f32, bf16 = jnp.float32, jnp.bfloat16
    operands = (
        queries, keys, values, gates, log_decay.T, norm_gain, out_weight, resid, post_mix_gain[None],
        pre_ffn_gain[None], w_gate, w_up, w_down.T, post_ffn_gain[None],
    )
    return pl.pallas_call(
        layer_kernel,
        out_shape=jax.ShapeDtypeStruct((256, 2048), bf16),
        in_specs=[pl.BlockSpec(memory_space=pl.ANY)] * 14,
        out_specs=pl.BlockSpec(memory_space=pltpu.VMEM),
        scratch_shapes=[
            pltpu.VMEM((4, 4, 2, 64, 1408), bf16),
            pltpu.VMEM((4, 4, 2, 64, 1408), bf16),
            pltpu.VMEM((4, 4, 1408, 128), bf16),
            pltpu.VMEM((4, 256, 2048), bf16),
            pltpu.VMEM((3, 256, 1408), bf16),
            pltpu.VMEM((4, 256, 2048), bf16),
            pltpu.VMEM((2, 128, 2048), bf16),
            pltpu.VMEM((2, 256, 2048), bf16),
            pltpu.VMEM((2, 64, 1408), bf16),
            pltpu.VMEM((1408, 128), bf16),
            pltpu.VMEM((1024, 256), bf16),
            pltpu.VMEM((1024, 256), bf16),
            pltpu.VMEM((1024, 256), bf16),
            pltpu.VMEM((1024, 256), bf16),
            pltpu.VMEM((2, 1024, 128), f32),
            pltpu.VMEM((2, 1024, 128), f32),
            pltpu.VMEM((2, 2, 144, 128), bf16),
            pltpu.VMEM((4, 144, 128), bf16),
            pltpu.VMEM((4, 144, 128), bf16),
            pltpu.VMEM((2, 128, 128), f32),
            pltpu.VMEM((4, 256, 256), bf16),
            pltpu.VMEM((4, 256, 256), bf16),
            pltpu.VMEM((128, 256), bf16),
            pltpu.VMEM((4, 256, 2048), bf16),
            pltpu.VMEM((256, 2048), f32),
            pltpu.VMEM((256, 2048), bf16),
            pltpu.VMEM((2, 1024), f32),
            pltpu.VMEM((3, 1, 2048), f32),
            pltpu.VMEM((2, 128), f32),
            pltpu.SemaphoreType.DMA((14,)),
            pltpu.SemaphoreType.DMA((SENDS,)),
            pltpu.SemaphoreType.DMA((ARRIVALS,)),
        ],
        compiler_params=pltpu.CompilerParams(
            collective_id=0, has_side_effects=True, vmem_limit_bytes=48 * 2**20
        ),
        name="layer",
    )(*(pltpu.with_memory_space_constraint(a, pltpu.HBM) for a in operands))


def solution(mesh):
    split = Mesh(mesh.devices.reshape(4, 4, 2, mesh.shape["tp"]), ("sp_0", "sp_1", "sp_2", "tp"))
    placed = (
        P(SP, "tp"),
        P(SP, "tp"),
        P(SP, "tp"),
        P(SP, "tp"),
        P(SP, "tp"),
        P("tp", None),
        P("tp", None),
        P(SP_TP, None),
        P(),
        P(),
        P(SP, "tp"),
        P(SP, "tp"),
        P("tp", SP),
        P(),
    )
    return jax.shard_map(
        per_device, mesh=split, in_specs=placed, out_specs=P(SP_TP, None), check_vma=False
    )
```

```python
import jax
import jax.numpy as jnp
from jax import lax
from jax.experimental import pallas as pl
from jax.experimental.pallas import tpu as pltpu
from jax.sharding import Mesh
from jax.sharding import PartitionSpec as P

BLOCK = 512
SP = ("sp_0", "sp_1", "sp_2")
SP_TP = ("sp_0", "sp_1", "sp_2", "tp")


EPSILON = 1e-06
MESH_ID = pl.DeviceIdType.MESH
SENDS, ARRIVALS = 32, 50
Z, Y, C, X = SP_TP


class Arrival:
    def __init__(self, links, at):
        self.links, self.at = links, at

    def wait(self, as_large):
        pltpu.make_async_remote_copy(
            src_ref=as_large,
            dst_ref=as_large,
            send_sem=self.links.send_sem.at[0],
            recv_sem=self.links.recv_sem.at[self.at],
            device_id={X: lax.rem(lax.axis_index(X) + 1, 4)},
            device_id_type=MESH_ID,
        ).wait_recv()


class Links:
    def __init__(self, send_sem, recv_sem):
        self.send_sem, self.recv_sem, self.copies, self.arrivals = send_sem, recv_sem, [], 0

    def arrival(self):
        self.arrivals += 1
        return Arrival(self, self.arrivals - 1)

    def send(self, arrival, src, dst, **where):
        at = len(self.copies)
        if at >= SENDS:
            self.copies[at - SENDS].wait_send()
        copy = pltpu.make_async_remote_copy(
            src_ref=src,
            dst_ref=dst,
            send_sem=self.send_sem.at[at % SENDS],
            recv_sem=self.recv_sem.at[arrival.at],
            device_id={axis: index for axis, index in where.items()},
            device_id_type=MESH_ID,
        )
        copy.start()
        self.copies.append(copy)

    def finish(self):
        for copy in self.copies[-SENDS:]:
            copy.wait_send()
        assert self.arrivals == ARRIVALS, self.arrivals


class PlaneGather:
    def __init__(self, links, at, first, second, here, core):
        self.links, self.at, self.first, self.second, self.core = links, at, first, second, core
        self.i, self.j = here
        self.i_up, self.i_down = lax.rem(self.i + 1, 4), lax.rem(self.i + 3, 4)
        self.j_up, self.j_down = lax.rem(self.j + 1, 4), lax.rem(self.j + 3, 4)
        self.across = links.arrival()

    def both_ways(self, axis, up, down, block_up, block_down):
        arrival = self.links.arrival()
        self.links.send(arrival, block_up, block_up, **{axis: up})
        self.links.send(arrival, block_down, block_down, **{axis: down})
        return arrival

    def own(self):
        block = self.at(self.i, self.j)
        self.came = self.both_ways(self.first, self.i_up, self.i_down, block, block)

    def pass_on(self):
        self.came.wait(self.at(pl.ds(0, 2), self.j))
        self.came = self.both_ways(
            self.first,
            self.i_up,
            self.i_down,
            self.at(self.i_down, self.j, part=0),
            self.at(self.i_up, self.j, part=1),
        )

    def give(self, j, items=pl.ds(0, 4)):
        block = self.at(items, j)
        self.links.send(self.across, block, block, **{C: 1 - self.core})

    def line(self):
        self.came.wait(self.at(self.i, self.j))
        block = self.at(pl.ds(0, 4), self.j)
        self.came = self.both_ways(self.second, self.j_up, self.j_down, block, block)

    def pass_line(self):
        self.came.wait(self.at(pl.ds(0, 4), pl.ds(0, 2)))
        self.passed = [
            self.both_ways(
                self.second,
                self.j_up,
                self.j_down,
                self.at(pl.ds(at, 1), self.j_down),
                self.at(pl.ds(2 + at, 1), self.j_up),
            )
            for at in range(2)
        ]
        self.give(self.j_down)
        self.give(self.j_up)

    def end_line(self):
        far = lax.rem(self.j + 2, 4)
        for at, arrival in enumerate(self.passed):
            arrival.wait(self.at(pl.ds(0, 2), far))
            for start in (0, 2):
                self.give(far, pl.ds(start + at, 1))

    def arrive(self):
        self.across.wait(self.at(pl.ds(0, 4), pl.ds(0, 4)))


class Ring:
    def __init__(self, links, where, own, passed, as_large):
        self.links, self.where, self.own, self.passed, self.as_large = links, where, own, passed, as_large

    def both_ways(self, pairs):
        self.came = self.links.arrival()
        for step, (src, dst) in zip((1, 3), pairs):
            self.links.send(self.came, src, dst, **self.where(step))

    def start(self):
        self.both_ways(self.own)

    def pass_on(self):
        self.came.wait(self.as_large[0])
        self.both_ways(self.passed)

    def finish(self):
        self.came.wait(self.as_large[1])


def rms_norm(values_in, gain_vec):
    widened = values_in.astype(jnp.float32)
    return (
        widened
        * lax.rsqrt(jnp.mean(widened * widened, axis=-1, keepdims=True) + EPSILON)
        * gain_vec
    )


def over_lanes(scalar):
    return jnp.broadcast_to(scalar, (1, 128))


def write_state(ref, state, decay):
    ref[pl.ds(0, 128), :] = state.astype(jnp.bfloat16)
    row = lax.broadcasted_iota(jnp.int32, (16, 128), 0)
    large = decay.astype(jnp.bfloat16).astype(jnp.float32)
    ref[pl.ds(128, 16), :] = jnp.where(row == 0, large, decay - large).astype(jnp.bfloat16)


def read_state(ref):
    both = ref[pl.ds(128, 16), :].astype(jnp.float32)
    return ref[pl.ds(0, 128), :].astype(jnp.float32), both[0:1] + both[1:2]


def followed_by(earlier, later):
    return later[1] * earlier[0] + later[0], later[1] * earlier[1]


def chosen(which, a, b):
    return jax.tree.map(lambda p, q: jnp.where(which, p, q), a, b)


def layer_kernel(
    queries, keys, values, gates, log_decay, norm_gain, out_weight, resid, mix_gain, in_gain,
    w_gate, w_up, w_down, out_gain, out,
    gate_all, up_all, down_all, rows, hidden, partial, relay, final, half_down, turned,
    q, k, v, g, retention, decayed, state_c, state_y, state_z, state_in, retained, regrouped, passing, out_all, mixed, middle, logs_in, gains, norm_in,
    local_sem, send_sem, recv_sem,
):
    f32, bf16 = jnp.float32, jnp.bfloat16
    z, y, c, x = (lax.axis_index(axis) for axis in SP_TP)
    other, x_up, x_down, x_far = 1 - c, lax.rem(x + 1, 4), lax.rem(x + 3, 4), lax.rem(x + 2, 4)
    own_half = pl.ds(pl.multiple_of(704 * c, 64), 704)
    names = ("logs", "k", "v", "gate", "up", "q", "down", "weight", "g", "resid", "mix", "in", "out", "norm")
    moves = (
        (log_decay, logs_in), (keys, k), (values, v), (w_gate, gate_all.at[z, y, c]), (w_up, up_all.at[z, y, c]), (queries, q),
        (w_down, half_down.at[c]), (out_weight, out_all.at[0]), (gates, g), (resid, middle),
        (mix_gain, gains.at[0]), (in_gain, gains.at[1]), (out_gain, gains.at[2]), (norm_gain, norm_in),
    )
    local = {
        name: pltpu.make_async_copy(src, dst, local_sem.at[at])
        for at, (name, (src, dst)) in enumerate(zip(names, moves))
    }
    for copy in local.values():
        copy.start()

    barrier = pltpu.get_barrier_semaphore()
    near = [{C: other}]
    for axis, index in ((X, x), (Y, y), (Z, z)):
        near += [{axis: lax.rem(index + step, 4)} for step in (1, 2, 3)]
    for where in near:
        pl.semaphore_signal(barrier, inc=1, device_id=where, device_id_type=MESH_ID)

    links = Links(send_sem, recv_sem)

    def gate_at(i, j, part=None):
        lines = pl.ds(0, 64) if part is None else pl.ds(32 * part, 32)
        return gate_all.at[j, i, c, lines]

    def up_at(i, j, part=None):
        lines = pl.ds(0, 64) if part is None else pl.ds(32 * part, 32)
        return up_all.at[i, j, c, lines]

    def down_lines(start, part):
        first, length = (start, 352) if part is None else (start + 176 * part, 176)
        return pl.ds(pl.multiple_of(704 * c + first, 16), length)

    wide = (
        PlaneGather(links, gate_at, Y, Z, (y, z), c),
        PlaneGather(links, up_at, Z, Y, (z, y), c),
    )
    narrow = (
        PlaneGather(
            links, lambda i, j, part=None: down_all.at[j, i, down_lines(0, part)], Y, Z, (y, z), c
        ),
        PlaneGather(
            links, lambda i, j, part=None: down_all.at[i, j, down_lines(352, part)], Z, Y, (z, y), c
        ),
    )

    along = (1 - c) * y + c * z

    def part_rows(i, part=None):
        first, length = (0, 32) if part is None else (16 * part, 16)
        return pl.ds(pl.multiple_of(128 * c + 32 * i + first, 16), length)

    def on_line(step):
        return {Y: lax.rem(y + (1 - c) * step, 4), Z: lax.rem(z + c * step, 4)}

    weight_x = Ring(
        links,
        lambda step: {X: lax.rem(x + step, 4)},
        (
            (out_all.at[0, part_rows(along)], out_all.at[2, part_rows(along)]),
            (out_all.at[0, part_rows(along)], out_all.at[1, part_rows(along)]),
        ),
        (
            (out_all.at[2, part_rows(along, 0)], out_all.at[3, part_rows(along, 0)]),
            (out_all.at[1, part_rows(along, 1)], out_all.at[3, part_rows(along, 1)]),
        ),
        (out_all.at[pl.ds(1, 2), part_rows(along)], out_all.at[3, part_rows(along)]),
    )

    def weight_ring(slots):
        own, low, high = (
            out_all.at[slots, part_rows(along)],
            out_all.at[slots, part_rows(lax.rem(along + 3, 4), 0)],
            out_all.at[slots, part_rows(lax.rem(along + 1, 4), 1)],
        )
        return Ring(
            links,
            on_line,
            ((own, own), (own, own)),
            ((low, low), (high, high)),
            (out_all.at[slots, pl.ds(0, 64)], own),
        )

    weight_far = weight_ring(pl.ds(3, 1))
    weight_rest = links.arrival()

    def send_rest(steps):
        for step in steps:
            part = part_rows(lax.rem(along + step, 4))
            for slot, target in ((2, x_up), (1, x_down)):
                links.send(weight_rest, out_all.at[0, part], out_all.at[slot, part], **{X: target})

    half_rows = pl.ds(pl.multiple_of(128 * c, 128), 128)

    scale = 128 ** (-0.5)
    at_row = lax.broadcasted_iota(jnp.int32, (BLOCK, BLOCK), 0)
    at_col = lax.broadcasted_iota(jnp.int32, (BLOCK, BLOCK), 1)
    upto = jnp.where(at_row <= at_col, 1.0, 0.0).astype(f32)
    cum_rows, cum_cols = [], []
    local["logs"].wait()
    for b in range(2):
        logs = jnp.concatenate(
            [logs_in[:, BLOCK * b : BLOCK * (b + 1)], jnp.zeros((6, BLOCK), f32)], axis=0
        )
        cum = jnp.dot(logs, upto, precision=lax.Precision.HIGHEST, preferred_element_type=f32)
        cum_rows.append(cum)
        cum_cols.append(cum.T)
    ends = [[cum_rows[b][h : h + 1, BLOCK - 1 : BLOCK] for b in range(2)] for h in range(2)]
    local["k"].wait()
    local["v"].wait()
    first_state, span = [], []
    for h in range(2):
        heads = slice(128 * h, 128 * (h + 1))
        added = []
        for b in range(2):
            lines = slice(BLOCK * b, BLOCK * (b + 1))
            to_end = jnp.exp(ends[h][b] - cum_cols[b][:, h : h + 1]) * scale
            scaled = (k[lines, heads].astype(f32) * to_end).astype(bf16)
            added.append(
                lax.dot_general(
                    scaled, v[lines, heads], (((0,), (0,)), ((), ())), preferred_element_type=f32
                )
            )
        first_state.append(added[0])
        span.append(
            (
                jnp.exp(over_lanes(ends[h][1])) * added[0] + added[1],
                jnp.exp(over_lanes(ends[h][0] + ends[h][1])),
            )
        )
        write_state(state_c.at[0, h], *span[h])
    pl.semaphore_wait(barrier, len(near))
    pair = links.arrival()
    links.send(pair, state_c.at[0], state_c.at[1], **{C: other})
    local["up"].wait()
    wide[1].own()
    local["weight"].wait()
    weight_x.start()
    send_rest((1,))
    local["down"].wait()
    swap = links.arrival()
    links.send(swap, half_down.at[c], half_down.at[c], **{C: other})
    local["gate"].wait()

    def within(h, b):
        heads, lines = slice(128 * h, 128 * (h + 1)), slice(BLOCK * b, BLOCK * (b + 1))
        col, row = cum_cols[b][:, h : h + 1], cum_rows[b][h : h + 1]
        products = lax.dot_general(
            q[lines, heads], k[lines, heads], (((1,), (1,)), ((), ())), preferred_element_type=f32
        )
        factor = jnp.where(at_row >= at_col, jnp.exp(jnp.minimum(col - row, 0.0)), 0.0)
        scores = (products * scale * factor).astype(bf16)
        result = jnp.dot(scores, v[lines, heads], preferred_element_type=f32)
        if b == 1:
            result = result + jnp.exp(col) * jnp.dot(
                q[lines, heads], first_state[h].astype(bf16), preferred_element_type=f32
            )
            col = col + ends[h][0]
        retention[h, lines, :] = result
        decayed[h, lines, :] = jnp.broadcast_to(jnp.exp(col), (BLOCK, 128))

    nothing = (jnp.zeros((128, 128), f32), jnp.ones((1, 128), f32))

    def among(slots, axis, index):
        came = links.arrival()
        for step in (2, 1, 3):
            links.send(came, slots.at[index], slots.at[index], **{axis: lax.rem(index + step, 4)})

        def fold():
            came.wait(slots.at[pl.ds(0, 3)])
            total, before = nothing, nothing
            for at in range(4):
                total = followed_by(total, read_state(slots.at[at]))
                before = chosen(at < index, total, before)
            return total, before

        return fold

    local["q"].wait()
    within(0, 0)
    pair.wait(state_c.at[1])
    partner = [read_state(state_c.at[1, h]) for h in range(2)]
    first = c == 0
    chip = [
        followed_by(chosen(first, span[h], partner[h]), chosen(first, partner[h], span[h]))
        for h in range(2)
    ]
    write_state(state_y.at[y], *chosen(first, chip[0], chip[1]))
    fold_y = among(state_y, Y, y)
    wide[0].own()
    within(0, 1)
    within(1, 0)
    line, before_y = fold_y()
    write_state(state_z.at[z], *line)
    fold_z = among(state_z, Z, z)
    swap.wait(half_down.at[other])
    turned[...] = jnp.concatenate([half_down[0], half_down[1]], axis=0).T
    down_all[z, y, own_half, :] = turned[own_half, :]
    within(1, 1)
    weight_x.pass_on()
    send_rest((2, 3))
    wide[1].pass_on()
    _, before_z = fold_z()
    state_in[c] = followed_by(before_z, before_y)[0]
    both_heads = links.arrival()
    links.send(both_heads, state_in.at[c], state_in.at[c], **{C: other})
    wide[0].pass_on()
    weight_x.finish()
    weight_far.start()
    for gather in narrow:
        gather.own()
    for name in ("g", "norm"):
        local[name].wait()
    both_heads.wait(state_in.at[other])
    entering = [
        jnp.where(first, state_in[h], partner[h][1] * state_in[h] + partner[h][0]).astype(bf16)
        for h in range(2)
    ]

    top, bottom = pl.ds(0, 128), pl.ds(128, 128)
    near_came, far_came, to_pass = (links.arrival() for _ in range(3))
    for step in (2, 1, 3, 0):
        quarter = lax.rem(x + step, 4)
        lines = pl.ds(pl.multiple_of(256 * quarter, 256), 256)
        for h in range(2):
            heads = slice(128 * h, 128 * (h + 1))
            carried = jnp.dot(q[lines, heads], entering[h], preferred_element_type=f32)
            value = retention[h, lines, :] + carried * decayed[h, lines, :]
            centered = value - jnp.mean(value, axis=-1, keepdims=True)
            variance = jnp.mean(centered * centered, axis=-1, keepdims=True)
            normed = centered * lax.rsqrt(variance + EPSILON) * norm_in[h : h + 1, :]
            retained[step, :, heads] = (jax.nn.silu(g[lines, heads].astype(f32)) * normed).astype(
                bf16
            )
        if step == 2:
            links.send(far_came, retained.at[2, top], regrouped.at[3, top], **{X: x_far})
            links.send(to_pass, retained.at[2, bottom], passing, **{X: x_down})
        elif step:
            slot = 2 if step == 1 else 1
            links.send(near_came, retained.at[step], regrouped.at[slot], **{X: quarter})
    weight_far.pass_on()
    for gather in narrow:
        gather.pass_on()
    for gather in (wide[1], wide[0]):
        gather.line()
    shared, shared_far = links.arrival(), links.arrival()
    weight_rest.wait(out_all.at[pl.ds(1, 2), pl.ds(0, 96)])
    near_half, far_half = out_all.at[pl.ds(1, 2), half_rows], out_all.at[3, half_rows]
    links.send(shared, near_half, near_half, **{C: other})
    to_pass.wait(passing)
    links.send(far_came, passing, regrouped.at[3, bottom], **{X: x_down})
    weight_far.finish()
    links.send(shared_far, far_half, far_half, **{C: other})
    for name in ("resid", "mix", "in", "out"):
        local[name].wait()
    near_came.wait(regrouped.at[pl.ds(1, 2)])
    shared.wait(out_all.at[pl.ds(1, 2), half_rows])

    def mix_part(slot, lanes):
        block = regrouped[slot] if slot else retained[0]
        part = jnp.dot(block, out_all[slot, :, lanes], preferred_element_type=f32)
        return part.astype(bf16).astype(f32)

    for j in range(8):
        lanes = slice(256 * j, 256 * (j + 1))
        mixed[:, lanes] = mix_part(0, lanes) + mix_part(1, lanes) + mix_part(2, lanes)
    far_came.wait(regrouped.at[3])
    shared_far.wait(out_all.at[3, half_rows])
    for j in range(8):
        lanes = slice(256 * j, 256 * (j + 1))
        partial[0, :, lanes] = (mixed[:, lanes] + mix_part(3, lanes)).astype(bf16)

    piece = [pl.ds(64 * at, 64) for at in range(4)]
    first_rows = [links.arrival(), links.arrival()]
    for at in range(4):

        @pl.loop(0, 2)
        def _(step):
            for start in (32 * at, 32 * at + 128):
                lines = pl.ds(pl.multiple_of(start + 16 * step, 16), 16)
                mid = (
                    middle[lines, :].astype(f32) + rms_norm(partial[0, lines, :], gains[0])
                ).astype(bf16)
                middle[lines, :] = mid
                rows[x, lines, :] = rms_norm(mid, gains[1]).astype(bf16)

        for target, start in ((x_up, 32 * at), (x_down, 32 * at + 128)):
            lines = pl.ds(start, 32)
            links.send(first_rows[at // 2], rows.at[x, lines], rows.at[x, lines], **{X: target})
    for gather in narrow:
        gather.line()
    for gather in (*wide, *narrow):
        gather.give(gather.j)
    far, nearby = links.arrival(), links.arrival()
    for at in range(2):
        first_rows[at].wait(rows.at[x, top])
        for target, source, lines in ((x_up, x_down, piece[at]), (x_down, x_up, piece[2 + at])):
            links.send(far, rows.at[source, lines], rows.at[source, lines], **{X: target})
        if at == 0:
            for gather in wide:
                gather.pass_line()
    for lines, target in ((bottom, x_up), (top, x_down)):
        links.send(nearby, rows.at[x, lines], rows.at[x, lines], **{X: target})
    for gather in narrow:
        gather.pass_line()
    for gather in wide:
        gather.end_line()
    for gather in wide:
        gather.arrive()

    def gate_up(owner, slot, tiles=range(11)):
        block = rows[owner]
        for j in tiles:
            lanes = slice(128 * j, 128 * (j + 1))
            weights = jnp.concatenate(
                [
                    gate_all[:, :, :, :, lanes].reshape(2048, 128),
                    up_all[:, :, :, :, lanes].reshape(2048, 128),
                ],
                axis=1,
            )
            both = jnp.dot(block, weights, preferred_element_type=f32)
            hidden[slot, :, lanes] = (jax.nn.silu(both[:, :128]) * both[:, 128:]).astype(bf16)

    def down(slot, to, lines=pl.ds(0, 256), extra=None, tiles=range(8)):
        block = hidden[slot, lines, :]
        for j in tiles:
            weights = jnp.concatenate(
                [down_all[j // 2, 2 * j % 4], down_all[j // 2, 2 * j % 4 + 1]], axis=1
            )
            part = jnp.dot(block, weights, preferred_element_type=f32)
            lanes = slice(256 * j, 256 * (j + 1))
            if extra is not None:
                part = part + relay[extra, :, lanes].astype(f32)
            partial[to, lines, lanes] = part.astype(bf16)

    far.wait(rows.at[x_far])
    gate_up(x_far, 2, range(6))
    for gather in narrow:
        gather.end_line()
    gate_up(x_far, 2, range(6, 11))
    for gather in narrow:
        gather.arrive()
    relay_up, relay_down = links.arrival(), links.arrival()
    for at in range(2):
        down(2, 1, tiles=range(4 * at, 4 * at + 4))
        lanes = pl.ds(1024 * at, 1024)
        links.send(relay_up, partial.at[1, top, lanes], relay.at[0, :, lanes], **{X: x_up})
        links.send(relay_down, partial.at[1, bottom, lanes], relay.at[1, :, lanes], **{X: x_down})
    nearby.wait(rows.at[x_up])
    gate_up(x_up, 0)
    down(0, 2, bottom)
    last = [links.arrival() for _ in range(5)]
    links.send(last[4], partial.at[2, bottom], final.at[0, bottom], **{X: x_up})
    gate_up(x_down, 1)
    down(1, 3, top)
    links.send(last[4], partial.at[3, top], final.at[1, top], **{X: x_down})
    gate_up(x, 2)
    relay_up.wait(relay.at[0])
    down(0, 2, top, 0)
    for at in range(4):
        lines = pl.ds(32 * at, 32)
        links.send(last[at], partial.at[2, lines], final.at[0, lines], **{X: x_up})
    relay_down.wait(relay.at[1])
    down(1, 3, bottom, 1)
    for at in range(4):
        lines = pl.ds(128 + 32 * at, 32)
        links.send(last[at], partial.at[3, lines], final.at[1, lines], **{X: x_down})
    down(2, 0)
    last[4].wait(final.at[0])

    @pl.loop(0, 4)
    def _(at):
        Arrival(links, last[0].at + at).wait(final.at[0, pl.ds(0, 64)])

        @pl.loop(0, 2)
        def _(step):
            for start in (0, 128):
                lines = pl.ds(pl.multiple_of(start + 32 * at + 16 * step, 16), 16)
                branch = (
                    partial[0, lines, :].astype(f32)
                    + final[0, lines, :].astype(f32)
                    + final[1, lines, :].astype(f32)
                ).astype(bf16)
                out[lines, :] = (
                    middle[lines, :].astype(f32) + rms_norm(branch, gains[2])
                ).astype(bf16)

    links.finish()


def per_device(
    queries, keys, values, gates, log_decay, norm_gain, out_weight, resid, post_mix_gain, pre_ffn_gain,
    w_gate, w_up, w_down, post_ffn_gain,
):
    f32, bf16 = jnp.float32, jnp.bfloat16
    operands = (
        queries, keys, values, gates, log_decay.T, norm_gain, out_weight, resid, post_mix_gain[None],
        pre_ffn_gain[None], w_gate, w_up, w_down.T, post_ffn_gain[None],
    )
    return pl.pallas_call(
        layer_kernel,
        out_shape=jax.ShapeDtypeStruct((256, 2048), bf16),
        in_specs=[pl.BlockSpec(memory_space=pl.ANY)] * 14,
        out_specs=pl.BlockSpec(memory_space=pltpu.VMEM),
        scratch_shapes=[
            pltpu.VMEM((4, 4, 2, 64, 1408), bf16),
            pltpu.VMEM((4, 4, 2, 64, 1408), bf16),
            pltpu.VMEM((4, 4, 1408, 128), bf16),
            pltpu.VMEM((4, 256, 2048), bf16),
            pltpu.VMEM((3, 256, 1408), bf16),
            pltpu.VMEM((4, 256, 2048), bf16),
            pltpu.VMEM((2, 128, 2048), bf16),
            pltpu.VMEM((2, 256, 2048), bf16),
            pltpu.VMEM((2, 64, 1408), bf16),
            pltpu.VMEM((1408, 128), bf16),
            pltpu.VMEM((1024, 256), bf16),
            pltpu.VMEM((1024, 256), bf16),
            pltpu.VMEM((1024, 256), bf16),
            pltpu.VMEM((1024, 256), bf16),
            pltpu.VMEM((2, 1024, 128), f32),
            pltpu.VMEM((2, 1024, 128), f32),
            pltpu.VMEM((2, 2, 144, 128), bf16),
            pltpu.VMEM((4, 144, 128), bf16),
            pltpu.VMEM((4, 144, 128), bf16),
            pltpu.VMEM((2, 128, 128), f32),
            pltpu.VMEM((4, 256, 256), bf16),
            pltpu.VMEM((4, 256, 256), bf16),
            pltpu.VMEM((128, 256), bf16),
            pltpu.VMEM((4, 256, 2048), bf16),
            pltpu.VMEM((256, 2048), f32),
            pltpu.VMEM((256, 2048), bf16),
            pltpu.VMEM((2, 1024), f32),
            pltpu.VMEM((3, 1, 2048), f32),
            pltpu.VMEM((2, 128), f32),
            pltpu.SemaphoreType.DMA((14,)),
            pltpu.SemaphoreType.DMA((SENDS,)),
            pltpu.SemaphoreType.DMA((ARRIVALS,)),
        ],
        compiler_params=pltpu.CompilerParams(
            collective_id=0, has_side_effects=True, vmem_limit_bytes=48 * 2**20
        ),
        name="layer",
    )(*(pltpu.with_memory_space_constraint(a, pltpu.HBM) for a in operands))


def solution(mesh):
    split = Mesh(mesh.devices.reshape(4, 4, 2, mesh.shape["tp"]), ("sp_0", "sp_1", "sp_2", "tp"))
    placed = (
        P(SP, "tp"),
        P(SP, "tp"),
        P(SP, "tp"),
        P(SP, "tp"),
        P(SP, "tp"),
        P("tp", None),
        P("tp", None),
        P(SP_TP, None),
        P(),
        P(),
        P(SP, "tp"),
        P(SP, "tp"),
        P("tp", SP),
        P(),
    )
    return jax.shard_map(
        per_device, mesh=split, in_specs=placed, out_specs=P(SP_TP, None), check_vma=False
    )
```

```python
import jax
import jax.numpy as jnp
from jax import lax
from jax.experimental import pallas as pl
from jax.experimental.pallas import tpu as pltpu
from jax.sharding import Mesh
from jax.sharding import PartitionSpec as P

BLOCK = 512
SP = ("sp_0", "sp_1", "sp_2")
SP_TP = ("sp_0", "sp_1", "sp_2", "tp")


EPSILON = 1e-06
MESH_ID = pl.DeviceIdType.MESH
SENDS, ARRIVALS = 32, 50
Z, Y, C, X = SP_TP


class Arrival:
    def __init__(self, links, at):
        self.links, self.at = links, at

    def wait(self, as_large):
        pltpu.make_async_remote_copy(
            src_ref=as_large,
            dst_ref=as_large,
            send_sem=self.links.send_sem.at[0],
            recv_sem=self.links.recv_sem.at[self.at],
            device_id={X: lax.rem(lax.axis_index(X) + 1, 4)},
            device_id_type=MESH_ID,
        ).wait_recv()


class Links:
    def __init__(self, send_sem, recv_sem):
        self.send_sem, self.recv_sem, self.copies, self.arrivals = send_sem, recv_sem, [], 0

    def arrival(self):
        self.arrivals += 1
        return Arrival(self, self.arrivals - 1)

    def send(self, arrival, src, dst, **where):
        at = len(self.copies)
        if at >= SENDS:
            self.copies[at - SENDS].wait_send()
        copy = pltpu.make_async_remote_copy(
            src_ref=src,
            dst_ref=dst,
            send_sem=self.send_sem.at[at % SENDS],
            recv_sem=self.recv_sem.at[arrival.at],
            device_id={axis: index for axis, index in where.items()},
            device_id_type=MESH_ID,
        )
        copy.start()
        self.copies.append(copy)

    def finish(self):
        for copy in self.copies[-SENDS:]:
            copy.wait_send()
        assert self.arrivals == ARRIVALS, self.arrivals


class PlaneGather:
    def __init__(self, links, at, first, second, here, core):
        self.links, self.at, self.first, self.second, self.core = links, at, first, second, core
        self.i, self.j = here
        self.i_up, self.i_down = lax.rem(self.i + 1, 4), lax.rem(self.i + 3, 4)
        self.j_up, self.j_down = lax.rem(self.j + 1, 4), lax.rem(self.j + 3, 4)
        self.across = links.arrival()

    def both_ways(self, axis, up, down, block_up, block_down):
        arrival = self.links.arrival()
        self.links.send(arrival, block_up, block_up, **{axis: up})
        self.links.send(arrival, block_down, block_down, **{axis: down})
        return arrival

    def own(self):
        block = self.at(self.i, self.j)
        self.came = self.both_ways(self.first, self.i_up, self.i_down, block, block)

    def pass_on(self):
        self.came.wait(self.at(pl.ds(0, 2), self.j))
        self.came = self.both_ways(
            self.first,
            self.i_up,
            self.i_down,
            self.at(self.i_down, self.j, part=0),
            self.at(self.i_up, self.j, part=1),
        )

    def give(self, j, items=pl.ds(0, 4)):
        block = self.at(items, j)
        self.links.send(self.across, block, block, **{C: 1 - self.core})

    def line(self):
        self.came.wait(self.at(self.i, self.j))
        block = self.at(pl.ds(0, 4), self.j)
        self.came = self.both_ways(self.second, self.j_up, self.j_down, block, block)

    def pass_line(self):
        self.came.wait(self.at(pl.ds(0, 4), pl.ds(0, 2)))
        self.passed = [
            self.both_ways(
                self.second,
                self.j_up,
                self.j_down,
                self.at(pl.ds(at, 1), self.j_down),
                self.at(pl.ds(2 + at, 1), self.j_up),
            )
            for at in range(2)
        ]
        self.give(self.j_down)
        self.give(self.j_up)

    def end_line(self, at):
        far = lax.rem(self.j + 2, 4)
        self.passed[at].wait(self.at(pl.ds(0, 2), far))
        for start in (0, 2):
            self.give(far, pl.ds(start + at, 1))

    def arrive(self):
        self.across.wait(self.at(pl.ds(0, 4), pl.ds(0, 4)))


class Ring:
    def __init__(self, links, where, own, passed, as_large):
        self.links, self.where, self.own, self.passed, self.as_large = links, where, own, passed, as_large

    def both_ways(self, pairs):
        self.came = self.links.arrival()
        for step, (src, dst) in zip((1, 3), pairs):
            self.links.send(self.came, src, dst, **self.where(step))

    def start(self):
        self.both_ways(self.own)

    def pass_on(self):
        self.came.wait(self.as_large[0])
        self.both_ways(self.passed)

    def finish(self):
        self.came.wait(self.as_large[1])


def rms_norm(values_in, gain_vec):
    widened = values_in.astype(jnp.float32)
    return (
        widened
        * lax.rsqrt(jnp.mean(widened * widened, axis=-1, keepdims=True) + EPSILON)
        * gain_vec
    )


def over_lanes(scalar):
    return jnp.broadcast_to(scalar, (1, 128))


def write_state(ref, state, decay):
    ref[pl.ds(0, 128), :] = state.astype(jnp.bfloat16)
    row = lax.broadcasted_iota(jnp.int32, (16, 128), 0)
    large = decay.astype(jnp.bfloat16).astype(jnp.float32)
    ref[pl.ds(128, 16), :] = jnp.where(row == 0, large, decay - large).astype(jnp.bfloat16)


def read_state(ref):
    both = ref[pl.ds(128, 16), :].astype(jnp.float32)
    return ref[pl.ds(0, 128), :].astype(jnp.float32), both[0:1] + both[1:2]


def followed_by(earlier, later):
    return later[1] * earlier[0] + later[0], later[1] * earlier[1]


def chosen(which, a, b):
    return jax.tree.map(lambda p, q: jnp.where(which, p, q), a, b)


def layer_kernel(
    queries, keys, values, gates, log_decay, norm_gain, out_weight, resid, mix_gain, in_gain,
    w_gate, w_up, w_down, out_gain, out,
    gate_all, up_all, down_all, rows, hidden, partial, relay, final, half_down, turned,
    q, k, v, g, retention, decayed, state_c, state_y, state_z, state_in, retained, regrouped, passing, out_all, mixed, middle, logs_in, gains, norm_in,
    local_sem, send_sem, recv_sem,
):
    f32, bf16 = jnp.float32, jnp.bfloat16
    z, y, c, x = (lax.axis_index(axis) for axis in SP_TP)
    other, x_up, x_down, x_far = 1 - c, lax.rem(x + 1, 4), lax.rem(x + 3, 4), lax.rem(x + 2, 4)
    own_half = pl.ds(pl.multiple_of(704 * c, 64), 704)
    names = ("logs", "k", "v", "gate", "up", "q", "down", "weight", "g", "resid", "mix", "in", "out", "norm")
    moves = (
        (log_decay, logs_in), (keys, k), (values, v), (w_gate, gate_all.at[z, y, c]), (w_up, up_all.at[z, y, c]), (queries, q),
        (w_down, half_down.at[c]), (out_weight, out_all.at[0]), (gates, g), (resid, middle),
        (mix_gain, gains.at[0]), (in_gain, gains.at[1]), (out_gain, gains.at[2]), (norm_gain, norm_in),
    )
    local = {
        name: pltpu.make_async_copy(src, dst, local_sem.at[at])
        for at, (name, (src, dst)) in enumerate(zip(names, moves))
    }
    for copy in local.values():
        copy.start()

    barrier = pltpu.get_barrier_semaphore()
    near = [{C: other}]
    for axis, index in ((X, x), (Y, y), (Z, z)):
        near += [{axis: lax.rem(index + step, 4)} for step in (1, 2, 3)]
    for where in near:
        pl.semaphore_signal(barrier, inc=1, device_id=where, device_id_type=MESH_ID)

    links = Links(send_sem, recv_sem)

    def gate_at(i, j, part=None):
        lines = pl.ds(0, 64) if part is None else pl.ds(32 * part, 32)
        return gate_all.at[j, i, c, lines]

    def up_at(i, j, part=None):
        lines = pl.ds(0, 64) if part is None else pl.ds(32 * part, 32)
        return up_all.at[i, j, c, lines]

    def down_lines(start, part):
        first, length = (start, 352) if part is None else (start + 176 * part, 176)
        return pl.ds(pl.multiple_of(704 * c + first, 16), length)

    wide = (
        PlaneGather(links, gate_at, Y, Z, (y, z), c),
        PlaneGather(links, up_at, Z, Y, (z, y), c),
    )
    narrow = (
        PlaneGather(
            links, lambda i, j, part=None: down_all.at[j, i, down_lines(0, part)], Y, Z, (y, z), c
        ),
        PlaneGather(
            links, lambda i, j, part=None: down_all.at[i, j, down_lines(352, part)], Z, Y, (z, y), c
        ),
    )

    along = (1 - c) * y + c * z

    def part_rows(i, part=None):
        first, length = (0, 32) if part is None else (16 * part, 16)
        return pl.ds(pl.multiple_of(128 * c + 32 * i + first, 16), length)

    def on_line(step):
        return {Y: lax.rem(y + (1 - c) * step, 4), Z: lax.rem(z + c * step, 4)}

    weight_x = Ring(
        links,
        lambda step: {X: lax.rem(x + step, 4)},
        (
            (out_all.at[0, part_rows(along)], out_all.at[2, part_rows(along)]),
            (out_all.at[0, part_rows(along)], out_all.at[1, part_rows(along)]),
        ),
        (
            (out_all.at[2, part_rows(along, 0)], out_all.at[3, part_rows(along, 0)]),
            (out_all.at[1, part_rows(along, 1)], out_all.at[3, part_rows(along, 1)]),
        ),
        (out_all.at[pl.ds(1, 2), part_rows(along)], out_all.at[3, part_rows(along)]),
    )

    def weight_ring(slots):
        own, low, high = (
            out_all.at[slots, part_rows(along)],
            out_all.at[slots, part_rows(lax.rem(along + 3, 4), 0)],
            out_all.at[slots, part_rows(lax.rem(along + 1, 4), 1)],
        )
        return Ring(
            links,
            on_line,
            ((own, own), (own, own)),
            ((low, low), (high, high)),
            (out_all.at[slots, pl.ds(0, 64)], own),
        )

    weight_far = weight_ring(pl.ds(3, 1))
    weight_rest = links.arrival()

    def send_rest(steps):
        for step in steps:
            part = part_rows(lax.rem(along + step, 4))
            for slot, target in ((2, x_up), (1, x_down)):
                links.send(weight_rest, out_all.at[0, part], out_all.at[slot, part], **{X: target})

    half_rows = pl.ds(pl.multiple_of(128 * c, 128), 128)

    scale = 128 ** (-0.5)
    at_row = lax.broadcasted_iota(jnp.int32, (BLOCK, BLOCK), 0)
    at_col = lax.broadcasted_iota(jnp.int32, (BLOCK, BLOCK), 1)
    upto = jnp.where(at_row <= at_col, 1.0, 0.0).astype(f32)
    cum_rows, cum_cols = [], []
    local["logs"].wait()
    for b in range(2):
        logs = jnp.concatenate(
            [logs_in[:, BLOCK * b : BLOCK * (b + 1)], jnp.zeros((6, BLOCK), f32)], axis=0
        )
        cum = jnp.dot(logs, upto, precision=lax.Precision.HIGHEST, preferred_element_type=f32)
        cum_rows.append(cum)
        cum_cols.append(cum.T)
    ends = [[cum_rows[b][h : h + 1, BLOCK - 1 : BLOCK] for b in range(2)] for h in range(2)]
    local["k"].wait()
    local["v"].wait()
    first_state, span = [], []
    for h in range(2):
        heads = slice(128 * h, 128 * (h + 1))
        added = []
        for b in range(2):
            lines = slice(BLOCK * b, BLOCK * (b + 1))
            to_end = jnp.exp(ends[h][b] - cum_cols[b][:, h : h + 1]) * scale
            scaled = (k[lines, heads].astype(f32) * to_end).astype(bf16)
            added.append(
                lax.dot_general(
                    scaled, v[lines, heads], (((0,), (0,)), ((), ())), preferred_element_type=f32
                )
            )
        first_state.append(added[0])
        span.append(
            (
                jnp.exp(over_lanes(ends[h][1])) * added[0] + added[1],
                jnp.exp(over_lanes(ends[h][0] + ends[h][1])),
            )
        )
        write_state(state_c.at[0, h], *span[h])
    pl.semaphore_wait(barrier, len(near))
    pair = links.arrival()
    links.send(pair, state_c.at[0], state_c.at[1], **{C: other})
    local["up"].wait()
    wide[1].own()
    local["weight"].wait()
    weight_x.start()
    send_rest((1,))
    local["down"].wait()
    swap = links.arrival()
    links.send(swap, half_down.at[c], half_down.at[c], **{C: other})
    local["gate"].wait()

    def within(h, b):
        heads, lines = slice(128 * h, 128 * (h + 1)), slice(BLOCK * b, BLOCK * (b + 1))
        col, row = cum_cols[b][:, h : h + 1], cum_rows[b][h : h + 1]
        products = lax.dot_general(
            q[lines, heads], k[lines, heads], (((1,), (1,)), ((), ())), preferred_element_type=f32
        )
        factor = jnp.where(at_row >= at_col, jnp.exp(jnp.minimum(col - row, 0.0)), 0.0)
        scores = (products * scale * factor).astype(bf16)
        result = jnp.dot(scores, v[lines, heads], preferred_element_type=f32)
        if b == 1:
            result = result + jnp.exp(col) * jnp.dot(
                q[lines, heads], first_state[h].astype(bf16), preferred_element_type=f32
            )
            col = col + ends[h][0]
        retention[h, lines, :] = result
        decayed[h, lines, :] = jnp.broadcast_to(jnp.exp(col), (BLOCK, 128))

    nothing = (jnp.zeros((128, 128), f32), jnp.ones((1, 128), f32))

    def among(slots, axis, index):
        came = links.arrival()
        for step in (2, 1, 3):
            links.send(came, slots.at[index], slots.at[index], **{axis: lax.rem(index + step, 4)})

        def fold():
            came.wait(slots.at[pl.ds(0, 3)])
            total, before = nothing, nothing
            for at in range(4):
                total = followed_by(total, read_state(slots.at[at]))
                before = chosen(at < index, total, before)
            return total, before

        return fold

    local["q"].wait()
    within(0, 0)
    pair.wait(state_c.at[1])
    partner = [read_state(state_c.at[1, h]) for h in range(2)]
    first = c == 0
    chip = [
        followed_by(chosen(first, span[h], partner[h]), chosen(first, partner[h], span[h]))
        for h in range(2)
    ]
    write_state(state_y.at[y], *chosen(first, chip[0], chip[1]))
    fold_y = among(state_y, Y, y)
    wide[0].own()
    within(0, 1)
    within(1, 0)
    line, before_y = fold_y()
    write_state(state_z.at[z], *line)
    fold_z = among(state_z, Z, z)
    swap.wait(half_down.at[other])
    turned[...] = jnp.concatenate([half_down[0], half_down[1]], axis=0).T
    down_all[z, y, own_half, :] = turned[own_half, :]
    within(1, 1)
    weight_x.pass_on()
    send_rest((2, 3))
    wide[1].pass_on()
    _, before_z = fold_z()
    state_in[c] = followed_by(before_z, before_y)[0]
    both_heads = links.arrival()
    links.send(both_heads, state_in.at[c], state_in.at[c], **{C: other})
    wide[0].pass_on()
    weight_x.finish()
    weight_far.start()
    for gather in narrow:
        gather.own()
    for name in ("g", "norm"):
        local[name].wait()
    both_heads.wait(state_in.at[other])
    entering = [
        jnp.where(first, state_in[h], partner[h][1] * state_in[h] + partner[h][0]).astype(bf16)
        for h in range(2)
    ]

    top, bottom = pl.ds(0, 128), pl.ds(128, 128)
    near_came, far_came, to_pass = (links.arrival() for _ in range(3))
    for step in (2, 1, 3, 0):
        quarter = lax.rem(x + step, 4)
        lines = pl.ds(pl.multiple_of(256 * quarter, 256), 256)
        for h in range(2):
            heads = slice(128 * h, 128 * (h + 1))
            carried = jnp.dot(q[lines, heads], entering[h], preferred_element_type=f32)
            value = retention[h, lines, :] + carried * decayed[h, lines, :]
            centered = value - jnp.mean(value, axis=-1, keepdims=True)
            variance = jnp.mean(centered * centered, axis=-1, keepdims=True)
            normed = centered * lax.rsqrt(variance + EPSILON) * norm_in[h : h + 1, :]
            retained[step, :, heads] = (jax.nn.silu(g[lines, heads].astype(f32)) * normed).astype(
                bf16
            )
        if step == 2:
            links.send(far_came, retained.at[2, top], regrouped.at[3, top], **{X: x_far})
            links.send(to_pass, retained.at[2, bottom], passing, **{X: x_down})
        elif step:
            slot = 2 if step == 1 else 1
            links.send(near_came, retained.at[step], regrouped.at[slot], **{X: quarter})
    weight_far.pass_on()
    for gather in narrow:
        gather.pass_on()
    for gather in (wide[1], wide[0]):
        gather.line()
    shared, shared_far = links.arrival(), links.arrival()
    weight_rest.wait(out_all.at[pl.ds(1, 2), pl.ds(0, 96)])
    near_half, far_half = out_all.at[pl.ds(1, 2), half_rows], out_all.at[3, half_rows]
    links.send(shared, near_half, near_half, **{C: other})
    to_pass.wait(passing)
    links.send(far_came, passing, regrouped.at[3, bottom], **{X: x_down})
    weight_far.finish()
    links.send(shared_far, far_half, far_half, **{C: other})
    for name in ("resid", "mix", "in", "out"):
        local[name].wait()
    near_came.wait(regrouped.at[pl.ds(1, 2)])
    shared.wait(out_all.at[pl.ds(1, 2), half_rows])

    def mix_part(slot, lanes):
        block = regrouped[slot] if slot else retained[0]
        part = jnp.dot(block, out_all[slot, :, lanes], preferred_element_type=f32)
        return part.astype(bf16).astype(f32)

    for j in range(8):
        lanes = slice(256 * j, 256 * (j + 1))
        mixed[:, lanes] = mix_part(0, lanes) + mix_part(1, lanes) + mix_part(2, lanes)
    far_came.wait(regrouped.at[3])
    shared_far.wait(out_all.at[3, half_rows])
    for j in range(8):
        lanes = slice(256 * j, 256 * (j + 1))
        partial[0, :, lanes] = (mixed[:, lanes] + mix_part(3, lanes)).astype(bf16)

    piece = [pl.ds(64 * at, 64) for at in range(4)]
    first_rows = [links.arrival(), links.arrival()]
    for at in range(4):

        @pl.loop(0, 2)
        def _(step):
            for start in (32 * at, 32 * at + 128):
                lines = pl.ds(pl.multiple_of(start + 16 * step, 16), 16)
                mid = (
                    middle[lines, :].astype(f32) + rms_norm(partial[0, lines, :], gains[0])
                ).astype(bf16)
                middle[lines, :] = mid
                rows[x, lines, :] = rms_norm(mid, gains[1]).astype(bf16)

        for target, start in ((x_up, 32 * at), (x_down, 32 * at + 128)):
            lines = pl.ds(start, 32)
            links.send(first_rows[at // 2], rows.at[x, lines], rows.at[x, lines], **{X: target})
    for gather in narrow:
        gather.line()
    for gather in (*wide, *narrow):
        gather.give(gather.j)
    far, nearby = links.arrival(), links.arrival()
    for at in range(2):
        first_rows[at].wait(rows.at[x, top])
        for target, source, lines in ((x_up, x_down, piece[at]), (x_down, x_up, piece[2 + at])):
            links.send(far, rows.at[source, lines], rows.at[source, lines], **{X: target})
        if at == 0:
            for gather in wide:
                gather.pass_line()
    for lines, target in ((bottom, x_up), (top, x_down)):
        links.send(nearby, rows.at[x, lines], rows.at[x, lines], **{X: target})
    for gather in narrow:
        gather.pass_line()
    for at in range(2):
        for gather in wide:
            gather.end_line(at)
    for gather in wide:
        gather.arrive()

    def gate_up(owner, slot, tiles=range(11)):
        block = rows[owner]
        for j in tiles:
            lanes = slice(128 * j, 128 * (j + 1))
            weights = jnp.concatenate(
                [
                    gate_all[:, :, :, :, lanes].reshape(2048, 128),
                    up_all[:, :, :, :, lanes].reshape(2048, 128),
                ],
                axis=1,
            )
            both = jnp.dot(block, weights, preferred_element_type=f32)
            hidden[slot, :, lanes] = (jax.nn.silu(both[:, :128]) * both[:, 128:]).astype(bf16)

    def down(slot, to, lines=pl.ds(0, 256), extra=None, tiles=range(8)):
        block = hidden[slot, lines, :]
        for j in tiles:
            weights = jnp.concatenate(
                [down_all[j // 2, 2 * j % 4], down_all[j // 2, 2 * j % 4 + 1]], axis=1
            )
            part = jnp.dot(block, weights, preferred_element_type=f32)
            lanes = slice(256 * j, 256 * (j + 1))
            if extra is not None:
                part = part + relay[extra, :, lanes].astype(f32)
            partial[to, lines, lanes] = part.astype(bf16)

    far.wait(rows.at[x_far])
    gate_up(x_far, 2, range(3))
    for at in range(2):
        for gather in narrow:
            gather.end_line(at)
    gate_up(x_far, 2, range(3, 11))
    for gather in narrow:
        gather.arrive()
    relay_up, relay_down = links.arrival(), links.arrival()
    for at in range(2):
        down(2, 1, tiles=range(4 * at, 4 * at + 4))
        lanes = pl.ds(1024 * at, 1024)
        links.send(relay_up, partial.at[1, top, lanes], relay.at[0, :, lanes], **{X: x_up})
        links.send(relay_down, partial.at[1, bottom, lanes], relay.at[1, :, lanes], **{X: x_down})
    nearby.wait(rows.at[x_up])
    gate_up(x_up, 0)
    down(0, 2, bottom)
    last = [links.arrival() for _ in range(5)]
    links.send(last[4], partial.at[2, bottom], final.at[0, bottom], **{X: x_up})
    gate_up(x_down, 1)
    down(1, 3, top)
    links.send(last[4], partial.at[3, top], final.at[1, top], **{X: x_down})
    gate_up(x, 2)
    relay_up.wait(relay.at[0])
    down(0, 2, top, 0)
    for at in range(4):
        lines = pl.ds(32 * at, 32)
        links.send(last[at], partial.at[2, lines], final.at[0, lines], **{X: x_up})
    relay_down.wait(relay.at[1])
    down(1, 3, bottom, 1)
    for at in range(4):
        lines = pl.ds(128 + 32 * at, 32)
        links.send(last[at], partial.at[3, lines], final.at[1, lines], **{X: x_down})
    down(2, 0)
    last[4].wait(final.at[0])

    @pl.loop(0, 4)
    def _(at):
        Arrival(links, last[0].at + at).wait(final.at[0, pl.ds(0, 64)])

        @pl.loop(0, 2)
        def _(step):
            for start in (0, 128):
                lines = pl.ds(pl.multiple_of(start + 32 * at + 16 * step, 16), 16)
                branch = (
                    partial[0, lines, :].astype(f32)
                    + final[0, lines, :].astype(f32)
                    + final[1, lines, :].astype(f32)
                ).astype(bf16)
                out[lines, :] = (
                    middle[lines, :].astype(f32) + rms_norm(branch, gains[2])
                ).astype(bf16)

    links.finish()


def per_device(
    queries, keys, values, gates, log_decay, norm_gain, out_weight, resid, post_mix_gain, pre_ffn_gain,
    w_gate, w_up, w_down, post_ffn_gain,
):
    f32, bf16 = jnp.float32, jnp.bfloat16
    operands = (
        queries, keys, values, gates, log_decay.T, norm_gain, out_weight, resid, post_mix_gain[None],
        pre_ffn_gain[None], w_gate, w_up, w_down.T, post_ffn_gain[None],
    )
    return pl.pallas_call(
        layer_kernel,
        out_shape=jax.ShapeDtypeStruct((256, 2048), bf16),
        in_specs=[pl.BlockSpec(memory_space=pl.ANY)] * 14,
        out_specs=pl.BlockSpec(memory_space=pltpu.VMEM),
        scratch_shapes=[
            pltpu.VMEM((4, 4, 2, 64, 1408), bf16),
            pltpu.VMEM((4, 4, 2, 64, 1408), bf16),
            pltpu.VMEM((4, 4, 1408, 128), bf16),
            pltpu.VMEM((4, 256, 2048), bf16),
            pltpu.VMEM((3, 256, 1408), bf16),
            pltpu.VMEM((4, 256, 2048), bf16),
            pltpu.VMEM((2, 128, 2048), bf16),
            pltpu.VMEM((2, 256, 2048), bf16),
            pltpu.VMEM((2, 64, 1408), bf16),
            pltpu.VMEM((1408, 128), bf16),
            pltpu.VMEM((1024, 256), bf16),
            pltpu.VMEM((1024, 256), bf16),
            pltpu.VMEM((1024, 256), bf16),
            pltpu.VMEM((1024, 256), bf16),
            pltpu.VMEM((2, 1024, 128), f32),
            pltpu.VMEM((2, 1024, 128), f32),
            pltpu.VMEM((2, 2, 144, 128), bf16),
            pltpu.VMEM((4, 144, 128), bf16),
            pltpu.VMEM((4, 144, 128), bf16),
            pltpu.VMEM((2, 128, 128), f32),
            pltpu.VMEM((4, 256, 256), bf16),
            pltpu.VMEM((4, 256, 256), bf16),
            pltpu.VMEM((128, 256), bf16),
            pltpu.VMEM((4, 256, 2048), bf16),
            pltpu.VMEM((256, 2048), f32),
            pltpu.VMEM((256, 2048), bf16),
            pltpu.VMEM((2, 1024), f32),
            pltpu.VMEM((3, 1, 2048), f32),
            pltpu.VMEM((2, 128), f32),
            pltpu.SemaphoreType.DMA((14,)),
            pltpu.SemaphoreType.DMA((SENDS,)),
            pltpu.SemaphoreType.DMA((ARRIVALS,)),
        ],
        compiler_params=pltpu.CompilerParams(
            collective_id=0, has_side_effects=True, vmem_limit_bytes=48 * 2**20
        ),
        name="layer",
    )(*(pltpu.with_memory_space_constraint(a, pltpu.HBM) for a in operands))


def solution(mesh):
    split = Mesh(mesh.devices.reshape(4, 4, 2, mesh.shape["tp"]), ("sp_0", "sp_1", "sp_2", "tp"))
    placed = (
        P(SP, "tp"),
        P(SP, "tp"),
        P(SP, "tp"),
        P(SP, "tp"),
        P(SP, "tp"),
        P("tp", None),
        P("tp", None),
        P(SP_TP, None),
        P(),
        P(),
        P(SP, "tp"),
        P(SP, "tp"),
        P("tp", SP),
        P(),
    )
    return jax.shard_map(
        per_device, mesh=split, in_specs=placed, out_specs=P(SP_TP, None), check_vma=False
    )
```

```python
import jax
import jax.numpy as jnp
from jax import lax
from jax.experimental import pallas as pl
from jax.experimental.pallas import tpu as pltpu
from jax.sharding import Mesh
from jax.sharding import PartitionSpec as P

BLOCK = 512
SP = ("sp_0", "sp_1", "sp_2")
SP_TP = ("sp_0", "sp_1", "sp_2", "tp")


EPSILON = 1e-06
MESH_ID = pl.DeviceIdType.MESH
SENDS, ARRIVALS = 32, 50
Z, Y, C, X = SP_TP


class Arrival:
    def __init__(self, links, at):
        self.links, self.at = links, at

    def wait(self, as_large):
        pltpu.make_async_remote_copy(
            src_ref=as_large,
            dst_ref=as_large,
            send_sem=self.links.send_sem.at[0],
            recv_sem=self.links.recv_sem.at[self.at],
            device_id={X: lax.rem(lax.axis_index(X) + 1, 4)},
            device_id_type=MESH_ID,
        ).wait_recv()


class Links:
    def __init__(self, send_sem, recv_sem):
        self.send_sem, self.recv_sem, self.copies, self.arrivals = send_sem, recv_sem, [], 0

    def arrival(self):
        self.arrivals += 1
        return Arrival(self, self.arrivals - 1)

    def send(self, arrival, src, dst, **where):
        at = len(self.copies)
        if at >= SENDS:
            self.copies[at - SENDS].wait_send()
        copy = pltpu.make_async_remote_copy(
            src_ref=src,
            dst_ref=dst,
            send_sem=self.send_sem.at[at % SENDS],
            recv_sem=self.recv_sem.at[arrival.at],
            device_id={axis: index for axis, index in where.items()},
            device_id_type=MESH_ID,
        )
        copy.start()
        self.copies.append(copy)

    def finish(self):
        for copy in self.copies[-SENDS:]:
            copy.wait_send()
        assert self.arrivals == ARRIVALS, self.arrivals


class PlaneGather:
    def __init__(self, links, at, first, second, here, core):
        self.links, self.at, self.first, self.second, self.core = links, at, first, second, core
        self.i, self.j = here
        self.i_up, self.i_down = lax.rem(self.i + 1, 4), lax.rem(self.i + 3, 4)
        self.j_up, self.j_down = lax.rem(self.j + 1, 4), lax.rem(self.j + 3, 4)
        self.across = links.arrival()

    def both_ways(self, axis, up, down, block_up, block_down):
        arrival = self.links.arrival()
        self.links.send(arrival, block_up, block_up, **{axis: up})
        self.links.send(arrival, block_down, block_down, **{axis: down})
        return arrival

    def own(self):
        block = self.at(self.i, self.j)
        self.came = self.both_ways(self.first, self.i_up, self.i_down, block, block)

    def pass_on(self):
        self.came.wait(self.at(pl.ds(0, 2), self.j))
        self.came = self.both_ways(
            self.first,
            self.i_up,
            self.i_down,
            self.at(self.i_down, self.j, part=0),
            self.at(self.i_up, self.j, part=1),
        )

    def give(self, j, items=pl.ds(0, 4)):
        block = self.at(items, j)
        self.links.send(self.across, block, block, **{C: 1 - self.core})

    def line(self):
        self.came.wait(self.at(self.i, self.j))
        block = self.at(pl.ds(0, 4), self.j)
        self.came = self.both_ways(self.second, self.j_up, self.j_down, block, block)

    def pass_line(self):
        self.came.wait(self.at(pl.ds(0, 4), pl.ds(0, 2)))
        self.passed = [
            self.both_ways(
                self.second,
                self.j_up,
                self.j_down,
                self.at(pl.ds(at, 1), self.j_down),
                self.at(pl.ds(2 + at, 1), self.j_up),
            )
            for at in range(2)
        ]
        self.give(self.j_down)
        self.give(self.j_up)

    def end_line(self, at):
        far = lax.rem(self.j + 2, 4)
        self.passed[at].wait(self.at(pl.ds(0, 2), far))
        for start in (0, 2):
            self.give(far, pl.ds(start + at, 1))

    def arrive(self):
        self.across.wait(self.at(pl.ds(0, 4), pl.ds(0, 4)))


class Ring:
    def __init__(self, links, where, own, passed, as_large):
        self.links, self.where, self.own, self.passed, self.as_large = links, where, own, passed, as_large

    def both_ways(self, pairs):
        self.came = self.links.arrival()
        for step, (src, dst) in zip((1, 3), pairs):
            self.links.send(self.came, src, dst, **self.where(step))

    def start(self):
        self.both_ways(self.own)

    def pass_on(self):
        self.came.wait(self.as_large[0])
        self.both_ways(self.passed)

    def finish(self):
        self.came.wait(self.as_large[1])


def rms_norm(values_in, gain_vec):
    widened = values_in.astype(jnp.float32)
    return (
        widened
        * lax.rsqrt(jnp.mean(widened * widened, axis=-1, keepdims=True) + EPSILON)
        * gain_vec
    )


def over_lanes(scalar):
    return jnp.broadcast_to(scalar, (1, 128))


def write_state(ref, state, decay):
    ref[pl.ds(0, 128), :] = state.astype(jnp.bfloat16)
    row = lax.broadcasted_iota(jnp.int32, (16, 128), 0)
    large = decay.astype(jnp.bfloat16).astype(jnp.float32)
    ref[pl.ds(128, 16), :] = jnp.where(row == 0, large, decay - large).astype(jnp.bfloat16)


def read_state(ref):
    both = ref[pl.ds(128, 16), :].astype(jnp.float32)
    return ref[pl.ds(0, 128), :].astype(jnp.float32), both[0:1] + both[1:2]


def followed_by(earlier, later):
    return later[1] * earlier[0] + later[0], later[1] * earlier[1]


def chosen(which, a, b):
    return jax.tree.map(lambda p, q: jnp.where(which, p, q), a, b)


def layer_kernel(
    queries, keys, values, gates, log_decay, norm_gain, out_weight, resid, mix_gain, in_gain,
    w_gate, w_up, w_down, out_gain, out,
    gate_all, up_all, down_all, rows, hidden, partial, relay, final, half_down, turned,
    q, k, v, g, retention, decayed, state_c, state_y, state_z, state_in, retained, regrouped, passing, out_all, mixed, middle, logs_in, gains, norm_in,
    local_sem, send_sem, recv_sem,
):
    f32, bf16 = jnp.float32, jnp.bfloat16
    z, y, c, x = (lax.axis_index(axis) for axis in SP_TP)
    other, x_up, x_down, x_far = 1 - c, lax.rem(x + 1, 4), lax.rem(x + 3, 4), lax.rem(x + 2, 4)
    own_half = pl.ds(pl.multiple_of(704 * c, 64), 704)
    names = ("logs", "k", "v", "gate", "up", "q", "down", "weight", "g", "resid", "mix", "in", "out", "norm")
    moves = (
        (log_decay, logs_in), (keys, k), (values, v), (w_gate, gate_all.at[z, y, c]), (w_up, up_all.at[z, y, c]), (queries, q),
        (w_down, half_down.at[c]), (out_weight, out_all.at[0]), (gates, g), (resid, middle),
        (mix_gain, gains.at[0]), (in_gain, gains.at[1]), (out_gain, gains.at[2]), (norm_gain, norm_in),
    )
    local = {
        name: pltpu.make_async_copy(src, dst, local_sem.at[at])
        for at, (name, (src, dst)) in enumerate(zip(names, moves))
    }
    for copy in local.values():
        copy.start()

    barrier = pltpu.get_barrier_semaphore()
    near = [{C: other}]
    for axis, index in ((X, x), (Y, y), (Z, z)):
        near += [{axis: lax.rem(index + step, 4)} for step in (1, 2, 3)]
    for where in near:
        pl.semaphore_signal(barrier, inc=1, device_id=where, device_id_type=MESH_ID)

    links = Links(send_sem, recv_sem)

    def gate_at(i, j, part=None):
        lines = pl.ds(0, 64) if part is None else pl.ds(32 * part, 32)
        return gate_all.at[j, i, c, lines]

    def up_at(i, j, part=None):
        lines = pl.ds(0, 64) if part is None else pl.ds(32 * part, 32)
        return up_all.at[i, j, c, lines]

    def down_lines(start, part):
        first, length = (start, 352) if part is None else (start + 176 * part, 176)
        return pl.ds(pl.multiple_of(704 * c + first, 16), length)

    wide = (
        PlaneGather(links, gate_at, Y, Z, (y, z), c),
        PlaneGather(links, up_at, Z, Y, (z, y), c),
    )
    narrow = (
        PlaneGather(
            links, lambda i, j, part=None: down_all.at[j, i, down_lines(0, part)], Y, Z, (y, z), c
        ),
        PlaneGather(
            links, lambda i, j, part=None: down_all.at[i, j, down_lines(352, part)], Z, Y, (z, y), c
        ),
    )

    along = (1 - c) * y + c * z

    def part_rows(i, part=None):
        first, length = (0, 32) if part is None else (16 * part, 16)
        return pl.ds(pl.multiple_of(128 * c + 32 * i + first, 16), length)

    def on_line(step):
        return {Y: lax.rem(y + (1 - c) * step, 4), Z: lax.rem(z + c * step, 4)}

    weight_x = Ring(
        links,
        lambda step: {X: lax.rem(x + step, 4)},
        (
            (out_all.at[0, part_rows(along)], out_all.at[2, part_rows(along)]),
            (out_all.at[0, part_rows(along)], out_all.at[1, part_rows(along)]),
        ),
        (
            (out_all.at[2, part_rows(along, 0)], out_all.at[3, part_rows(along, 0)]),
            (out_all.at[1, part_rows(along, 1)], out_all.at[3, part_rows(along, 1)]),
        ),
        (out_all.at[pl.ds(1, 2), part_rows(along)], out_all.at[3, part_rows(along)]),
    )

    def weight_ring(slots):
        own, low, high = (
            out_all.at[slots, part_rows(along)],
            out_all.at[slots, part_rows(lax.rem(along + 3, 4), 0)],
            out_all.at[slots, part_rows(lax.rem(along + 1, 4), 1)],
        )
        return Ring(
            links,
            on_line,
            ((own, own), (own, own)),
            ((low, low), (high, high)),
            (out_all.at[slots, pl.ds(0, 64)], own),
        )

    weight_far = weight_ring(pl.ds(3, 1))
    weight_rest = links.arrival()

    def send_rest(steps):
        for step in steps:
            part = part_rows(lax.rem(along + step, 4))
            for slot, target in ((2, x_up), (1, x_down)):
                links.send(weight_rest, out_all.at[0, part], out_all.at[slot, part], **{X: target})

    half_rows = pl.ds(pl.multiple_of(128 * c, 128), 128)

    scale = 128 ** (-0.5)
    at_row = lax.broadcasted_iota(jnp.int32, (BLOCK, BLOCK), 0)
    at_col = lax.broadcasted_iota(jnp.int32, (BLOCK, BLOCK), 1)
    upto = jnp.where(at_row <= at_col, 1.0, 0.0).astype(f32)
    cum_rows, cum_cols = [], []
    local["logs"].wait()
    for b in range(2):
        logs = jnp.concatenate(
            [logs_in[:, BLOCK * b : BLOCK * (b + 1)], jnp.zeros((6, BLOCK), f32)], axis=0
        )
        cum = jnp.dot(logs, upto, precision=lax.Precision.HIGHEST, preferred_element_type=f32)
        cum_rows.append(cum)
        cum_cols.append(cum.T)
    ends = [[cum_rows[b][h : h + 1, BLOCK - 1 : BLOCK] for b in range(2)] for h in range(2)]
    local["k"].wait()
    local["v"].wait()
    first_state, span = [], []
    for h in range(2):
        heads = slice(128 * h, 128 * (h + 1))
        added = []
        for b in range(2):
            lines = slice(BLOCK * b, BLOCK * (b + 1))
            to_end = jnp.exp(ends[h][b] - cum_cols[b][:, h : h + 1]) * scale
            scaled = (k[lines, heads].astype(f32) * to_end).astype(bf16)
            added.append(
                lax.dot_general(
                    scaled, v[lines, heads], (((0,), (0,)), ((), ())), preferred_element_type=f32
                )
            )
        first_state.append(added[0])
        span.append(
            (
                jnp.exp(over_lanes(ends[h][1])) * added[0] + added[1],
                jnp.exp(over_lanes(ends[h][0] + ends[h][1])),
            )
        )
        write_state(state_c.at[0, h], *span[h])
    pl.semaphore_wait(barrier, len(near))
    pair = links.arrival()
    links.send(pair, state_c.at[0], state_c.at[1], **{C: other})
    local["up"].wait()
    wide[1].own()
    local["weight"].wait()
    weight_x.start()
    send_rest((1,))
    local["down"].wait()
    swap = links.arrival()
    links.send(swap, half_down.at[c], half_down.at[c], **{C: other})
    local["gate"].wait()

    def within(h, b):
        heads, lines = slice(128 * h, 128 * (h + 1)), slice(BLOCK * b, BLOCK * (b + 1))
        col, row = cum_cols[b][:, h : h + 1], cum_rows[b][h : h + 1]
        products = lax.dot_general(
            q[lines, heads], k[lines, heads], (((1,), (1,)), ((), ())), preferred_element_type=f32
        )
        factor = jnp.where(at_row >= at_col, jnp.exp(jnp.minimum(col - row, 0.0)), 0.0)
        scores = (products * scale * factor).astype(bf16)
        result = jnp.dot(scores, v[lines, heads], preferred_element_type=f32)
        if b == 1:
            result = result + jnp.exp(col) * jnp.dot(
                q[lines, heads], first_state[h].astype(bf16), preferred_element_type=f32
            )
            col = col + ends[h][0]
        retention[h, lines, :] = result
        decayed[h, lines, :] = jnp.broadcast_to(jnp.exp(col), (BLOCK, 128))

    nothing = (jnp.zeros((128, 128), f32), jnp.ones((1, 128), f32))

    def among(slots, axis, index):
        came = links.arrival()
        for step in (2, 1, 3):
            links.send(came, slots.at[index], slots.at[index], **{axis: lax.rem(index + step, 4)})

        def fold():
            came.wait(slots.at[pl.ds(0, 3)])
            total, before = nothing, nothing
            for at in range(4):
                total = followed_by(total, read_state(slots.at[at]))
                before = chosen(at < index, total, before)
            return total, before

        return fold

    local["q"].wait()
    within(0, 0)
    pair.wait(state_c.at[1])
    partner = [read_state(state_c.at[1, h]) for h in range(2)]
    first = c == 0
    chip = [
        followed_by(chosen(first, span[h], partner[h]), chosen(first, partner[h], span[h]))
        for h in range(2)
    ]
    write_state(state_y.at[y], *chosen(first, chip[0], chip[1]))
    fold_y = among(state_y, Y, y)
    wide[0].own()
    within(0, 1)
    within(1, 0)
    line, before_y = fold_y()
    write_state(state_z.at[z], *line)
    fold_z = among(state_z, Z, z)
    swap.wait(half_down.at[other])
    turned[...] = jnp.concatenate([half_down[0], half_down[1]], axis=0).T
    down_all[z, y, own_half, :] = turned[own_half, :]
    within(1, 1)
    weight_x.pass_on()
    send_rest((2, 3))
    wide[1].pass_on()
    _, before_z = fold_z()
    state_in[c] = followed_by(before_z, before_y)[0]
    both_heads = links.arrival()
    links.send(both_heads, state_in.at[c], state_in.at[c], **{C: other})
    wide[0].pass_on()
    weight_x.finish()
    weight_far.start()
    for gather in narrow:
        gather.own()
    for name in ("g", "norm"):
        local[name].wait()
    both_heads.wait(state_in.at[other])
    entering = [
        jnp.where(first, state_in[h], partner[h][1] * state_in[h] + partner[h][0]).astype(bf16)
        for h in range(2)
    ]

    top, bottom = pl.ds(0, 128), pl.ds(128, 128)
    near_came, far_came, to_pass = (links.arrival() for _ in range(3))
    for step in (2, 1, 3, 0):
        quarter = lax.rem(x + step, 4)
        lines = pl.ds(pl.multiple_of(256 * quarter, 256), 256)
        for h in range(2):
            heads = slice(128 * h, 128 * (h + 1))
            carried = jnp.dot(q[lines, heads], entering[h], preferred_element_type=f32)
            value = retention[h, lines, :] + carried * decayed[h, lines, :]
            centered = value - jnp.mean(value, axis=-1, keepdims=True)
            variance = jnp.mean(centered * centered, axis=-1, keepdims=True)
            normed = centered * lax.rsqrt(variance + EPSILON) * norm_in[h : h + 1, :]
            retained[step, :, heads] = (jax.nn.silu(g[lines, heads].astype(f32)) * normed).astype(
                bf16
            )
        if step == 2:
            links.send(far_came, retained.at[2, top], regrouped.at[3, top], **{X: x_far})
            links.send(to_pass, retained.at[2, bottom], passing, **{X: x_down})
        elif step:
            slot = 2 if step == 1 else 1
            links.send(near_came, retained.at[step], regrouped.at[slot], **{X: quarter})
    weight_far.pass_on()
    for gather in narrow:
        gather.pass_on()
    for gather in (wide[1], wide[0]):
        gather.line()
    shared, shared_far = links.arrival(), links.arrival()
    weight_rest.wait(out_all.at[pl.ds(1, 2), pl.ds(0, 96)])
    near_half, far_half = out_all.at[pl.ds(1, 2), half_rows], out_all.at[3, half_rows]
    links.send(shared, near_half, near_half, **{C: other})
    to_pass.wait(passing)
    links.send(far_came, passing, regrouped.at[3, bottom], **{X: x_down})
    weight_far.finish()
    links.send(shared_far, far_half, far_half, **{C: other})
    for name in ("resid", "mix", "in", "out"):
        local[name].wait()
    near_came.wait(regrouped.at[pl.ds(1, 2)])
    shared.wait(out_all.at[pl.ds(1, 2), half_rows])

    def mix_part(slot, lanes):
        block = regrouped[slot] if slot else retained[0]
        part = jnp.dot(block, out_all[slot, :, lanes], preferred_element_type=f32)
        return part.astype(bf16).astype(f32)

    for j in range(8):
        lanes = slice(256 * j, 256 * (j + 1))
        mixed[:, lanes] = mix_part(0, lanes) + mix_part(1, lanes) + mix_part(2, lanes)
    far_came.wait(regrouped.at[3])
    shared_far.wait(out_all.at[3, half_rows])
    for j in range(8):
        lanes = slice(256 * j, 256 * (j + 1))
        partial[0, :, lanes] = (mixed[:, lanes] + mix_part(3, lanes)).astype(bf16)

    piece = [pl.ds(64 * at, 64) for at in range(4)]
    first_rows = [links.arrival(), links.arrival()]
    for at in range(4):

        @pl.loop(0, 2)
        def _(step):
            for start in (32 * at, 32 * at + 128):
                lines = pl.ds(pl.multiple_of(start + 16 * step, 16), 16)
                mid = (
                    middle[lines, :].astype(f32) + rms_norm(partial[0, lines, :], gains[0])
                ).astype(bf16)
                middle[lines, :] = mid
                rows[x, lines, :] = rms_norm(mid, gains[1]).astype(bf16)

        for target, start in ((x_up, 32 * at), (x_down, 32 * at + 128)):
            lines = pl.ds(start, 32)
            links.send(first_rows[at // 2], rows.at[x, lines], rows.at[x, lines], **{X: target})
    for gather in narrow:
        gather.line()
    for gather in (*wide, *narrow):
        gather.give(gather.j)
    far, nearby = links.arrival(), links.arrival()
    for at in range(2):
        first_rows[at].wait(rows.at[x, top])
        for target, source, lines in ((x_up, x_down, piece[at]), (x_down, x_up, piece[2 + at])):
            links.send(far, rows.at[source, lines], rows.at[source, lines], **{X: target})
        if at == 0:
            for gather in wide:
                gather.pass_line()
    for lines, target in ((bottom, x_up), (top, x_down)):
        links.send(nearby, rows.at[x, lines], rows.at[x, lines], **{X: target})
    for gather in narrow:
        gather.pass_line()
    for at in range(2):
        for gather in wide:
            gather.end_line(at)
    for gather in wide:
        gather.arrive()

    def gate_up(owner, slot, tiles=range(11)):
        block = rows[owner]
        for j in tiles:
            lanes = slice(128 * j, 128 * (j + 1))
            weights = jnp.concatenate(
                [
                    gate_all[:, :, :, :, lanes].reshape(2048, 128),
                    up_all[:, :, :, :, lanes].reshape(2048, 128),
                ],
                axis=1,
            )
            both = jnp.dot(block, weights, preferred_element_type=f32)
            hidden[slot, :, lanes] = (jax.nn.silu(both[:, :128]) * both[:, 128:]).astype(bf16)

    def down(slot, to, lines=pl.ds(0, 256), extra=None, tiles=range(8)):
        block = hidden[slot, lines, :]
        for j in tiles:
            weights = jnp.concatenate(
                [down_all[j // 2, 2 * j % 4], down_all[j // 2, 2 * j % 4 + 1]], axis=1
            )
            part = jnp.dot(block, weights, preferred_element_type=f32)
            lanes = slice(256 * j, 256 * (j + 1))
            if extra is not None:
                part = part + relay[extra, :, lanes].astype(f32)
            partial[to, lines, lanes] = part.astype(bf16)

    far.wait(rows.at[x_far])
    gate_up(x_far, 2, range(3))
    for at in range(2):
        for gather in narrow:
            gather.end_line(at)
    gate_up(x_far, 2, range(3, 11))
    for gather in narrow:
        gather.arrive()
    relay_up, relay_down = links.arrival(), links.arrival()
    for at in range(4):
        down(2, 1, tiles=range(2 * at, 2 * at + 2))
        lanes = pl.ds(512 * at, 512)
        links.send(relay_up, partial.at[1, top, lanes], relay.at[0, :, lanes], **{X: x_up})
        links.send(relay_down, partial.at[1, bottom, lanes], relay.at[1, :, lanes], **{X: x_down})
    nearby.wait(rows.at[x_up])
    gate_up(x_up, 0)
    down(0, 2, bottom)
    last = [links.arrival() for _ in range(5)]
    links.send(last[4], partial.at[2, bottom], final.at[0, bottom], **{X: x_up})
    gate_up(x_down, 1)
    down(1, 3, top)
    links.send(last[4], partial.at[3, top], final.at[1, top], **{X: x_down})
    gate_up(x, 2)
    relay_up.wait(relay.at[0])
    down(0, 2, top, 0)
    for at in range(4):
        lines = pl.ds(32 * at, 32)
        links.send(last[at], partial.at[2, lines], final.at[0, lines], **{X: x_up})
    relay_down.wait(relay.at[1])
    down(1, 3, bottom, 1)
    for at in range(4):
        lines = pl.ds(128 + 32 * at, 32)
        links.send(last[at], partial.at[3, lines], final.at[1, lines], **{X: x_down})
    down(2, 0)
    last[4].wait(final.at[0])

    @pl.loop(0, 4)
    def _(at):
        Arrival(links, last[0].at + at).wait(final.at[0, pl.ds(0, 64)])

        @pl.loop(0, 2)
        def _(step):
            for start in (0, 128):
                lines = pl.ds(pl.multiple_of(start + 32 * at + 16 * step, 16), 16)
                branch = (
                    partial[0, lines, :].astype(f32)
                    + final[0, lines, :].astype(f32)
                    + final[1, lines, :].astype(f32)
                ).astype(bf16)
                out[lines, :] = (
                    middle[lines, :].astype(f32) + rms_norm(branch, gains[2])
                ).astype(bf16)

    links.finish()


def per_device(
    queries, keys, values, gates, log_decay, norm_gain, out_weight, resid, post_mix_gain, pre_ffn_gain,
    w_gate, w_up, w_down, post_ffn_gain,
):
    f32, bf16 = jnp.float32, jnp.bfloat16
    operands = (
        queries, keys, values, gates, log_decay.T, norm_gain, out_weight, resid, post_mix_gain[None],
        pre_ffn_gain[None], w_gate, w_up, w_down.T, post_ffn_gain[None],
    )
    return pl.pallas_call(
        layer_kernel,
        out_shape=jax.ShapeDtypeStruct((256, 2048), bf16),
        in_specs=[pl.BlockSpec(memory_space=pl.ANY)] * 14,
        out_specs=pl.BlockSpec(memory_space=pltpu.VMEM),
        scratch_shapes=[
            pltpu.VMEM((4, 4, 2, 64, 1408), bf16),
            pltpu.VMEM((4, 4, 2, 64, 1408), bf16),
            pltpu.VMEM((4, 4, 1408, 128), bf16),
            pltpu.VMEM((4, 256, 2048), bf16),
            pltpu.VMEM((3, 256, 1408), bf16),
            pltpu.VMEM((4, 256, 2048), bf16),
            pltpu.VMEM((2, 128, 2048), bf16),
            pltpu.VMEM((2, 256, 2048), bf16),
            pltpu.VMEM((2, 64, 1408), bf16),
            pltpu.VMEM((1408, 128), bf16),
            pltpu.VMEM((1024, 256), bf16),
            pltpu.VMEM((1024, 256), bf16),
            pltpu.VMEM((1024, 256), bf16),
            pltpu.VMEM((1024, 256), bf16),
            pltpu.VMEM((2, 1024, 128), f32),
            pltpu.VMEM((2, 1024, 128), f32),
            pltpu.VMEM((2, 2, 144, 128), bf16),
            pltpu.VMEM((4, 144, 128), bf16),
            pltpu.VMEM((4, 144, 128), bf16),
            pltpu.VMEM((2, 128, 128), f32),
            pltpu.VMEM((4, 256, 256), bf16),
            pltpu.VMEM((4, 256, 256), bf16),
            pltpu.VMEM((128, 256), bf16),
            pltpu.VMEM((4, 256, 2048), bf16),
            pltpu.VMEM((256, 2048), f32),
            pltpu.VMEM((256, 2048), bf16),
            pltpu.VMEM((2, 1024), f32),
            pltpu.VMEM((3, 1, 2048), f32),
            pltpu.VMEM((2, 128), f32),
            pltpu.SemaphoreType.DMA((14,)),
            pltpu.SemaphoreType.DMA((SENDS,)),
            pltpu.SemaphoreType.DMA((ARRIVALS,)),
        ],
        compiler_params=pltpu.CompilerParams(
            collective_id=0, has_side_effects=True, vmem_limit_bytes=48 * 2**20
        ),
        name="layer",
    )(*(pltpu.with_memory_space_constraint(a, pltpu.HBM) for a in operands))


def solution(mesh):
    split = Mesh(mesh.devices.reshape(4, 4, 2, mesh.shape["tp"]), ("sp_0", "sp_1", "sp_2", "tp"))
    placed = (
        P(SP, "tp"),
        P(SP, "tp"),
        P(SP, "tp"),
        P(SP, "tp"),
        P(SP, "tp"),
        P("tp", None),
        P("tp", None),
        P(SP_TP, None),
        P(),
        P(),
        P(SP, "tp"),
        P(SP, "tp"),
        P("tp", SP),
        P(),
    )
    return jax.shard_map(
        per_device, mesh=split, in_specs=placed, out_specs=P(SP_TP, None), check_vma=False
    )
```
